256 devices in a mesh: sp: 16 (over y, x), tp: 16 (over z, core).
Axes of the slice: x: 4, y: 4, z: 8, core: 2. Of those that a mesh axis runs over, the one named last changes fastest.
Arguments:
- queries: bfloat16 [16384, 1536], P('sp', 'tp'), may hold values from -34 to 34
- latent: bfloat16 [16384, 512], P('sp'), may hold values from -6 to 6
- rot_key: bfloat16 [16384, 32], P('sp'), may hold values from -34 to 34
- latent_gain: float32 [512], replicated, may hold values from 0.1 to 1.9
- key_up: bfloat16 [512, 1024], P(None, 'tp'), may hold values from -0.25 to 0.25
- value_up: bfloat16 [512, 1024], P(None, 'tp'), may hold values from -0.70710678 to 0.70710678
- query_gain: float32 [96], replicated, may hold values from 0.5 to 6
- key_gain: float32 [96], replicated, may hold values from 0.5 to 6
- out_gain: float32 [1024], replicated, may hold values from 0.1 to 1.9
- out_weight: bfloat16 [1024, 2048], replicated, may hold values from -0.1875 to 0.1875
- residual: bfloat16 [16384, 2048], P(('sp', 'tp')), may hold values from -6 to 6
- ffn_gain: float32 [2048], replicated, may hold values from 0.1 to 1.9
- routes: int32 [16384, 2], P(('sp', 'tp')), may hold values from 0 to 15, all different within a row; in each aligned block of 64 rows (0 to 63, 64 to 127, ...) at most 9 rows name the same one
- route_weights: float32 [16384, 2], P(('sp', 'tp')), may hold values from 0.2 to 1
- expert_gate: bfloat16 [16, 2048, 2048], P('sp', None, 'tp'), may hold values from -0.125 to 0.125
- expert_up: bfloat16 [16, 2048, 2048], P('sp', None, 'tp'), may hold values from -0.125 to 0.125
- expert_down: bfloat16 [16, 2048, 2048], P('sp', 'tp'), may hold values from -0.125 to 0.125
Outputs:
- layer_out: bfloat16 [16384, 2048], P(('sp', 'tp'))
The draws below stay inside these ranges and needn't reach their ends.
Inputs may be any that keep to these rules, and one draw needn't show every extreme that they name: `routes`: the 2 experts of a token differ. Among the 64 rows of one device each expert is named by at most 9 rows, a bound that some block reaches.
All inputs are finite; a program needn't handle non-finite values.
Results may differ from the reference program's by a relative error of at most 0.02.
The reference program's roundings to bfloat16 on the way count: a program that leaves them out, or rounds other values in their place, can miss the bound.
Values may be sent and summed in bfloat16 or wider, within the bound.
A program may use at most 128 MiB of HBM per device.

```python
import math
import jax
import jax.numpy as jnp
import numpy as np
from jax import lax

D = 2048
HEADS = 16
NOPE = 64
ROPE = 32
VH = 64
LAT = 512
FF_E = 2048
TOPK = 2
TOK_DEV = 64
QK = 96
ATT_WIDTH = 1024
POS_SP = 1024
LENGTH = 16384
EXPERTS = 16
CAP = 9
N_SP = 16
N_TP = 16


def drawn_pair(key):
    base_query = jnp.clip(jax.random.normal(jax.random.fold_in(key, 11), (LENGTH, HEADS, QK), jnp.float32), -6.0, 6.0)
    base_key = jnp.clip(jax.random.normal(jax.random.fold_in(key, 12), (LENGTH, ROPE), jnp.float32), -6.0, 6.0)
    return (base_query.reshape(LENGTH, HEADS * QK), base_key)


def draw_queries(key, part):
    return drawn_pair(key)[0].astype(jnp.bfloat16)


def draw_rot_key(key, part):
    return drawn_pair(key)[1].astype(jnp.bfloat16)


def head_gains(key):
    spread = 1.0 + 0.18 * jax.random.uniform(jax.random.fold_in(key, 1), (QK,), jnp.float32, -2.5, 2.5)
    return spread


def draw_query_gain(key, part):
    return head_gains(jax.random.fold_in(key, 21))


def draw_key_gain(key, part):
    return head_gains(jax.random.fold_in(key, 22))


def draw_value_up(key, part):
    head_ids = jnp.arange(HEADS * VH, dtype=jnp.int32) // VH
    rising = head_ids.astype(jnp.float32) / max(HEADS - 1, 1)
    entries = jnp.clip(jax.random.normal(jax.random.fold_in(key, 32), (LAT, HEADS * VH), jnp.float32), -4.0, 4.0)
    column_scale = 3.0 ** rising
    return (entries * column_scale[None, :] / jnp.sqrt(jnp.float32(LAT))).astype(jnp.bfloat16)


def shard_levels(rng, extent, shards, smallest, top_value):
    loudness = 1.0
    for position, parts in shards:
        steps = jax.random.uniform(jax.random.fold_in(jax.random.fold_in(rng, 6), position), (parts,), jnp.float32, smallest / len(shards), top_value / len(shards))
        loudness = loudness * jnp.repeat(jnp.exp(steps), extent[position] // parts).reshape((-1,) + (1,) * (len(extent) - 1 - position))
    return loudness


def shared_out(own_key, own, number, rows, number_of, top, reach, lean):
    ranking = jax.random.permutation(own_key, number_of)
    packed, ordinary = load_shares(number_of, rows * top, reach, lean, True), load_shares(number_of, rows * top, reach, lean, False)
    places = jnp.arange(number_of)

    def named(lengths, offset_by):
        used = int((lengths > 0).sum())
        fixed = max(1, used // 4)
        moved = fixed + (places - fixed + offset_by * (used - fixed)) % max(1, number_of - fixed)
        return jnp.zeros((number_of,), jnp.int32).at[ranking[jnp.where(places < fixed, places, moved)]].set(jnp.asarray(lengths, jnp.int32))

    lengths = jnp.where(number % 4 == 0, named(packed, number // 4), named(ordinary, number - number // 4 - 1))
    mixed = jax.random.permutation(jax.random.fold_in(own, 3), number_of)
    giver, sink = mixed[0:number_of // 2 * 2:2], mixed[1:number_of // 2 * 2:2]
    slack = jnp.minimum(lengths[giver] - 1, reach - lengths[sink]) // 2
    slack = jnp.where((giver == ranking[0]) | (sink == ranking[0]) | (lengths[sink] == 0), 0, jnp.maximum(slack, 0))
    moved = jax.random.randint(jax.random.fold_in(own, 4), (number_of // 2,), 0, 1 << 20) % (slack + 1)
    lengths = lengths.at[giver].add(-moved).at[sink].add(moved)
    members = jnp.searchsorted(jnp.cumsum(lengths), jnp.arange(rows * top), side="right").astype(jnp.int32)
    listing = members.reshape(top, rows).T
    listing = listing[jax.random.permutation(jax.random.fold_in(own, 1), rows)]
    offset_by = jax.random.randint(jax.random.fold_in(own, 2), (rows, 1), 0, top)
    return jnp.take_along_axis(listing, (jnp.arange(top)[None, :] + offset_by) % top, axis=1)


def load_shares(number_of, total, bound, slope, full):
    portions = [(1 << 20) // math.isqrt(rank ** slope) + 1 for rank in range(1, number_of + 1)]
    largest = bound if full else min(bound, max(-(-total // number_of), total * portions[0] // sum(portions)))
    least = 1 if total - largest >= number_of - 1 else 0
    given, rest = [largest] + [least] * (number_of - 1), total - largest - least * (number_of - 1)
    while rest > 0:
        candidates = [i for i in range(1, number_of) if given[i] < largest] or [i for i in range(1, number_of) if given[i] < bound]
        pool, budget = sum([portions[i] for i in candidates]), rest
        for i in candidates:
            more = min(bound - given[i], max(1, budget * portions[i] // pool), rest)
            given[i] = given[i] + more
            rest = rest - more
    return np.array(given)


def bell_draw(rng, dims, deviation, bound, split=(), kind=jnp.bfloat16):
    values = deviation * jax.random.normal(rng, dims, jnp.float32)
    if split:
        values = values * shard_levels(rng, dims, split, -0.22, 0.18)
    return jnp.clip(values, -bound, bound).astype(kind)


def setup_inputs(seed: int = 0) -> dict:
    streams_of = jax.random.split(jax.random.key(seed), 18)
    queries = draw_queries(jax.random.fold_in(streams_of[17], 71), 0)
    latent = bell_draw(streams_of[1], (LENGTH, LAT), 1.0, 6.0, ((0, 16),))
    rot_key = draw_rot_key(jax.random.fold_in(streams_of[17], 71), 0)
    latent_gain = jnp.clip(1.0 + 0.18 * jax.random.normal(streams_of[3], (LAT,), jnp.float32), 0.1, 1.9)
    key_up = bell_draw(streams_of[4], (LAT, HEADS * NOPE), LAT ** -0.5, 0.25, ((1, 16),))
    value_up = draw_value_up(jax.random.fold_in(streams_of[17], 71), 0)
    query_gain = draw_query_gain(jax.random.fold_in(streams_of[17], 71), 0)
    key_gain = draw_key_gain(jax.random.fold_in(streams_of[17], 71), 0)
    out_gain = jnp.clip(1.0 + 0.18 * jax.random.normal(streams_of[8], (ATT_WIDTH,), jnp.float32), 0.1, 1.9)
    out_weight = bell_draw(streams_of[9], (ATT_WIDTH, D), ATT_WIDTH ** -0.5, 0.1875)
    residual = bell_draw(streams_of[10], (LENGTH, D), 1.0, 6.0, ((0, 256),))
    ffn_gain = jnp.clip(1.0 + 0.18 * jax.random.normal(streams_of[11], (D,), jnp.float32), 0.1, 1.9)
    routes_keys = jax.random.split(jax.random.fold_in(streams_of[12], 1), LENGTH // TOK_DEV)
    routes_turns = jax.random.permutation(jax.random.fold_in(streams_of[12], 3), LENGTH // TOK_DEV)
    routes = jax.vmap(lambda own, number: shared_out(jax.random.fold_in(streams_of[12], 2), own, number, TOK_DEV, EXPERTS, TOPK, CAP, 1))(routes_keys, routes_turns).reshape((LENGTH, TOPK))
    route_weights = jnp.clip(0.2 + 0.8 * jax.random.uniform(streams_of[13], (LENGTH, TOPK), jnp.float32) ** shard_levels(streams_of[13], (LENGTH, TOPK), ((0, 256),), -0.2, 0.2), 0.2, 1.0)
    expert_gate = bell_draw(streams_of[14], (EXPERTS, D, FF_E), D ** -0.5, 0.125, ((0, 16), (2, 16)))
    expert_up = bell_draw(streams_of[15], (EXPERTS, D, FF_E), D ** -0.5, 0.125, ((0, 16), (2, 16)))
    expert_down = bell_draw(streams_of[16], (EXPERTS, FF_E, D), FF_E ** -0.5, 0.125, ((0, 16), (1, 16)))
    return dict(queries=queries, latent=latent, rot_key=rot_key, latent_gain=latent_gain, key_up=key_up, value_up=value_up, query_gain=query_gain, key_gain=key_gain, out_gain=out_gain, out_weight=out_weight, residual=residual, ffn_gain=ffn_gain, routes=routes, route_weights=route_weights, expert_gate=expert_gate, expert_up=expert_up, expert_down=expert_down)


epsilon = 1e-06
rope_base = 10000.0

def rms_scale(values):
    return lax.rsqrt(lax.optimization_barrier(jnp.mean(values * values, axis=-1, keepdims=True)) + epsilon)

def rotate_half(values, angles):
    half_dims = values.shape[-1] // 2
    first_half = values[..., :half_dims]
    second_half = values[..., half_dims:]
    cosine = jnp.cos(angles)
    sine_val = jnp.sin(angles)
    return jnp.concatenate([first_half * cosine - second_half * sine_val, second_half * cosine + first_half * sine_val], axis=-1)

def head_prepare(raw_rows, gain_vec, angles):
    normed_rows = raw_rows * rms_scale(raw_rows) * gain_vec
    turned_rows = rotate_half(normed_rows[..., NOPE:], angles[:, None, :])
    return jnp.concatenate([normed_rows[..., :NOPE], turned_rows], axis=-1).astype(jnp.bfloat16)

def attend_head(head_inputs):
    query_head, key_head, value_head = head_inputs
    query_f32 = query_head.astype(jnp.float32)
    key_f32 = key_head.astype(jnp.float32)
    value_f32 = value_head.astype(jnp.float32)
    block_count = LENGTH // POS_SP
    query_blocks = query_f32.reshape(block_count, POS_SP, QK)
    key_pos = jnp.arange(LENGTH, dtype=jnp.int32)

    def one_block(block_inputs):
        block_index, query_block = block_inputs
        scores = jnp.dot(query_block, key_f32.T, precision=lax.Precision.HIGHEST) * QK ** (-0.5)
        query_pos = block_index * POS_SP + jnp.arange(POS_SP, dtype=jnp.int32)
        allowed = key_pos[None, :] <= query_pos[:, None]
        scores = jnp.where(allowed, scores, -1e+30)
        row_peak = lax.optimization_barrier(jnp.max(scores, axis=1, keepdims=True))
        exponent = jnp.where(allowed, jnp.exp(scores - row_peak), 0.0)
        row_total = lax.optimization_barrier(jnp.sum(exponent, axis=1))
        rounded_exp = lax.optimization_barrier(exponent.astype(jnp.bfloat16)).astype(jnp.float32)
        result = jnp.dot(rounded_exp, value_f32, precision=lax.Precision.HIGHEST) / row_total[:, None]
        return result.astype(jnp.bfloat16)
    outputs = lax.map(one_block, (jnp.arange(block_count, dtype=jnp.int32), query_blocks))
    return outputs.reshape(LENGTH, VH)

def reference(queries, latent, rot_key, latent_gain, key_up, value_up, query_gain, key_gain, out_gain, out_weight, residual, ffn_gain, routes, route_weights, expert_gate, expert_up, expert_down):
    lat_f32 = latent.astype(jnp.float32)
    normed_latent = (lat_f32 * rms_scale(lat_f32) * latent_gain).astype(jnp.bfloat16)
    key_nope = jnp.dot(normed_latent, key_up, preferred_element_type=jnp.float32).astype(jnp.bfloat16)
    values = jnp.dot(normed_latent, value_up, preferred_element_type=jnp.float32).astype(jnp.bfloat16)
    positions = jnp.arange(LENGTH, dtype=jnp.int32)
    inverse = rope_base ** (-jnp.arange(0, ROPE, 2, dtype=jnp.float32) / ROPE)
    angles = positions.astype(jnp.float32)[:, None] * inverse[None, :]
    shared = jnp.broadcast_to(rot_key.astype(jnp.float32)[:, None, :], (LENGTH, HEADS, ROPE))
    raw_keys = jnp.concatenate([key_nope.astype(jnp.float32).reshape(LENGTH, HEADS, NOPE), shared], axis=-1)
    key_rows = head_prepare(raw_keys, key_gain, angles)
    query_rows = head_prepare(queries.astype(jnp.float32).reshape(LENGTH, HEADS, QK), query_gain, angles)
    value_heads = values.reshape(LENGTH, HEADS, VH)
    attended = lax.map(attend_head, (jnp.transpose(query_rows, (1, 0, 2)), jnp.transpose(key_rows, (1, 0, 2)), jnp.transpose(value_heads, (1, 0, 2))))
    att_rows = jnp.transpose(attended, (1, 0, 2)).reshape(LENGTH, ATT_WIDTH).astype(jnp.float32)
    normed_att = (att_rows * rms_scale(att_rows) * out_gain).astype(jnp.bfloat16)
    group_width = ATT_WIDTH // N_TP
    mixed = jnp.zeros((LENGTH, D), jnp.float32)
    for group_index in range(N_TP):
        low = group_index * group_width
        partial_value = jnp.dot(normed_att[:, low:low + group_width], out_weight[low:low + group_width], preferred_element_type=jnp.float32).astype(jnp.bfloat16)
        mixed = mixed + lax.optimization_barrier(partial_value).astype(jnp.float32)
    middle = residual.astype(jnp.float32) + mixed
    ffn_input = (middle * rms_scale(middle) * ffn_gain).astype(jnp.bfloat16)
    flat_routes = routes.reshape(-1).astype(jnp.int32)
    row_order = jnp.argsort(flat_routes, stable=True).astype(jnp.int32)
    expert_counts = lax.optimization_barrier(jnp.sum((flat_routes[:, None] == jnp.arange(EXPERTS, dtype=jnp.int32)[None, :]).astype(jnp.int32), axis=0))
    offsets = (jnp.cumsum(expert_counts) - expert_counts).astype(jnp.int32)
    row_limit = N_SP * N_TP * CAP
    weights_flat = route_weights.reshape(-1).astype(jnp.float32)
    hidden_width = FF_E // N_TP

    def per_expert(expert_id, combined):
        slot_ids = jnp.arange(row_limit, dtype=jnp.int32)
        is_live = slot_ids < expert_counts[expert_id]
        picked = row_order[jnp.minimum(offsets[expert_id] + slot_ids, LENGTH * TOPK - 1)]
        token_ids = (picked // TOPK).astype(jnp.int32)
        expert_in = ffn_input[token_ids]
        gate_pre = jnp.dot(expert_in, expert_gate[expert_id], preferred_element_type=jnp.float32)
        up_pre = jnp.dot(expert_in, expert_up[expert_id], preferred_element_type=jnp.float32)
        hidden = (jax.nn.silu(gate_pre) * up_pre).astype(jnp.bfloat16)
        down_weight = expert_down[expert_id]
        down_sum = jnp.zeros((row_limit, D), jnp.float32)
        for group_index in range(N_TP):
            low = group_index * hidden_width
            partial_value = jnp.dot(hidden[:, low:low + hidden_width], down_weight[low:low + hidden_width], preferred_element_type=jnp.float32).astype(jnp.bfloat16)
            down_sum = down_sum + lax.optimization_barrier(partial_value).astype(jnp.float32)
        expert_out = lax.optimization_barrier(down_sum.astype(jnp.bfloat16)).astype(jnp.float32)
        contrib_rows = expert_out * (weights_flat[picked] * is_live.astype(jnp.float32))[:, None]
        return combined.at[token_ids].add(contrib_rows)
    combined = lax.fori_loop(0, EXPERTS, per_expert, jnp.zeros((LENGTH, D), jnp.float32))
    return (middle + combined).astype(jnp.bfloat16)
```

```python
import jax
import jax.numpy as jnp
from jax import lax
from jax.experimental import pallas as pl
from jax.experimental.pallas import tpu as pltpu
from jax.sharding import PartitionSpec as P

D = 2048
NOPE = 64
ROPE = 32
VH = 64
TOPK = 2
QK = 96


epsilon = 1e-06
rope_base = 10000.0


def rms_scale(values):
    return lax.rsqrt(jnp.mean(values * values, axis=-1, keepdims=True) + epsilon)


def rotate_half(values, angles):
    half_dims = values.shape[-1] // 2
    first_half = values[..., :half_dims]
    second_half = values[..., half_dims:]
    cosine = jnp.cos(angles)
    sine_val = jnp.sin(angles)
    return jnp.concatenate(
        [
            first_half * cosine - second_half * sine_val,
            second_half * cosine + first_half * sine_val,
        ],
        axis=-1,
    )


def head_prepare(raw_rows, gain_vec, angles):
    normed_rows = raw_rows * rms_scale(raw_rows) * gain_vec
    turned_rows = rotate_half(normed_rows[..., NOPE:], angles[:, None, :])
    return jnp.concatenate([normed_rows[..., :NOPE], turned_rows], axis=-1).astype(jnp.bfloat16)


def slot_targets(route_rows, expert_total, slot_cap):
    flat_routes = route_rows.reshape(-1)
    one_hot = (flat_routes[:, None] == jnp.arange(expert_total, dtype=jnp.int32)[None, :]).astype(
        jnp.int32
    )
    earlier = jnp.cumsum(one_hot, axis=0) - one_hot
    rank_in = jnp.sum(earlier * one_hot, axis=1)
    return (flat_routes * slot_cap + rank_in).reshape(route_rows.shape)


def select_matrix(targets, slot_total):
    hits = targets[:, :, None] == jnp.arange(slot_total, dtype=jnp.int32)[None, None, :]
    return jnp.sum(hits.astype(jnp.bfloat16), axis=1)


SCORE_EXP = 1.4426950408889634 * QK ** (-0.5)
Q_TILE = 256


def attend_body(q_ref, kv_ref, out_ref, peak_ref, acc_ref, val_ref, block_count):
    shard_len = kv_ref.shape[2]
    half = shard_len // 2
    mine = lax.axis_index("sp")
    low = jnp.minimum(mine, block_count - 1 - mine)
    high = block_count - 1 - low
    shift = jnp.where(mine < block_count // 2, 0, half)
    peak_ref[...] = jnp.full_like(peak_ref, -1e30)
    acc_ref[...] = jnp.zeros_like(acc_ref)
    lane = lax.broadcasted_iota(jnp.int32, (shard_len, 128), 1)
    val_ref[...] = jnp.where(lane == VH, 1.0, 0.0).astype(jnp.bfloat16)

    def one_block(block, parts):
        keys = kv_ref[block, :QK, :]
        val_ref[:, :VH] = kv_ref[block, QK:, :].T
        values = val_ref[...]
        for start, masked in parts:
            for first in range(start, start + half, Q_TILE):
                rows = pl.ds(first, Q_TILE)
                scores = jnp.dot(q_ref[rows, :], keys, preferred_element_type=jnp.float32)
                if masked:
                    row = lax.broadcasted_iota(jnp.int32, scores.shape, 0)
                    col = lax.broadcasted_iota(jnp.int32, scores.shape, 1)
                    scores = jnp.where(col - row <= shift + (first - start), scores, -1e30)
                old = peak_ref[rows, :]
                new = jnp.maximum(old, jnp.max(scores, axis=1, keepdims=True))
                weights = jnp.exp2((scores - new[:, :1]) * SCORE_EXP).astype(jnp.bfloat16)
                factor = jnp.exp2((old - new) * SCORE_EXP)
                peak_ref[rows, :] = new
                acc_ref[rows, :] = acc_ref[rows, :] * factor + jnp.dot(
                    weights, values, preferred_element_type=jnp.float32
                )

    lax.fori_loop(0, low, lambda j, _: one_block(j, ((0, False), (half, False))), None)
    one_block(low, ((0, True), (half, False)))
    lax.fori_loop(low + 1, high, lambda j, _: one_block(j, ((half, False),)), None)
    one_block(high, ((half, True),))
    total = acc_ref[:, VH : VH + 1]
    out_ref[...] = (acc_ref[:, :VH] / total).astype(jnp.bfloat16)


def flash_attention(query_pair, key_blocks, block_count):
    shard_len = query_pair.shape[0]

    def kernel(q_ref, kv_ref, out_ref, peak_ref, acc_ref, val_ref):
        attend_body(q_ref, kv_ref, out_ref, peak_ref, acc_ref, val_ref, block_count)

    return pl.pallas_call(
        kernel,
        out_shape=jax.ShapeDtypeStruct((shard_len, VH), jnp.bfloat16),
        in_specs=[pl.BlockSpec(memory_space=pltpu.VMEM)] * 2,
        out_specs=pl.BlockSpec(memory_space=pltpu.VMEM),
        scratch_shapes=[
            pltpu.VMEM((shard_len, 128), jnp.float32),
            pltpu.VMEM((shard_len, 128), jnp.float32),
            pltpu.VMEM((shard_len, 128), jnp.bfloat16),
        ],
        compiler_params=pltpu.CompilerParams(vmem_limit_bytes=40 * 1024 * 1024),
        cost_estimate=pl.CostEstimate(
            flops=9 * shard_len * shard_len * 320, bytes_accessed=6 << 20, transcendentals=9 << 20
        ),
    )(query_pair, key_blocks)


ROW_CUT = 80


def expert_ring(rows, gate, up, down):
    count, width = rows.shape
    hidden = gate.shape[1]
    chips = lax.axis_size("tp") // 2
    both = 2 * count

    def kernel(
        x_ref, gate_ref, up_ref, down_ref, out_ref,
        both_ref, seen, own_part, far_part, near_part, run_in, run_out,
        fwd_send, fwd_recv, back_send, back_recv, twin_send, twin_recv,
        part_send, part_recv, sum_fwd_send, sum_fwd_recv, sum_back_send, sum_back_recv,
    ):
        place = lax.axis_index("tp")
        chip, core = place // 2, place % 2
        toward = jnp.where(core == 0, 1, chips - 1)
        ahead = ((chip + toward) % chips) * 2 + core
        behind = ((chip + chips - toward) % chips) * 2 + core
        twin = chip * 2 + 1 - core

        barrier = pltpu.get_barrier_semaphore()
        for other in (ahead, behind, twin):
            pl.semaphore_signal(
                barrier, inc=1, device_id={"tp": other}, device_id_type=pl.DeviceIdType.MESH
            )
        pl.semaphore_wait(barrier, 3)

        def remote(source, target, send, recv, other):
            return pltpu.make_async_remote_copy(
                src_ref=source,
                dst_ref=target,
                send_sem=send,
                recv_sem=recv,
                device_id={"tp": other},
                device_id_type=pl.DeviceIdType.MESH,
            )

        first, second = pl.ds(0, ROW_CUT), pl.ds(ROW_CUT, count - ROW_CUT)
        front, rear = pl.ds(0, count), pl.ds(count, count)

        def forward(step):
            return (
                remote(seen.at[step, first], seen.at[step + 1, first],
                       fwd_send.at[step], fwd_recv.at[step + 1], ahead),
                remote(seen.at[step, second], seen.at[step + 1, second],
                       back_send.at[step], back_recv.at[step + 1], behind),
            )

        def forward_own():
            return (
                remote(x_ref.at[first], seen.at[1, first], fwd_send.at[0], fwd_recv.at[1], ahead),
                remote(x_ref.at[second], seen.at[1, second],
                       back_send.at[0], back_recv.at[1], behind),
            )

        def share(step):
            return remote(seen.at[step, front], seen.at[step, rear],
                          twin_send.at[step], twin_recv.at[step], twin)

        def share_own():
            return remote(x_ref, seen.at[0, rear], twin_send.at[0], twin_recv.at[0], twin)

        def hand_over(step):
            return remote(far_part.at[step], near_part.at[step],
                          part_send.at[step], part_recv.at[step], twin)

        def pass_sum(step):
            return (
                remote(run_out.at[step, first], run_in.at[step + 1, first],
                       sum_fwd_send.at[step], sum_fwd_recv.at[step + 1], ahead),
                remote(run_out.at[step, second], run_in.at[step + 1, second],
                       sum_back_send.at[step], sum_back_recv.at[step + 1], behind),
            )

        def experts(step):
            tokens = seen[step]
            pre = jnp.dot(tokens, both_ref[...], preferred_element_type=jnp.float32)
            inner = (jax.nn.silu(pre[:, :hidden]) * pre[:, hidden:]).astype(jnp.bfloat16)
            part = jnp.dot(inner, down_ref[...], preferred_element_type=jnp.float32).astype(
                jnp.bfloat16
            )
            own_part[step] = part[:count]
            far_part[step] = part[count:]

        for copy in (*forward_own(), share_own()):
            copy.start()
        both_ref[:, :hidden] = gate_ref[...]
        both_ref[:, hidden:] = up_ref[...]
        seen[0, front, :] = x_ref[...]
        share_own().wait_recv()
        experts(0)
        hand_over(0).start()

        def step_of(step, _):
            arrived = forward(step - 1)
            arrived[0].wait_recv()
            arrived[1].wait_recv()

            @pl.when(step < chips - 1)
            def _():
                for copy in forward(step):
                    copy.start()

            share(step).start()
            share(step).wait_recv()
            experts(step)
            hand_over(step).start()
            hand_over(step).wait_recv()

            @pl.when(step > 1)
            def _():
                for copy in pass_sum(step - 1):
                    copy.wait_recv()
                run_out[step] = (
                    run_in[step].astype(jnp.float32)
                    + own_part[step].astype(jnp.float32)
                    + near_part[step].astype(jnp.float32)
                ).astype(jnp.bfloat16)

            @pl.when(step == 1)
            def _():
                run_out[step] = (
                    own_part[step].astype(jnp.float32) + near_part[step].astype(jnp.float32)
                ).astype(jnp.bfloat16)

            for copy in pass_sum(step):
                copy.start()

        lax.fori_loop(1, chips, step_of, None)
        hand_over(0).wait_recv()
        for copy in pass_sum(chips - 1):
            copy.wait_recv()
        out_ref[...] = (
            run_in[chips].astype(jnp.float32)
            + own_part[0].astype(jnp.float32)
            + near_part[0].astype(jnp.float32)
        ).astype(jnp.bfloat16)

        for copy in (*forward_own(), share_own(), hand_over(0)):
            copy.wait_send()

        def drain(step, _):
            @pl.when(step < chips - 1)
            def _():
                for copy in forward(step):
                    copy.wait_send()

            share(step).wait_send()
            hand_over(step).wait_send()
            for copy in pass_sum(step):
                copy.wait_send()

        lax.fori_loop(1, chips, drain, None)

    block = (count, width)
    sems = [pltpu.SemaphoreType.DMA((chips + 1,)) for _ in range(12)]
    return pl.pallas_call(
        kernel,
        out_shape=jax.ShapeDtypeStruct(block, jnp.bfloat16),
        in_specs=[pl.BlockSpec(memory_space=pltpu.VMEM)] * 4,
        out_specs=pl.BlockSpec(memory_space=pltpu.VMEM),
        scratch_shapes=[
            pltpu.VMEM((width, 2 * hidden), jnp.bfloat16),
            pltpu.VMEM((chips, both, width), jnp.bfloat16),
            pltpu.VMEM((chips, *block), jnp.bfloat16),
            pltpu.VMEM((chips, *block), jnp.bfloat16),
            pltpu.VMEM((chips, *block), jnp.bfloat16),
            pltpu.VMEM((chips + 1, *block), jnp.bfloat16),
            pltpu.VMEM((chips, *block), jnp.bfloat16),
            *sems,
        ],
        compiler_params=pltpu.CompilerParams(
            collective_id=3, has_side_effects=True, vmem_limit_bytes=50 * 1024 * 1024
        ),
    )(rows, gate, up, down)


def shards(
    queries,
    latent,
    rot_key,
    latent_gain,
    key_up,
    value_up,
    query_gain,
    key_gain,
    out_gain,
    out_weight,
    residual,
    ffn_gain,
    routes,
    route_weights,
    expert_gate,
    expert_up,
    expert_down,
):
    shard_len = queries.shape[0]
    local_heads = key_up.shape[1] // NOPE
    sp_count = lax.axis_size("sp")
    tp_count = lax.axis_size("tp")
    my_first = lax.axis_index("sp") * shard_len
    positions = my_first + jnp.arange(shard_len, dtype=jnp.int32)
    inverse = rope_base ** (-jnp.arange(0, ROPE, 2, dtype=jnp.float32) / ROPE)
    angles = positions.astype(jnp.float32)[:, None] * inverse[None, :]
    lat_f32 = latent.astype(jnp.float32)
    normed_latent = (lat_f32 * rms_scale(lat_f32) * latent_gain).astype(jnp.bfloat16)
    key_nope = jnp.dot(normed_latent, key_up, preferred_element_type=jnp.float32).astype(
        jnp.bfloat16
    )
    value_rows = jnp.dot(normed_latent, value_up, preferred_element_type=jnp.float32).astype(
        jnp.bfloat16
    )
    shared = rot_key.astype(jnp.float32)[:, None, :]
    raw_keys = jnp.concatenate(
        [key_nope.astype(jnp.float32).reshape(shard_len, local_heads, NOPE), shared], axis=-1
    )
    key_rows = head_prepare(raw_keys, key_gain, angles)
    query_rows = head_prepare(
        queries.astype(jnp.float32).reshape(shard_len, local_heads, QK), query_gain, angles
    )
    bundle = jnp.concatenate([key_rows.reshape(shard_len, QK).T, value_rows.T], axis=0)
    key_blocks = lax.all_gather(bundle, "sp", axis=0, tiled=False)
    low_side = lax.axis_index("sp") < sp_count // 2
    half = shard_len // 2
    query_rows = query_rows.reshape(shard_len, QK)
    mirror = [(place, sp_count - 1 - place) for place in range(sp_count)]
    kept = jnp.where(low_side, query_rows[:half], query_rows[half:])
    sent = jnp.where(low_side, query_rows[half:], query_rows[:half])
    traded = lax.ppermute(sent, "sp", mirror)
    query_pair = jnp.where(
        low_side, jnp.concatenate([kept, traded]), jnp.concatenate([traded, kept])
    )
    pair_out = flash_attention(query_pair, key_blocks, sp_count)
    own_out = jnp.where(low_side, pair_out[:half], pair_out[half:])
    other_out = jnp.where(low_side, pair_out[half:], pair_out[:half])
    traded_out = lax.ppermute(other_out, "sp", mirror)
    head_major = jnp.where(
        low_side, jnp.concatenate([own_out, traded_out]), jnp.concatenate([traded_out, own_out])
    )
    tok_count = residual.shape[0]
    token_rows = lax.all_to_all(head_major, "tp", split_axis=0, concat_axis=1, tiled=True).astype(
        jnp.float32
    )
    normed_rows = (token_rows * rms_scale(token_rows) * out_gain).astype(jnp.bfloat16)
    partials = jnp.einsum(
        "tgc,gcd->tgd",
        normed_rows.reshape(tok_count, tp_count, -1),
        out_weight.reshape(tp_count, -1, D),
        preferred_element_type=jnp.float32,
    )
    rounded = lax.optimization_barrier(partials.astype(jnp.bfloat16))
    mixed = jnp.sum(rounded.astype(jnp.float32), axis=1)
    middle = residual.astype(jnp.float32) + mixed
    ffn_input = (middle * rms_scale(middle) * ffn_gain).astype(jnp.bfloat16)
    slot_cap = max(2, 9 * tok_count * TOPK // (8 * sp_count))
    slot_total = sp_count * slot_cap
    targets = slot_targets(routes, sp_count, slot_cap)
    chooser = select_matrix(targets, slot_total)
    outbound = (
        jnp.einsum("ts,td->sd", chooser, ffn_input, preferred_element_type=jnp.float32)
        .astype(jnp.bfloat16)
        .reshape(sp_count, slot_cap, D)
    )
    arrived = lax.all_to_all(outbound, "sp", split_axis=0, concat_axis=0, tiled=True)
    item_count = arrived.shape[1]
    flat_rows = arrived.reshape(sp_count * item_count, D)
    served = expert_ring(flat_rows, expert_gate[0], expert_up[0], expert_down[0]).reshape(
        sp_count, item_count, D
    )
    returned_rows = lax.all_to_all(served, "sp", split_axis=0, concat_axis=0, tiled=True).reshape(
        slot_total, D
    )
    picked = (
        jnp.take(returned_rows, targets.reshape(-1), axis=0)
        .reshape(tok_count, TOPK, D)
        .astype(jnp.float32)
    )
    moe_sum = jnp.sum(picked * route_weights[:, :, None], axis=1)
    return (middle + moe_sum).astype(jnp.bfloat16)


def solution(mesh):
    return jax.shard_map(
        shards,
        mesh=mesh,
        in_specs=(
            P("sp", "tp"),
            P("sp", None),
            P("sp", None),
            P(),
            P(None, "tp"),
            P(None, "tp"),
            P(),
            P(),
            P(),
            P(),
            P(("sp", "tp"), None),
            P(),
            P(("sp", "tp"), None),
            P(("sp", "tp"), None),
            P("sp", None, "tp"),
            P("sp", None, "tp"),
            P("sp", "tp", None),
        ),
        out_specs=P(("sp", "tp"), None),
        check_vma=False,
    )
```

```python
import jax
import jax.numpy as jnp
from jax import lax
from jax.experimental import pallas as pl
from jax.experimental.pallas import tpu as pltpu
from jax.sharding import PartitionSpec as P

D = 2048
NOPE = 64
ROPE = 32
VH = 64
TOPK = 2
QK = 96


epsilon = 1e-06
rope_base = 10000.0


def rms_scale(values):
    return lax.rsqrt(jnp.mean(values * values, axis=-1, keepdims=True) + epsilon)


def rotate_half(values, angles):
    half_dims = values.shape[-1] // 2
    first_half = values[..., :half_dims]
    second_half = values[..., half_dims:]
    cosine = jnp.cos(angles)
    sine_val = jnp.sin(angles)
    return jnp.concatenate(
        [
            first_half * cosine - second_half * sine_val,
            second_half * cosine + first_half * sine_val,
        ],
        axis=-1,
    )


def head_prepare(raw_rows, gain_vec, angles):
    normed_rows = raw_rows * rms_scale(raw_rows) * gain_vec
    turned_rows = rotate_half(normed_rows[..., NOPE:], angles[:, None, :])
    return jnp.concatenate([normed_rows[..., :NOPE], turned_rows], axis=-1).astype(jnp.bfloat16)


def slot_targets(route_rows, expert_total, slot_cap):
    flat_routes = route_rows.reshape(-1)
    one_hot = (flat_routes[:, None] == jnp.arange(expert_total, dtype=jnp.int32)[None, :]).astype(
        jnp.int32
    )
    earlier = jnp.cumsum(one_hot, axis=0) - one_hot
    rank_in = jnp.sum(earlier * one_hot, axis=1)
    return (flat_routes * slot_cap + rank_in).reshape(route_rows.shape)


def select_matrix(targets, slot_total):
    hits = targets[:, :, None] == jnp.arange(slot_total, dtype=jnp.int32)[None, None, :]
    return jnp.sum(hits.astype(jnp.bfloat16), axis=1)


SCORE_EXP = 1.4426950408889634 * QK ** (-0.5)
Q_TILE = 256
SIDE = 4
VISITS = (
    (0, 0), (1, 0), (3, 0), (0, 1), (0, 3), (1, 1), (1, 3), (3, 1),
    (3, 3), (2, 0), (0, 2), (2, 1), (2, 3), (1, 2), (3, 2), (2, 2),
)


def attention(query_rows, bundle):
    shard_len = query_rows.shape[0]
    half = shard_len // 2
    block_count = lax.axis_size("sp")
    tp_count = lax.axis_size("tp")
    tok = shard_len // tp_count
    bundle_rows = bundle.shape[0]
    part_rows = bundle_rows // 2

    def kernel(
        q_ref, own_ref, out_ref,
        kv_ref, pair_ref, peak_ref, acc_ref, val_ref, done_ref, tok_ref,
        kv_send, kv_recv, q_send, q_recv, out_send, out_recv,
    ):
        mine = lax.axis_index("sp")
        head = lax.axis_index("tp")
        mirror = block_count - 1 - mine
        low = jnp.minimum(mine, mirror)
        high = jnp.maximum(mine, mirror)
        shift = pl.multiple_of(jnp.where(mine < block_count // 2, 0, half), half)
        rest = pl.multiple_of(half - shift, half)
        row, col = mine // SIDE, mine % SIDE

        def block_at(dx, dy):
            return ((row + dy) % SIDE) * SIDE + (col + dx) % SIDE

        barrier = pltpu.get_barrier_semaphore()

        def greet(place, lane):
            pl.semaphore_signal(
                barrier,
                inc=1,
                device_id={"sp": place, "tp": lane},
                device_id_type=pl.DeviceIdType.MESH,
            )

        for dx, dy in ((1, 0), (3, 0), (0, 1), (0, 3)):
            greet(block_at(dx, dy), head)
        for other in range(tp_count):
            greet(mirror, other)

            @pl.when(other != head)
            def _():
                greet(mine, other)

        pl.semaphore_wait(barrier, 4 + 2 * tp_count - 1)

        def remote(source, target, send, recv, place, lane):
            return pltpu.make_async_remote_copy(
                src_ref=source,
                dst_ref=target,
                send_sem=send,
                recv_sem=recv,
                device_id={"sp": place, "tp": lane},
                device_id_type=pl.DeviceIdType.MESH,
            )

        def trade():
            return remote(q_ref.at[pl.ds(rest, half)], pair_ref.at[pl.ds(shift, half)],
                          q_send.at[0], q_recv.at[0], mirror, head)

        def traded():
            return remote(q_ref.at[pl.ds(rest, half)], pair_ref.at[pl.ds(rest, half)],
                          q_send.at[0], q_recv.at[0], mirror, head)

        def at(part, along, across):
            return (along, across) if part == 0 else (across, along)

        def piece(part, where, way, own=False, side=None):
            block = block_at(*where)
            rows = pl.ds(part * part_rows, part_rows)
            cols = slice(None) if side is None else pl.ds(side * half, half)
            index = (part * block_count + block) * 2
            source = own_ref.at[rows] if own else kv_ref.at[block, rows, cols]
            compass = ((1, 0), (3, 0), (0, 1), (0, 3)).index(way)
            return remote(source, kv_ref.at[block, rows, cols],
                          kv_send.at[index * 2 + compass],
                          kv_recv.at[index + (0 if side is None else side)],
                          block_at(*way), head)

        def landed(part, where, side=None):
            piece(part, where, (1, 0), side=side).wait_recv()

        sent = []

        def push(part, where, way, own=False, side=None):
            piece(part, where, way, own, side).start()
            sent.append((part, where, way, own, side))

        def spread(part, where):
            push(part, where, at(part, 0, 1))
            push(part, where, at(part, 0, 3))

        def neighbours_first():
            for part in (0, 1):
                for along, side, way in ((3, 0, 1), (1, 1, 3)):
                    landed(part, at(part, along, 0))
                    push(part, at(part, along, 0), at(part, way, 0), side=side)
                    spread(part, at(part, along, 0))

        def pass_across(alongs):
            for part in (0, 1):
                for along in alongs:
                    for across, side, way in ((3, 0, 1), (1, 1, 3)):
                        landed(part, at(part, along, across))
                        push(part, at(part, along, across), at(part, 0, way), side=side)

        def far_first():
            for part in (0, 1):
                landed(part, at(part, 2, 0), 0)
                landed(part, at(part, 2, 0), 1)
                spread(part, at(part, 2, 0))

        def far_across(alongs):
            for part in (0, 1):
                for along in alongs:
                    landed(part, at(part, along, 2), 0)
                    landed(part, at(part, along, 2), 1)

        trade().start()
        for part in (0, 1):
            push(part, (0, 0), at(part, 1, 0), own=True)
            push(part, (0, 0), at(part, 3, 0), own=True)
        for part in (0, 1):
            push(part, (0, 0), at(part, 0, 1), own=True)
            push(part, (0, 0), at(part, 0, 3), own=True)
        kv_ref[mine] = own_ref[...]
        pair_ref[pl.ds(shift, half), :] = q_ref[pl.ds(shift, half), :]
        peak_ref[...] = jnp.full_like(peak_ref, -1e30)
        acc_ref[...] = jnp.zeros_like(acc_ref)
        lane = lax.broadcasted_iota(jnp.int32, (shard_len, 128), 1)
        val_ref[...] = jnp.where(lane == VH, 1.0, 0.0).astype(jnp.bfloat16)

        def attend(block, parts):
            keys = kv_ref[block, :QK, :]
            val_ref[:, :VH] = kv_ref[block, QK:, :].T
            values = val_ref[...]
            for start, masked in parts:
                for first in range(start, start + half, Q_TILE):
                    rows = pl.ds(first, Q_TILE)
                    scores = jnp.dot(pair_ref[rows, :], keys, preferred_element_type=jnp.float32)
                    if masked:
                        q_pos = lax.broadcasted_iota(jnp.int32, scores.shape, 0)
                        k_pos = lax.broadcasted_iota(jnp.int32, scores.shape, 1)
                        scores = jnp.where(
                            k_pos - q_pos <= shift + (first - start), scores, -1e30
                        )
                    old = peak_ref[rows, :]
                    new = jnp.maximum(old, jnp.max(scores, axis=1, keepdims=True))
                    weights = jnp.exp2((scores - new[:, :1]) * SCORE_EXP).astype(jnp.bfloat16)
                    factor = jnp.exp2((old - new) * SCORE_EXP)
                    peak_ref[rows, :] = new
                    acc_ref[rows, :] = acc_ref[rows, :] * factor + jnp.dot(
                        weights, values, preferred_element_type=jnp.float32
                    )

        def visit(step, _):
            @pl.when(step == 0)
            def _():
                neighbours_first()
                traded().wait_recv()

            @pl.when(step == 1)
            def _():
                pass_across((0,))

            @pl.when(step == 2)
            def _():
                far_first()

            @pl.when(step == 5)
            def _():
                pass_across((1, 3))

            @pl.when(step == 9)
            def _():
                far_across((0,))
                pass_across((2,))

            @pl.when(step == 11)
            def _():
                far_across((1, 3))

            @pl.when(step == 15)
            def _():
                far_across((2,))

            dx = sum(jnp.where(step == k, v[0], 0) for k, v in enumerate(VISITS) if v[0])
            dy = sum(jnp.where(step == k, v[1], 0) for k, v in enumerate(VISITS) if v[1])
            block = block_at(dx, dy)

            @pl.when(block < low)
            def _():
                attend(block, ((0, False), (half, False)))

            @pl.when(block == low)
            def _():
                attend(block, ((0, True), (half, False)))

            @pl.when((block > low) & (block < high))
            def _():
                attend(block, ((half, False),))

            @pl.when(block == high)
            def _():
                attend(block, ((half, True),))

        lax.fori_loop(0, block_count, visit, None)
        done_ref[...] = (acc_ref[:, :VH] / acc_ref[:, VH : VH + 1]).astype(jnp.bfloat16)

        first_lane = shift // tok

        def result(index):
            side, order = index // (tp_count // 2), index % (tp_count // 2)
            own_side = jnp.where(side == 0, shift, rest)
            start = pl.multiple_of(own_side + order * tok, tok)
            return remote(done_ref.at[pl.ds(start, tok)], tok_ref.at[head],
                          out_send.at[index], out_recv.at[head],
                          jnp.where(side == 0, mine, mirror), first_lane + order)

        here = (head >= first_lane) & (head < first_lane + tp_count // 2)
        self_index = jnp.where(here, head - first_lane, tp_count)

        def send_result(index, _):
            @pl.when(index != self_index)
            def _():
                result(index).start()

        lax.fori_loop(0, tp_count, send_result, None)

        @pl.when(here)
        def _():
            tok_ref[head] = done_ref[pl.ds(pl.multiple_of(head * tok, tok), tok), :]

        def take_result(index, _):
            @pl.when(jnp.logical_not(here & (index == head)))
            def _():
                remote(done_ref.at[pl.ds(0, tok)], tok_ref.at[index],
                       out_send.at[index], out_recv.at[index], mirror, head).wait_recv()

        lax.fori_loop(0, tp_count, take_result, None)
        out_ref[...] = tok_ref[...]

        trade().wait_send()
        for message in sent:
            piece(*message).wait_send()

        def drain(index, _):
            @pl.when(index != self_index)
            def _():
                result(index).wait_send()

        lax.fori_loop(0, tp_count, drain, None)

    return pl.pallas_call(
        kernel,
        out_shape=jax.ShapeDtypeStruct((tp_count, tok, VH), jnp.bfloat16),
        in_specs=[pl.BlockSpec(memory_space=pltpu.VMEM)] * 2,
        out_specs=pl.BlockSpec(memory_space=pltpu.VMEM),
        scratch_shapes=[
            pltpu.VMEM((block_count, bundle_rows, shard_len), jnp.bfloat16),
            pltpu.VMEM((shard_len, QK), jnp.bfloat16),
            pltpu.VMEM((shard_len, 128), jnp.float32),
            pltpu.VMEM((shard_len, 128), jnp.float32),
            pltpu.VMEM((shard_len, 128), jnp.bfloat16),
            pltpu.VMEM((shard_len, VH), jnp.bfloat16),
            pltpu.VMEM((tp_count, tok, VH), jnp.bfloat16),
            pltpu.SemaphoreType.DMA((block_count * 8,)),
            pltpu.SemaphoreType.DMA((block_count * 4,)),
            pltpu.SemaphoreType.DMA((1,)),
            pltpu.SemaphoreType.DMA((1,)),
            pltpu.SemaphoreType.DMA((tp_count,)),
            pltpu.SemaphoreType.DMA((tp_count,)),
        ],
        compiler_params=pltpu.CompilerParams(
            collective_id=4, has_side_effects=True, vmem_limit_bytes=40 * 1024 * 1024
        ),
    )(query_rows, bundle)


ROW_CUT = 80


def expert_ring(rows, gate, up, down):
    count, width = rows.shape
    hidden = gate.shape[1]
    chips = lax.axis_size("tp") // 2
    both = 2 * count

    def kernel(
        x_ref, gate_ref, up_ref, down_ref, out_ref,
        both_ref, seen, own_part, far_part, near_part, run_in, run_out,
        fwd_send, fwd_recv, back_send, back_recv, twin_send, twin_recv,
        part_send, part_recv, sum_fwd_send, sum_fwd_recv, sum_back_send, sum_back_recv,
    ):
        place = lax.axis_index("tp")
        chip, core = place // 2, place % 2
        toward = jnp.where(core == 0, 1, chips - 1)
        ahead = ((chip + toward) % chips) * 2 + core
        behind = ((chip + chips - toward) % chips) * 2 + core
        twin = chip * 2 + 1 - core

        barrier = pltpu.get_barrier_semaphore()
        for other in (ahead, behind, twin):
            pl.semaphore_signal(
                barrier, inc=1, device_id={"tp": other}, device_id_type=pl.DeviceIdType.MESH
            )
        pl.semaphore_wait(barrier, 3)

        def remote(source, target, send, recv, other):
            return pltpu.make_async_remote_copy(
                src_ref=source,
                dst_ref=target,
                send_sem=send,
                recv_sem=recv,
                device_id={"tp": other},
                device_id_type=pl.DeviceIdType.MESH,
            )

        first, second = pl.ds(0, ROW_CUT), pl.ds(ROW_CUT, count - ROW_CUT)
        front, rear = pl.ds(0, count), pl.ds(count, count)

        def forward(step):
            return (
                remote(seen.at[step, first], seen.at[step + 1, first],
                       fwd_send.at[step], fwd_recv.at[step + 1], ahead),
                remote(seen.at[step, second], seen.at[step + 1, second],
                       back_send.at[step], back_recv.at[step + 1], behind),
            )

        def forward_own():
            return (
                remote(x_ref.at[first], seen.at[1, first], fwd_send.at[0], fwd_recv.at[1], ahead),
                remote(x_ref.at[second], seen.at[1, second],
                       back_send.at[0], back_recv.at[1], behind),
            )

        def share(step):
            return remote(seen.at[step, front], seen.at[step, rear],
                          twin_send.at[step], twin_recv.at[step], twin)

        def share_own():
            return remote(x_ref, seen.at[0, rear], twin_send.at[0], twin_recv.at[0], twin)

        def hand_over(step):
            return remote(far_part.at[step], near_part.at[step],
                          part_send.at[step], part_recv.at[step], twin)

        def pass_sum(step):
            return (
                remote(run_out.at[step, first], run_in.at[step + 1, first],
                       sum_fwd_send.at[step], sum_fwd_recv.at[step + 1], ahead),
                remote(run_out.at[step, second], run_in.at[step + 1, second],
                       sum_back_send.at[step], sum_back_recv.at[step + 1], behind),
            )

        def experts(step):
            tokens = seen[step]
            pre = jnp.dot(tokens, both_ref[...], preferred_element_type=jnp.float32)
            inner = (jax.nn.silu(pre[:, :hidden]) * pre[:, hidden:]).astype(jnp.bfloat16)
            part = jnp.dot(inner, down_ref[...], preferred_element_type=jnp.float32).astype(
                jnp.bfloat16
            )
            own_part[step] = part[:count]
            far_part[step] = part[count:]

        for copy in (*forward_own(), share_own()):
            copy.start()
        both_ref[:, :hidden] = gate_ref[...]
        both_ref[:, hidden:] = up_ref[...]
        seen[0, front, :] = x_ref[...]
        share_own().wait_recv()
        experts(0)
        hand_over(0).start()

        def step_of(step, _):
            arrived = forward(step - 1)
            arrived[0].wait_recv()
            arrived[1].wait_recv()

            @pl.when(step < chips - 1)
            def _():
                for copy in forward(step):
                    copy.start()

            share(step).start()
            share(step).wait_recv()
            experts(step)
            hand_over(step).start()
            hand_over(step).wait_recv()

            @pl.when(step > 1)
            def _():
                for copy in pass_sum(step - 1):
                    copy.wait_recv()
                run_out[step] = (
                    run_in[step].astype(jnp.float32)
                    + own_part[step].astype(jnp.float32)
                    + near_part[step].astype(jnp.float32)
                ).astype(jnp.bfloat16)

            @pl.when(step == 1)
            def _():
                run_out[step] = (
                    own_part[step].astype(jnp.float32) + near_part[step].astype(jnp.float32)
                ).astype(jnp.bfloat16)

            for copy in pass_sum(step):
                copy.start()

        lax.fori_loop(1, chips, step_of, None)
        hand_over(0).wait_recv()
        for copy in pass_sum(chips - 1):
            copy.wait_recv()
        out_ref[...] = (
            run_in[chips].astype(jnp.float32)
            + own_part[0].astype(jnp.float32)
            + near_part[0].astype(jnp.float32)
        ).astype(jnp.bfloat16)

        for copy in (*forward_own(), share_own(), hand_over(0)):
            copy.wait_send()

        def drain(step, _):
            @pl.when(step < chips - 1)
            def _():
                for copy in forward(step):
                    copy.wait_send()

            share(step).wait_send()
            hand_over(step).wait_send()
            for copy in pass_sum(step):
                copy.wait_send()

        lax.fori_loop(1, chips, drain, None)

    block = (count, width)
    sems = [pltpu.SemaphoreType.DMA((chips + 1,)) for _ in range(12)]
    return pl.pallas_call(
        kernel,
        out_shape=jax.ShapeDtypeStruct(block, jnp.bfloat16),
        in_specs=[pl.BlockSpec(memory_space=pltpu.VMEM)] * 4,
        out_specs=pl.BlockSpec(memory_space=pltpu.VMEM),
        scratch_shapes=[
            pltpu.VMEM((width, 2 * hidden), jnp.bfloat16),
            pltpu.VMEM((chips, both, width), jnp.bfloat16),
            pltpu.VMEM((chips, *block), jnp.bfloat16),
            pltpu.VMEM((chips, *block), jnp.bfloat16),
            pltpu.VMEM((chips, *block), jnp.bfloat16),
            pltpu.VMEM((chips + 1, *block), jnp.bfloat16),
            pltpu.VMEM((chips, *block), jnp.bfloat16),
            *sems,
        ],
        compiler_params=pltpu.CompilerParams(
            collective_id=3, has_side_effects=True, vmem_limit_bytes=50 * 1024 * 1024
        ),
    )(rows, gate, up, down)


def shards(
    queries,
    latent,
    rot_key,
    latent_gain,
    key_up,
    value_up,
    query_gain,
    key_gain,
    out_gain,
    out_weight,
    residual,
    ffn_gain,
    routes,
    route_weights,
    expert_gate,
    expert_up,
    expert_down,
):
    shard_len = queries.shape[0]
    local_heads = key_up.shape[1] // NOPE
    sp_count = lax.axis_size("sp")
    tp_count = lax.axis_size("tp")
    my_first = lax.axis_index("sp") * shard_len
    positions = my_first + jnp.arange(shard_len, dtype=jnp.int32)
    inverse = rope_base ** (-jnp.arange(0, ROPE, 2, dtype=jnp.float32) / ROPE)
    angles = positions.astype(jnp.float32)[:, None] * inverse[None, :]
    lat_f32 = latent.astype(jnp.float32)
    normed_latent = (lat_f32 * rms_scale(lat_f32) * latent_gain).astype(jnp.bfloat16)
    key_nope = jnp.dot(normed_latent, key_up, preferred_element_type=jnp.float32).astype(
        jnp.bfloat16
    )
    value_rows = jnp.dot(normed_latent, value_up, preferred_element_type=jnp.float32).astype(
        jnp.bfloat16
    )
    shared = rot_key.astype(jnp.float32)[:, None, :]
    raw_keys = jnp.concatenate(
        [key_nope.astype(jnp.float32).reshape(shard_len, local_heads, NOPE), shared], axis=-1
    )
    key_rows = head_prepare(raw_keys, key_gain, angles)
    query_rows = head_prepare(
        queries.astype(jnp.float32).reshape(shard_len, local_heads, QK), query_gain, angles
    )
    bundle = jnp.concatenate([key_rows.reshape(shard_len, QK).T, value_rows.T], axis=0)
    tok_count = residual.shape[0]
    by_head = attention(query_rows.reshape(shard_len, QK), bundle)
    token_rows = jnp.transpose(by_head, (1, 0, 2)).reshape(tok_count, -1).astype(jnp.float32)
    normed_rows = (token_rows * rms_scale(token_rows) * out_gain).astype(jnp.bfloat16)
    partials = jnp.einsum(
        "tgc,gcd->tgd",
        normed_rows.reshape(tok_count, tp_count, -1),
        out_weight.reshape(tp_count, -1, D),
        preferred_element_type=jnp.float32,
    )
    rounded = lax.optimization_barrier(partials.astype(jnp.bfloat16))
    mixed = jnp.sum(rounded.astype(jnp.float32), axis=1)
    middle = residual.astype(jnp.float32) + mixed
    ffn_input = (middle * rms_scale(middle) * ffn_gain).astype(jnp.bfloat16)
    slot_cap = max(2, 9 * tok_count * TOPK // (8 * sp_count))
    slot_total = sp_count * slot_cap
    targets = slot_targets(routes, sp_count, slot_cap)
    chooser = select_matrix(targets, slot_total)
    outbound = (
        jnp.einsum("ts,td->sd", chooser, ffn_input, preferred_element_type=jnp.float32)
        .astype(jnp.bfloat16)
        .reshape(sp_count, slot_cap, D)
    )
    arrived = lax.all_to_all(outbound, "sp", split_axis=0, concat_axis=0, tiled=True)
    item_count = arrived.shape[1]
    flat_rows = arrived.reshape(sp_count * item_count, D)
    served = expert_ring(flat_rows, expert_gate[0], expert_up[0], expert_down[0]).reshape(
        sp_count, item_count, D
    )
    returned_rows = lax.all_to_all(served, "sp", split_axis=0, concat_axis=0, tiled=True).reshape(
        slot_total, D
    )
    picked = (
        jnp.take(returned_rows, targets.reshape(-1), axis=0)
        .reshape(tok_count, TOPK, D)
        .astype(jnp.float32)
    )
    moe_sum = jnp.sum(picked * route_weights[:, :, None], axis=1)
    return (middle + moe_sum).astype(jnp.bfloat16)


def solution(mesh):
    return jax.shard_map(
        shards,
        mesh=mesh,
        in_specs=(
            P("sp", "tp"),
            P("sp", None),
            P("sp", None),
            P(),
            P(None, "tp"),
            P(None, "tp"),
            P(),
            P(),
            P(),
            P(),
            P(("sp", "tp"), None),
            P(),
            P(("sp", "tp"), None),
            P(("sp", "tp"), None),
            P("sp", None, "tp"),
            P("sp", None, "tp"),
            P("sp", "tp", None),
        ),
        out_specs=P(("sp", "tp"), None),
        check_vma=False,
    )
```

```python
import jax
import jax.numpy as jnp
from jax import lax
from jax.experimental import pallas as pl
from jax.experimental.pallas import tpu as pltpu
from jax.sharding import PartitionSpec as P

D = 2048
NOPE = 64
ROPE = 32
VH = 64
TOPK = 2
QK = 96


epsilon = 1e-06
rope_base = 10000.0


def rms_scale(values):
    return lax.rsqrt(jnp.mean(values * values, axis=-1, keepdims=True) + epsilon)


def rotate_half(values, angles):
    half_dims = values.shape[-1] // 2
    first_half = values[..., :half_dims]
    second_half = values[..., half_dims:]
    cosine = jnp.cos(angles)
    sine_val = jnp.sin(angles)
    return jnp.concatenate(
        [
            first_half * cosine - second_half * sine_val,
            second_half * cosine + first_half * sine_val,
        ],
        axis=-1,
    )


def head_prepare(raw_rows, gain_vec, angles):
    normed_rows = raw_rows * rms_scale(raw_rows) * gain_vec
    turned_rows = rotate_half(normed_rows[..., NOPE:], angles[:, None, :])
    return jnp.concatenate([normed_rows[..., :NOPE], turned_rows], axis=-1).astype(jnp.bfloat16)


def slot_targets(route_rows, expert_total, slot_cap):
    flat_routes = route_rows.reshape(-1)
    one_hot = (flat_routes[:, None] == jnp.arange(expert_total, dtype=jnp.int32)[None, :]).astype(
        jnp.int32
    )
    earlier = jnp.cumsum(one_hot, axis=0) - one_hot
    rank_in = jnp.sum(earlier * one_hot, axis=1)
    return (flat_routes * slot_cap + rank_in).reshape(route_rows.shape)


SCORE_EXP = 1.4426950408889634 * QK ** (-0.5)
Q_TILE = 256
SIDE = 4
VISITS = (
    (0, 0), (1, 0), (3, 0), (0, 1), (0, 3), (1, 1), (1, 3), (3, 1),
    (3, 3), (2, 0), (0, 2), (2, 1), (2, 3), (1, 2), (3, 2), (2, 2),
)


def attention(query_rows, bundle):
    shard_len = query_rows.shape[0]
    half = shard_len // 2
    block_count = lax.axis_size("sp")
    tp_count = lax.axis_size("tp")
    tok = shard_len // tp_count
    bundle_rows = bundle.shape[0]
    part_rows = bundle_rows // 2

    def kernel(
        q_ref, own_ref, out_ref,
        kv_ref, pair_ref, peak_ref, acc_ref, val_ref, done_ref, tok_ref,
        kv_send, kv_recv, q_send, q_recv, out_send, out_recv,
    ):
        mine = lax.axis_index("sp")
        head = lax.axis_index("tp")
        mirror = block_count - 1 - mine
        low = jnp.minimum(mine, mirror)
        high = jnp.maximum(mine, mirror)
        shift = pl.multiple_of(jnp.where(mine < block_count // 2, 0, half), half)
        rest = pl.multiple_of(half - shift, half)
        row, col = mine // SIDE, mine % SIDE

        def block_at(dx, dy):
            return ((row + dy) % SIDE) * SIDE + (col + dx) % SIDE

        barrier = pltpu.get_barrier_semaphore()

        def greet(place, lane):
            pl.semaphore_signal(
                barrier,
                inc=1,
                device_id={"sp": place, "tp": lane},
                device_id_type=pl.DeviceIdType.MESH,
            )

        for dx, dy in ((1, 0), (3, 0), (0, 1), (0, 3)):
            greet(block_at(dx, dy), head)
        for other in range(tp_count):
            greet(mirror, other)

            @pl.when(other != head)
            def _():
                greet(mine, other)

        pl.semaphore_wait(barrier, 4 + 2 * tp_count - 1)

        def remote(source, target, send, recv, place, lane):
            return pltpu.make_async_remote_copy(
                src_ref=source,
                dst_ref=target,
                send_sem=send,
                recv_sem=recv,
                device_id={"sp": place, "tp": lane},
                device_id_type=pl.DeviceIdType.MESH,
            )

        def trade():
            return remote(q_ref.at[pl.ds(rest, half)], pair_ref.at[pl.ds(shift, half)],
                          q_send.at[0], q_recv.at[0], mirror, head)

        def traded():
            return remote(q_ref.at[pl.ds(rest, half)], pair_ref.at[pl.ds(rest, half)],
                          q_send.at[0], q_recv.at[0], mirror, head)

        def at(part, along, across):
            return (along, across) if part == 0 else (across, along)

        def piece(part, where, way, own=False, side=None):
            block = block_at(*where)
            rows = pl.ds(part * part_rows, part_rows)
            cols = slice(None) if side is None else pl.ds(side * half, half)
            index = (part * block_count + block) * 2
            source = own_ref.at[rows] if own else kv_ref.at[block, rows, cols]
            compass = ((1, 0), (3, 0), (0, 1), (0, 3)).index(way)
            return remote(source, kv_ref.at[block, rows, cols],
                          kv_send.at[index * 2 + compass],
                          kv_recv.at[index + (0 if side is None else side)],
                          block_at(*way), head)

        def landed(part, where, side=None):
            piece(part, where, (1, 0), side=side).wait_recv()

        sent = []

        def push(part, where, way, own=False, side=None):
            piece(part, where, way, own, side).start()
            sent.append((part, where, way, own, side))

        def spread(part, where):
            push(part, where, at(part, 0, 1))
            push(part, where, at(part, 0, 3))

        def neighbours_first():
            for part in (0, 1):
                for along, side, way in ((3, 0, 1), (1, 1, 3)):
                    landed(part, at(part, along, 0))
                    push(part, at(part, along, 0), at(part, way, 0), side=side)
                    spread(part, at(part, along, 0))

        def pass_across(alongs):
            for part in (0, 1):
                for along in alongs:
                    for across, side, way in ((3, 0, 1), (1, 1, 3)):
                        landed(part, at(part, along, across))
                        push(part, at(part, along, across), at(part, 0, way), side=side)

        def far_first():
            for part in (0, 1):
                landed(part, at(part, 2, 0), 0)
                landed(part, at(part, 2, 0), 1)
                spread(part, at(part, 2, 0))

        def far_across(alongs):
            for part in (0, 1):
                for along in alongs:
                    landed(part, at(part, along, 2), 0)
                    landed(part, at(part, along, 2), 1)

        trade().start()
        for part in (0, 1):
            push(part, (0, 0), at(part, 1, 0), own=True)
            push(part, (0, 0), at(part, 3, 0), own=True)
        for part in (0, 1):
            push(part, (0, 0), at(part, 0, 1), own=True)
            push(part, (0, 0), at(part, 0, 3), own=True)
        kv_ref[mine] = own_ref[...]
        pair_ref[pl.ds(shift, half), :] = q_ref[pl.ds(shift, half), :]
        peak_ref[...] = jnp.full_like(peak_ref, -1e30)
        acc_ref[...] = jnp.zeros_like(acc_ref)
        lane = lax.broadcasted_iota(jnp.int32, (shard_len, 128), 1)
        val_ref[...] = jnp.where(lane == VH, 1.0, 0.0).astype(jnp.bfloat16)

        def attend(block, parts):
            keys = kv_ref[block, :QK, :]
            val_ref[:, :VH] = kv_ref[block, QK:, :].T
            values = val_ref[...]
            for start, masked in parts:
                for first in range(start, start + half, Q_TILE):
                    rows = pl.ds(first, Q_TILE)
                    scores = jnp.dot(
                        pair_ref[rows, :QK], keys, preferred_element_type=jnp.float32
                    )
                    if masked:
                        q_pos = lax.broadcasted_iota(jnp.int32, scores.shape, 0)
                        k_pos = lax.broadcasted_iota(jnp.int32, scores.shape, 1)
                        scores = jnp.where(
                            k_pos - q_pos <= shift + (first - start), scores, -1e30
                        )
                    old = peak_ref[rows, :]
                    new = jnp.maximum(old, jnp.max(scores, axis=1, keepdims=True))
                    weights = jnp.exp2((scores - new[:, :1]) * SCORE_EXP).astype(jnp.bfloat16)
                    factor = jnp.exp2((old - new) * SCORE_EXP)
                    peak_ref[rows, :] = new
                    acc_ref[rows, :] = acc_ref[rows, :] * factor + jnp.dot(
                        weights, values, preferred_element_type=jnp.float32
                    )

        def visit(step, _):
            @pl.when(step == 0)
            def _():
                neighbours_first()
                traded().wait_recv()

            @pl.when(step == 1)
            def _():
                pass_across((0,))

            @pl.when(step == 2)
            def _():
                far_first()

            @pl.when(step == 5)
            def _():
                pass_across((1, 3))

            @pl.when(step == 9)
            def _():
                far_across((0,))
                pass_across((2,))

            @pl.when(step == 11)
            def _():
                far_across((1, 3))

            @pl.when(step == 15)
            def _():
                far_across((2,))

            dx = sum(jnp.where(step == k, v[0], 0) for k, v in enumerate(VISITS) if v[0])
            dy = sum(jnp.where(step == k, v[1], 0) for k, v in enumerate(VISITS) if v[1])
            block = block_at(dx, dy)

            @pl.when(block < low)
            def _():
                attend(block, ((0, False), (half, False)))

            @pl.when(block == low)
            def _():
                attend(block, ((0, True), (half, False)))

            @pl.when((block > low) & (block < high))
            def _():
                attend(block, ((half, False),))

            @pl.when(block == high)
            def _():
                attend(block, ((half, True),))

        lax.fori_loop(0, block_count, visit, None)
        done_ref[...] = (acc_ref[...] / acc_ref[:, VH : VH + 1]).astype(jnp.bfloat16)

        first_lane = shift // tok

        def result(index):
            side, order = index // (tp_count // 2), index % (tp_count // 2)
            own_side = jnp.where(side == 0, shift, rest)
            start = pl.multiple_of(own_side + order * tok, tok)
            return remote(done_ref.at[pl.ds(start, tok)], tok_ref.at[head],
                          out_send.at[index], out_recv.at[head],
                          jnp.where(side == 0, mine, mirror), first_lane + order)

        here = (head >= first_lane) & (head < first_lane + tp_count // 2)
        self_index = jnp.where(here, head - first_lane, tp_count)

        def send_result(index, _):
            @pl.when(index != self_index)
            def _():
                result(index).start()

        lax.fori_loop(0, tp_count, send_result, None)

        @pl.when(here)
        def _():
            tok_ref[head] = done_ref[pl.ds(pl.multiple_of(head * tok, tok), tok), :]

        def take_result(index, _):
            @pl.when(jnp.logical_not(here & (index == head)))
            def _():
                remote(done_ref.at[pl.ds(0, tok)], tok_ref.at[index],
                       out_send.at[index], out_recv.at[index], mirror, head).wait_recv()

        lax.fori_loop(0, tp_count, take_result, None)
        out_ref[...] = tok_ref[:, :, :VH]

        trade().wait_send()
        for message in sent:
            piece(*message).wait_send()

        def drain(index, _):
            @pl.when(index != self_index)
            def _():
                result(index).wait_send()

        lax.fori_loop(0, tp_count, drain, None)

    return pl.pallas_call(
        kernel,
        out_shape=jax.ShapeDtypeStruct((tp_count, tok, VH), jnp.bfloat16),
        in_specs=[pl.BlockSpec(memory_space=pltpu.VMEM)] * 2,
        out_specs=pl.BlockSpec(memory_space=pltpu.VMEM),
        scratch_shapes=[
            pltpu.VMEM((block_count, bundle_rows, shard_len), jnp.bfloat16),
            pltpu.VMEM((shard_len, 128), jnp.bfloat16),
            pltpu.VMEM((shard_len, 128), jnp.float32),
            pltpu.VMEM((shard_len, 128), jnp.float32),
            pltpu.VMEM((shard_len, 128), jnp.bfloat16),
            pltpu.VMEM((shard_len, 128), jnp.bfloat16),
            pltpu.VMEM((tp_count, tok, 128), jnp.bfloat16),
            pltpu.SemaphoreType.DMA((block_count * 8,)),
            pltpu.SemaphoreType.DMA((block_count * 4,)),
            pltpu.SemaphoreType.DMA((1,)),
            pltpu.SemaphoreType.DMA((1,)),
            pltpu.SemaphoreType.DMA((tp_count,)),
            pltpu.SemaphoreType.DMA((tp_count,)),
        ],
        compiler_params=pltpu.CompilerParams(
            collective_id=4, has_side_effects=True, vmem_limit_bytes=40 * 1024 * 1024
        ),
    )(query_rows, bundle)


ROW_CUT = 80


def expert_ring(chooser, ffn_input, gate, up, down, near_weights, middle):
    count = chooser.shape[0]
    width = ffn_input.shape[1]
    places = lax.axis_size("sp")
    slots = count // places
    chunks = width // 128
    slab = slots * chunks
    hidden = gate.shape[1]
    chips = lax.axis_size("tp") // 2
    both = 2 * count

    def kernel(
        choose_ref, token_ref, gate_ref, up_ref, down_hbm, mix_ref, middle_ref, out_ref,
        wide_ref, load_sem, away_ref, got_ref, home_ref, back_ref, ret_ref, x_ref,
        away_send, away_recv, home_send, home_recv,
        both_ref, down_ref, seen, own_part, far_part, near_part, run_in, run_out,
        fwd_send, fwd_recv, back_send, back_recv, twin_send, twin_recv,
        part_send, part_recv, sum_fwd_send, sum_fwd_recv, sum_back_send, sum_back_recv,
    ):
        place = lax.axis_index("tp")
        chip, core = place // 2, place % 2
        toward = jnp.where(core == 0, 1, chips - 1)
        ahead = ((chip + toward) % chips) * 2 + core
        behind = ((chip + chips - toward) % chips) * 2 + core
        twin = chip * 2 + 1 - core

        barrier = pltpu.get_barrier_semaphore()
        for other in (ahead, behind, twin):
            pl.semaphore_signal(
                barrier, inc=1, device_id={"tp": other}, device_id_type=pl.DeviceIdType.MESH
            )
        mine = lax.axis_index("sp")

        def peer(turn):
            return (mine + turn) % places

        def greet(turn, _):
            pl.semaphore_signal(
                barrier, inc=1, device_id={"sp": peer(turn)}, device_id_type=pl.DeviceIdType.MESH
            )

        lax.fori_loop(1, places, greet, None)
        loads = (
            pltpu.make_async_copy(gate_ref, both_ref.at[:, pl.ds(0, hidden)], load_sem.at[0]),
            pltpu.make_async_copy(up_ref, both_ref.at[:, pl.ds(hidden, hidden)], load_sem.at[1]),
            pltpu.make_async_copy(down_hbm, down_ref, load_sem.at[2]),
        )
        for load in loads:
            load.start()
        chosen = jnp.dot(choose_ref[...], token_ref[...], preferred_element_type=jnp.float32)
        for chunk in range(chunks):
            wide_ref[pl.ds(chunk, count, stride=chunks), :] = chosen[
                :, chunk * 128 : (chunk + 1) * 128
            ]
        away_ref[...] = wide_ref[...].astype(jnp.bfloat16)
        pl.semaphore_wait(barrier, 3 + places - 1)

        def slab_of(place):
            return pl.ds(pl.multiple_of(place * slab, slab), slab)

        def swap(source, target, send, recv, turn):
            return pltpu.make_async_remote_copy(
                src_ref=source.at[slab_of(peer(turn))],
                dst_ref=target.at[slab_of(mine)],
                send_sem=send.at[turn],
                recv_sem=recv.at[turn],
                device_id={"sp": peer(turn)},
                device_id_type=pl.DeviceIdType.MESH,
            )

        def exchange(source, target, send, recv):
            def start(turn, _):
                swap(source, target, send, recv, turn).start()

            lax.fori_loop(1, places, start, None)
            target[slab_of(mine), :] = source[slab_of(mine), :]

            def finish(turn, _):
                swap(source, target, send, recv, turn).wait_recv()

            lax.fori_loop(1, places, finish, None)

        def narrow(target):
            for chunk in range(chunks):
                target[:, pl.ds(chunk * 128, 128)] = wide_ref[
                    pl.ds(chunk, count, stride=chunks), :
                ].astype(jnp.bfloat16)

        exchange(away_ref, got_ref, away_send, away_recv)
        wide_ref[...] = got_ref[...].astype(jnp.float32)
        narrow(x_ref)

        def remote(source, target, send, recv, other):
            return pltpu.make_async_remote_copy(
                src_ref=source,
                dst_ref=target,
                send_sem=send,
                recv_sem=recv,
                device_id={"tp": other},
                device_id_type=pl.DeviceIdType.MESH,
            )

        first, second = pl.ds(0, ROW_CUT), pl.ds(ROW_CUT, count - ROW_CUT)
        front, rear = pl.ds(0, count), pl.ds(count, count)

        def forward(step):
            return (
                remote(seen.at[step, first], seen.at[step + 1, first],
                       fwd_send.at[step], fwd_recv.at[step + 1], ahead),
                remote(seen.at[step, second], seen.at[step + 1, second],
                       back_send.at[step], back_recv.at[step + 1], behind),
            )

        def forward_own():
            return (
                remote(x_ref.at[first], seen.at[1, first], fwd_send.at[0], fwd_recv.at[1], ahead),
                remote(x_ref.at[second], seen.at[1, second],
                       back_send.at[0], back_recv.at[1], behind),
            )

        def share(step):
            return remote(seen.at[step, front], seen.at[step, rear],
                          twin_send.at[step], twin_recv.at[step], twin)

        def share_own():
            return remote(x_ref, seen.at[0, rear], twin_send.at[0], twin_recv.at[0], twin)

        def hand_over(step):
            return remote(far_part.at[step], near_part.at[step],
                          part_send.at[step], part_recv.at[step], twin)

        def pass_sum(step):
            return (
                remote(run_out.at[step, first], run_in.at[step + 1, first],
                       sum_fwd_send.at[step], sum_fwd_recv.at[step + 1], ahead),
                remote(run_out.at[step, second], run_in.at[step + 1, second],
                       sum_back_send.at[step], sum_back_recv.at[step + 1], behind),
            )

        def experts(step):
            tokens = seen[step]
            pre = jnp.dot(tokens, both_ref[...], preferred_element_type=jnp.float32)
            inner = (jax.nn.silu(pre[:, :hidden]) * pre[:, hidden:]).astype(jnp.bfloat16)
            part = jnp.dot(inner, down_ref[...], preferred_element_type=jnp.float32).astype(
                jnp.bfloat16
            )
            own_part[step] = part[:count]
            far_part[step] = part[count:]

        for copy in (*forward_own(), share_own()):
            copy.start()
        for load in loads:
            load.wait()
        seen[0, front, :] = x_ref[...]
        share_own().wait_recv()
        experts(0)
        hand_over(0).start()

        def step_of(step, _):
            arrived = forward(step - 1)
            arrived[0].wait_recv()
            arrived[1].wait_recv()

            @pl.when(step < chips - 1)
            def _():
                for copy in forward(step):
                    copy.start()

            share(step).start()
            share(step).wait_recv()
            experts(step)
            hand_over(step).start()
            hand_over(step).wait_recv()

            @pl.when(step > 1)
            def _():
                for copy in pass_sum(step - 1):
                    copy.wait_recv()
                run_out[step] = (
                    run_in[step].astype(jnp.float32)
                    + own_part[step].astype(jnp.float32)
                    + near_part[step].astype(jnp.float32)
                ).astype(jnp.bfloat16)

            @pl.when(step == 1)
            def _():
                run_out[step] = (
                    own_part[step].astype(jnp.float32) + near_part[step].astype(jnp.float32)
                ).astype(jnp.bfloat16)

            for copy in pass_sum(step):
                copy.start()

        lax.fori_loop(1, chips, step_of, None)
        hand_over(0).wait_recv()
        for copy in pass_sum(chips - 1):
            copy.wait_recv()
        served = (
            run_in[chips].astype(jnp.float32)
            + own_part[0].astype(jnp.float32)
            + near_part[0].astype(jnp.float32)
        )
        for chunk in range(chunks):
            wide_ref[pl.ds(chunk, count, stride=chunks), :] = served[
                :, chunk * 128 : (chunk + 1) * 128
            ]
        home_ref[...] = wide_ref[...].astype(jnp.bfloat16)
        exchange(home_ref, back_ref, home_send, home_recv)
        wide_ref[...] = back_ref[...].astype(jnp.float32)
        narrow(ret_ref)
        returned = ret_ref[...]
        out_ref[...] = (
            middle_ref[...]
            + jnp.dot(mix_ref[0], returned, preferred_element_type=jnp.float32)
            + jnp.dot(mix_ref[1], returned, preferred_element_type=jnp.float32)
            + jnp.dot(mix_ref[2], returned, preferred_element_type=jnp.float32)
        ).astype(jnp.bfloat16)

        def settle(turn, _):
            swap(away_ref, got_ref, away_send, away_recv, turn).wait_send()
            swap(home_ref, back_ref, home_send, home_recv, turn).wait_send()

        lax.fori_loop(1, places, settle, None)

        for copy in (*forward_own(), share_own(), hand_over(0)):
            copy.wait_send()

        def drain(step, _):
            @pl.when(step < chips - 1)
            def _():
                for copy in forward(step):
                    copy.wait_send()

            share(step).wait_send()
            hand_over(step).wait_send()
            for copy in pass_sum(step):
                copy.wait_send()

        lax.fori_loop(1, chips, drain, None)

    block = (count, width)
    sems = [pltpu.SemaphoreType.DMA((chips + 1,)) for _ in range(12)]
    return pl.pallas_call(
        kernel,
        out_shape=jax.ShapeDtypeStruct(middle.shape, jnp.bfloat16),
        in_specs=[pl.BlockSpec(memory_space=pltpu.VMEM)] * 2
        + [pl.BlockSpec(memory_space=pltpu.HBM)] * 3
        + [pl.BlockSpec(memory_space=pltpu.VMEM)] * 2,
        out_specs=pl.BlockSpec(memory_space=pltpu.VMEM),
        scratch_shapes=[
            pltpu.VMEM((count * chunks, 128), jnp.float32),
            pltpu.SemaphoreType.DMA((3,)),
            *[pltpu.VMEM((count * chunks, 128), jnp.bfloat16) for _ in range(4)],
            pltpu.VMEM(block, jnp.bfloat16),
            pltpu.VMEM(block, jnp.bfloat16),
            *[pltpu.SemaphoreType.DMA((places,)) for _ in range(4)],
            pltpu.VMEM((width, 2 * hidden), jnp.bfloat16),
            pltpu.VMEM((hidden, width), jnp.bfloat16),
            pltpu.VMEM((chips, both, width), jnp.bfloat16),
            pltpu.VMEM((chips, *block), jnp.bfloat16),
            pltpu.VMEM((chips, *block), jnp.bfloat16),
            pltpu.VMEM((chips, *block), jnp.bfloat16),
            pltpu.VMEM((chips + 1, *block), jnp.bfloat16),
            pltpu.VMEM((chips, *block), jnp.bfloat16),
            *sems,
        ],
        compiler_params=pltpu.CompilerParams(
            collective_id=3, has_side_effects=True, vmem_limit_bytes=50 * 1024 * 1024
        ),
    )(chooser, ffn_input, gate, up, down, near_weights, middle)


def shards(
    queries,
    latent,
    rot_key,
    latent_gain,
    key_up,
    value_up,
    query_gain,
    key_gain,
    out_gain,
    out_weight,
    residual,
    ffn_gain,
    routes,
    route_weights,
    expert_gate,
    expert_up,
    expert_down,
):
    shard_len = queries.shape[0]
    local_heads = key_up.shape[1] // NOPE
    sp_count = lax.axis_size("sp")
    my_first = lax.axis_index("sp") * shard_len
    positions = my_first + jnp.arange(shard_len, dtype=jnp.int32)
    inverse = rope_base ** (-jnp.arange(0, ROPE, 2, dtype=jnp.float32) / ROPE)
    angles = positions.astype(jnp.float32)[:, None] * inverse[None, :]
    lat_f32 = latent.astype(jnp.float32)
    normed_latent = (lat_f32 * rms_scale(lat_f32) * latent_gain).astype(jnp.bfloat16)
    key_nope = jnp.dot(normed_latent, key_up, preferred_element_type=jnp.float32).astype(
        jnp.bfloat16
    )
    value_rows = jnp.dot(normed_latent, value_up, preferred_element_type=jnp.float32).astype(
        jnp.bfloat16
    )
    shared = rot_key.astype(jnp.float32)[:, None, :]
    raw_keys = jnp.concatenate(
        [key_nope.astype(jnp.float32).reshape(shard_len, local_heads, NOPE), shared], axis=-1
    )
    key_rows = head_prepare(raw_keys, key_gain, angles)
    query_rows = head_prepare(
        queries.astype(jnp.float32).reshape(shard_len, local_heads, QK), query_gain, angles
    )
    bundle = jnp.concatenate([key_rows.reshape(shard_len, QK).T, value_rows.T], axis=0)
    tok_count = residual.shape[0]
    by_head = attention(jnp.pad(query_rows.reshape(shard_len, QK), ((0, 0), (0, 128 - QK))), bundle)
    token_rows = jnp.transpose(by_head, (1, 0, 2)).reshape(tok_count, -1).astype(jnp.float32)
    normed_rows = (token_rows * rms_scale(token_rows) * out_gain).astype(jnp.bfloat16)
    mixed = jnp.dot(normed_rows, out_weight, preferred_element_type=jnp.float32)
    middle = residual.astype(jnp.float32) + mixed
    ffn_input = (middle * rms_scale(middle) * ffn_gain).astype(jnp.bfloat16)
    slot_cap = max(2, 9 * tok_count * TOPK // (8 * sp_count))
    slot_total = sp_count * slot_cap
    targets = slot_targets(routes, sp_count, slot_cap)
    slot_ids = jnp.arange(slot_total, dtype=jnp.int32)
    hits = targets[:, :, None] == slot_ids[None, None, :]
    chooser = jnp.any(slot_ids[:, None, None] == targets[None, :, :], axis=2).astype(jnp.bfloat16)
    mix = jnp.sum(jnp.where(hits, route_weights[:, :, None], 0.0), axis=1)
    mix_high = lax.reduce_precision(mix, 8, 7)
    mix_mid = lax.reduce_precision(mix - mix_high, 8, 7)
    mix_low = mix - mix_high - mix_mid
    mix_parts = jnp.stack([mix_high, mix_mid, mix_low]).astype(jnp.bfloat16)
    return expert_ring(
        chooser, ffn_input, expert_gate[0], expert_up[0], expert_down[0], mix_parts, middle
    )


def solution(mesh):
    return jax.shard_map(
        shards,
        mesh=mesh,
        in_specs=(
            P("sp", "tp"),
            P("sp", None),
            P("sp", None),
            P(),
            P(None, "tp"),
            P(None, "tp"),
            P(),
            P(),
            P(),
            P(),
            P(("sp", "tp"), None),
            P(),
            P(("sp", "tp"), None),
            P(("sp", "tp"), None),
            P("sp", None, "tp"),
            P("sp", None, "tp"),
            P("sp", "tp", None),
        ),
        out_specs=P(("sp", "tp"), None),
        check_vma=False,
    )
```

```python
import jax
import jax.numpy as jnp
from jax import lax
from jax.experimental import pallas as pl
from jax.experimental.pallas import tpu as pltpu
from jax.sharding import PartitionSpec as P

D = 2048
NOPE = 64
ROPE = 32
VH = 64
TOPK = 2
QK = 96


epsilon = 1e-06
rope_base = 10000.0


def rms_scale(values):
    return lax.rsqrt(jnp.mean(values * values, axis=-1, keepdims=True) + epsilon)


def rotate_half(values, angles):
    half_dims = values.shape[-1] // 2
    first_half = values[..., :half_dims]
    second_half = values[..., half_dims:]
    cosine = jnp.cos(angles)
    sine_val = jnp.sin(angles)
    return jnp.concatenate(
        [
            first_half * cosine - second_half * sine_val,
            second_half * cosine + first_half * sine_val,
        ],
        axis=-1,
    )


def head_prepare(raw_rows, gain_vec, angles):
    normed_rows = raw_rows * rms_scale(raw_rows) * gain_vec
    turned_rows = rotate_half(normed_rows[..., NOPE:], angles[:, None, :])
    return jnp.concatenate([normed_rows[..., :NOPE], turned_rows], axis=-1).astype(jnp.bfloat16)


def slot_targets(route_rows, expert_total, slot_cap):
    flat_routes = route_rows.reshape(-1)
    one_hot = (flat_routes[:, None] == jnp.arange(expert_total, dtype=jnp.int32)[None, :]).astype(
        jnp.int32
    )
    earlier = jnp.cumsum(one_hot, axis=0) - one_hot
    rank_in = jnp.sum(earlier * one_hot, axis=1)
    return (flat_routes * slot_cap + rank_in).reshape(route_rows.shape)


SCORE_EXP = 1.4426950408889634 * QK ** (-0.5)
Q_TILE = 256
SIDE = 4
VISITS = (
    (0, 0), (1, 0), (3, 0), (0, 1), (0, 3), (1, 1), (1, 3), (3, 1),
    (3, 3), (2, 0), (0, 2), (2, 1), (2, 3), (1, 2), (3, 2), (2, 2),
)


def attention(query_rows, bundle, down):
    shard_len = query_rows.shape[0]
    half = shard_len // 2
    block_count = lax.axis_size("sp")
    tp_count = lax.axis_size("tp")
    tok = shard_len // tp_count
    chips = tp_count // 2
    pack = tok // 2
    groups = tp_count // 4
    hidden, width = down.shape
    share_rows = hidden // 2
    bundle_rows = bundle.shape[0]
    part_rows = bundle_rows // 2

    def kernel(
        q_ref, own_ref, down_ref, out_ref, all_ref,
        kv_ref, pair_ref, peak_ref, acc_ref, val_ref, done_ref, tok_ref,
        kv_send, kv_recv, q_send, q_recv, out_send, out_recv,
        w_send, w_recv, twin_send, twin_recv,
    ):
        mine = lax.axis_index("sp")
        head = lax.axis_index("tp")
        mirror = block_count - 1 - mine
        low = jnp.minimum(mine, mirror)
        high = jnp.maximum(mine, mirror)
        early = mine < block_count // 2
        shift = pl.multiple_of(jnp.where(early, 0, 2 * tok), 2 * tok)
        own_slot = pl.multiple_of(jnp.where(early, 0, half), half)
        far_slot = pl.multiple_of(half - own_slot, half)
        chip, core = head // 2, head % 2
        twin = chip * 2 + 1 - core
        row, col = mine // SIDE, mine % SIDE

        def block_at(dx, dy):
            return ((row + dy) % SIDE) * SIDE + (col + dx) % SIDE

        barrier = pltpu.get_barrier_semaphore()

        def greet(place, lane):
            pl.semaphore_signal(
                barrier,
                inc=1,
                device_id={"sp": place, "tp": lane},
                device_id_type=pl.DeviceIdType.MESH,
            )

        for dx, dy in ((1, 0), (3, 0), (0, 1), (0, 3)):
            greet(block_at(dx, dy), head)
        for other in range(tp_count):
            greet(mirror, other)

            @pl.when(other != head)
            def _():
                greet(mine, other)

        pl.semaphore_wait(barrier, 4 + 2 * tp_count - 1)

        def remote(source, target, send, recv, place, lane):
            return pltpu.make_async_remote_copy(
                src_ref=source,
                dst_ref=target,
                send_sem=send,
                recv_sem=recv,
                device_id={"sp": place, "tp": lane},
                device_id_type=pl.DeviceIdType.MESH,
            )

        def queries_of(group, offset):
            return q_ref.at[pl.ds(pl.multiple_of(group * 4 * tok + offset, 2 * tok), 2 * tok)]

        def trade(group, slot):
            target = pair_ref.at[pl.ds(pl.multiple_of(slot + group * 2 * tok, 2 * tok), 2 * tok)]
            return remote(queries_of(group, 2 * tok - shift), target,
                          q_send.at[group], q_recv.at[group], mirror, head)

        def lane_of(way, distance):
            return ((chip + (chips - distance if way == 0 else distance)) % chips) * 2 + core

        def wanted(way, distance, part):
            far = chips // 2
            return distance < far or (distance == far and part == way)

        def weight(way, distance, part):
            lane = lane_of(way, distance - 1)
            rows = pl.ds(part * share_rows, share_rows)
            source = down_ref.at[rows] if distance == 1 else all_ref.at[lane, rows]
            index = (way * chips + distance) * 2 + part
            return remote(source, all_ref.at[lane, rows], w_send.at[index], w_recv.at[index],
                          mine, ((chip + (1 if way == 0 else chips - 1)) % chips) * 2 + core)

        def share(way, distance, part):
            lane = lane_of(way, distance)
            rows = pl.ds(part * share_rows, share_rows)
            source = down_ref.at[rows] if distance == 0 else all_ref.at[lane, rows]
            index = (way * chips + distance) * 2 + part
            return remote(source, all_ref.at[lane, rows],
                          twin_send.at[index], twin_recv.at[index], mine, twin)

        def weights_arrive(distance, parts):
            for part in parts:
                for way in (0, 1):
                    if wanted(way, distance, part):
                        weight(way, distance, part).wait_recv()
                        if wanted(way, distance + 1, part):
                            weight(way, distance + 1, part).start()
                        share(way, distance, part).start()

        def at(part, along, across):
            return (along, across) if part == 0 else (across, along)

        def piece(part, where, way, own=False, side=None):
            block = block_at(*where)
            rows = pl.ds(part * part_rows, part_rows)
            cols = slice(None) if side is None else pl.ds(side * half, half)
            index = (part * block_count + block) * 2
            source = own_ref.at[rows] if own else kv_ref.at[block, rows, cols]
            compass = ((1, 0), (3, 0), (0, 1), (0, 3)).index(way)
            return remote(source, kv_ref.at[block, rows, cols],
                          kv_send.at[index * 2 + compass],
                          kv_recv.at[index + (0 if side is None else side)],
                          block_at(*way), head)

        def landed(part, where, side=None):
            piece(part, where, (1, 0), side=side).wait_recv()

        sent = []

        def push(part, where, way, own=False, side=None):
            piece(part, where, way, own, side).start()
            sent.append((part, where, way, own, side))

        def spread(part, where):
            push(part, where, at(part, 0, 1))
            push(part, where, at(part, 0, 3))

        def neighbours_first():
            for part in (0, 1):
                for along, side, way in ((3, 0, 1), (1, 1, 3)):
                    landed(part, at(part, along, 0))
                    push(part, at(part, along, 0), at(part, way, 0), side=side)
                    spread(part, at(part, along, 0))

        def pass_across(alongs):
            for part in (0, 1):
                for along in alongs:
                    for across, side, way in ((3, 0, 1), (1, 1, 3)):
                        landed(part, at(part, along, across))
                        push(part, at(part, along, across), at(part, 0, way), side=side)

        def far_first():
            for part in (0, 1):
                landed(part, at(part, 2, 0), 0)
                landed(part, at(part, 2, 0), 1)
                spread(part, at(part, 2, 0))

        def far_across(alongs):
            for part in (0, 1):
                for along in alongs:
                    landed(part, at(part, along, 2), 0)
                    landed(part, at(part, along, 2), 1)

        for group in range(groups):
            trade(group, own_slot).start()
        for part in (0, 1):
            for way in (0, 1):
                weight(way, 1, part).start()
            share(0, 0, part).start()
        for part in (0, 1):
            push(part, (0, 0), at(part, 1, 0), own=True)
            push(part, (0, 0), at(part, 3, 0), own=True)
        for part in (0, 1):
            push(part, (0, 0), at(part, 0, 1), own=True)
            push(part, (0, 0), at(part, 0, 3), own=True)
        kv_ref[mine] = own_ref[...]
        for group in range(groups):
            target = pl.ds(pl.multiple_of(own_slot + group * 2 * tok, 2 * tok), 2 * tok)
            pair_ref[target, :] = queries_of(group, shift)[...]
        peak_ref[...] = jnp.full_like(peak_ref, -1e30)
        acc_ref[...] = jnp.zeros_like(acc_ref)
        lane = lax.broadcasted_iota(jnp.int32, (shard_len, 128), 1)
        val_ref[...] = jnp.where(lane == VH, 1.0, 0.0).astype(jnp.bfloat16)

        def attend(block, parts):
            keys = kv_ref[block, :QK, :]
            val_ref[:, :VH] = kv_ref[block, QK:, :].T
            values = val_ref[...]
            for start, masked in parts:
                for first in range(start, start + half, Q_TILE):
                    rows = pl.ds(first, Q_TILE)
                    scores = jnp.dot(
                        pair_ref[rows, :QK], keys, preferred_element_type=jnp.float32
                    )
                    if masked:
                        q_pos = lax.broadcasted_iota(jnp.int32, scores.shape, 0)
                        k_pos = lax.broadcasted_iota(jnp.int32, scores.shape, 1)
                        q_pos = q_pos + (first - start)
                        q_pos = q_pos + (q_pos // (2 * tok)) * (2 * tok)
                        scores = jnp.where(k_pos - q_pos <= shift, scores, -1e30)
                    old = peak_ref[rows, :]
                    new = jnp.maximum(old, jnp.max(scores, axis=1, keepdims=True))
                    weights = jnp.exp2((scores - new[:, :1]) * SCORE_EXP).astype(jnp.bfloat16)
                    factor = jnp.exp2((old - new) * SCORE_EXP)
                    peak_ref[rows, :] = new
                    acc_ref[rows, :] = acc_ref[rows, :] * factor + jnp.dot(
                        weights, values, preferred_element_type=jnp.float32
                    )

        def visit(step, _):
            @pl.when(step == 0)
            def _():
                neighbours_first()
                for group in range(groups):
                    trade(group, far_slot).wait_recv()

            @pl.when(step == 1)
            def _():
                pass_across((0,))
                weights_arrive(1, (0,))

            @pl.when(step == 3)
            def _():
                weights_arrive(1, (1,))

            @pl.when(step == 6)
            def _():
                weights_arrive(2, (0,))

            @pl.when(step == 8)
            def _():
                weights_arrive(2, (1,))

            @pl.when(step == 10)
            def _():
                weights_arrive(3, (0,))

            @pl.when(step == 13)
            def _():
                weights_arrive(3, (1,))

            @pl.when(step == 2)
            def _():
                far_first()

            @pl.when(step == 5)
            def _():
                pass_across((1, 3))

            @pl.when(step == 9)
            def _():
                far_across((0,))
                pass_across((2,))

            @pl.when(step == 11)
            def _():
                far_across((1, 3))

            @pl.when(step == 15)
            def _():
                far_across((2,))

            dx = sum(jnp.where(step == k, v[0], 0) for k, v in enumerate(VISITS) if v[0])
            dy = sum(jnp.where(step == k, v[1], 0) for k, v in enumerate(VISITS) if v[1])
            block = block_at(dx, dy)

            @pl.when(block < low)
            def _():
                attend(block, ((0, False), (half, False)))

            @pl.when(block == low)
            def _():
                attend(block, ((0, True), (half, False)))

            @pl.when((block > low) & (block < high))
            def _():
                attend(block, ((half, False),))

            @pl.when(block == high)
            def _():
                attend(block, ((half, True),))

        lax.fori_loop(0, block_count, visit, None)
        shares = (acc_ref[...] / acc_ref[:, VH : VH + 1]).reshape(tp_count, 2, pack, 128)
        lanes = lax.broadcasted_iota(jnp.int32, (tp_count, pack, 128), 2)
        done_ref[...] = (
            jnp.where(lanes < VH, shares[:, 0], pltpu.roll(shares[:, 1], VH, 2))
            .reshape(tp_count * pack, 128)
            .astype(jnp.bfloat16)
        )

        per_slot = tp_count // 2

        def piece_of(slot, order):
            return pl.ds(pl.multiple_of((slot // tok + order) * pack, pack), pack)

        def result(index):
            side, order = index // per_slot, index % per_slot
            slot = jnp.where(side == 0, own_slot, far_slot)
            return remote(done_ref.at[piece_of(slot, order)], tok_ref.at[head],
                          out_send.at[index], out_recv.at[head],
                          jnp.where(side == 0, mine, mirror),
                          (order // 2) * 4 + shift // tok + order % 2)

        here = (chip % 2) * 2 * tok == shift
        self_order = (head // 4) * 2 + core
        self_index = jnp.where(here, self_order, tp_count)

        def send_result(index, _):
            @pl.when(index != self_index)
            def _():
                result(index).start()

        lax.fori_loop(0, tp_count, send_result, None)

        @pl.when(here)
        def _():
            tok_ref[head] = done_ref[piece_of(own_slot, self_order), :]

        def take_result(index, _):
            @pl.when(jnp.logical_not(here & (index == head)))
            def _():
                remote(done_ref.at[pl.ds(0, pack)], tok_ref.at[index],
                       out_send.at[index], out_recv.at[index], mirror, head).wait_recv()

        lax.fori_loop(0, tp_count, take_result, None)
        out_ref[...] = tok_ref[...]

        far = chips // 2
        weights_arrive(far, (0, 1))
        for part in (0, 1):
            share(0, 0, part).wait()
            for distance in range(1, far + 1):
                for way in (0, 1):
                    if wanted(way, distance, part):
                        weight(way, distance, part).wait_send()
                        share(way, distance, part).wait()
        for group in range(groups):
            trade(group, own_slot).wait_send()
        for message in sent:
            piece(*message).wait_send()

        def drain(index, _):
            @pl.when(index != self_index)
            def _():
                result(index).wait_send()

        lax.fori_loop(0, tp_count, drain, None)

    return pl.pallas_call(
        kernel,
        out_shape=(
            jax.ShapeDtypeStruct((tp_count, pack, 128), jnp.bfloat16),
            jax.ShapeDtypeStruct((tp_count, hidden, width), jnp.bfloat16),
        ),
        in_specs=[pl.BlockSpec(memory_space=pltpu.VMEM)] * 2
        + [pl.BlockSpec(memory_space=pltpu.HBM)],
        out_specs=(
            pl.BlockSpec(memory_space=pltpu.VMEM),
            pl.BlockSpec(memory_space=pltpu.HBM),
        ),
        scratch_shapes=[
            pltpu.VMEM((block_count, bundle_rows, shard_len), jnp.bfloat16),
            pltpu.VMEM((shard_len, 128), jnp.bfloat16),
            pltpu.VMEM((shard_len, 128), jnp.float32),
            pltpu.VMEM((shard_len, 128), jnp.float32),
            pltpu.VMEM((shard_len, 128), jnp.bfloat16),
            pltpu.VMEM((tp_count * pack, 128), jnp.bfloat16),
            pltpu.VMEM((tp_count, pack, 128), jnp.bfloat16),
            pltpu.SemaphoreType.DMA((block_count * 8,)),
            pltpu.SemaphoreType.DMA((block_count * 4,)),
            pltpu.SemaphoreType.DMA((groups,)),
            pltpu.SemaphoreType.DMA((groups,)),
            pltpu.SemaphoreType.DMA((tp_count,)),
            pltpu.SemaphoreType.DMA((tp_count,)),
            *[pltpu.SemaphoreType.DMA((4 * chips,)) for _ in range(4)],
        ],
        compiler_params=pltpu.CompilerParams(
            collective_id=4, has_side_effects=True, vmem_limit_bytes=40 * 1024 * 1024
        ),
    )(query_rows, bundle, down)


ROW_CUT = 80


def expert_ring(chooser, ffn_input, gate, up, down, all_down, near_weights, middle):
    count = chooser.shape[0]
    width = ffn_input.shape[1]
    places = lax.axis_size("sp")
    slots = count // places
    chunks = width // 128
    slab = slots * chunks
    hidden = gate.shape[1]
    chips = lax.axis_size("tp") // 2
    both = 2 * count

    def kernel(
        choose_ref, token_ref, gate_ref, up_ref, down_hbm, all_hbm, mix_ref, middle_ref, out_ref,
        wide_ref, load_sem, away_ref, got_ref, home_ref, back_ref, ret_ref, x_ref,
        away_send, away_recv, home_send, home_recv,
        both_ref, down_ref, down_sem, seen, inner_ref, hid_ref, served_ref,
        fwd_send, fwd_recv, back_send, back_recv, twin_send, twin_recv, hid_send, hid_recv,
    ):
        place = lax.axis_index("tp")
        chip, core = place // 2, place % 2
        toward = jnp.where(core == 0, 1, chips - 1)
        ahead = ((chip + toward) % chips) * 2 + core
        behind = ((chip + chips - toward) % chips) * 2 + core
        twin = chip * 2 + 1 - core

        barrier = pltpu.get_barrier_semaphore()
        for other in (ahead, behind, twin):
            pl.semaphore_signal(
                barrier, inc=1, device_id={"tp": other}, device_id_type=pl.DeviceIdType.MESH
            )
        mine = lax.axis_index("sp")

        def peer(turn):
            return (mine + turn) % places

        def greet(turn, _):
            pl.semaphore_signal(
                barrier, inc=1, device_id={"sp": peer(turn)}, device_id_type=pl.DeviceIdType.MESH
            )

        lax.fori_loop(1, places, greet, None)
        loads = (
            pltpu.make_async_copy(gate_ref, both_ref.at[:, pl.ds(0, hidden)], load_sem.at[0]),
            pltpu.make_async_copy(up_ref, both_ref.at[:, pl.ds(hidden, hidden)], load_sem.at[1]),
        )
        for load in loads:
            load.start()

        def lane_rows(lane):
            return pl.ds(pl.multiple_of(lane * hidden, hidden), hidden)

        def load_down(lane):
            return pltpu.make_async_copy(
                all_hbm.at[lane], down_ref.at[lane_rows(lane)], down_sem.at[lane]
            )

        own_down = pltpu.make_async_copy(
            down_hbm, down_ref.at[lane_rows(place)], down_sem.at[place]
        )
        own_down.start()

        def fetch(lane, _):
            @pl.when(lane != place)
            def _():
                load_down(lane).start()

        lax.fori_loop(0, 2 * chips, fetch, None)
        chosen = jnp.dot(choose_ref[...], token_ref[...], preferred_element_type=jnp.float32)
        for chunk in range(chunks):
            wide_ref[pl.ds(chunk, count, stride=chunks), :] = chosen[
                :, chunk * 128 : (chunk + 1) * 128
            ]
        away_ref[...] = wide_ref[...].astype(jnp.bfloat16)
        pl.semaphore_wait(barrier, 3 + places - 1)

        def slab_of(place):
            return pl.ds(pl.multiple_of(place * slab, slab), slab)

        def swap(source, target, send, recv, turn):
            return pltpu.make_async_remote_copy(
                src_ref=source.at[slab_of(peer(turn))],
                dst_ref=target.at[slab_of(mine)],
                send_sem=send.at[turn],
                recv_sem=recv.at[turn],
                device_id={"sp": peer(turn)},
                device_id_type=pl.DeviceIdType.MESH,
            )

        def exchange(source, target, send, recv):
            def start(turn, _):
                swap(source, target, send, recv, turn).start()

            lax.fori_loop(1, places, start, None)
            target[slab_of(mine), :] = source[slab_of(mine), :]

            def finish(turn, _):
                swap(source, target, send, recv, turn).wait_recv()

            lax.fori_loop(1, places, finish, None)

        def narrow(target):
            for chunk in range(chunks):
                target[:, pl.ds(chunk * 128, 128)] = wide_ref[
                    pl.ds(chunk, count, stride=chunks), :
                ].astype(jnp.bfloat16)

        exchange(away_ref, got_ref, away_send, away_recv)
        wide_ref[...] = got_ref[...].astype(jnp.float32)
        narrow(x_ref)

        def remote(source, target, send, recv, other):
            return pltpu.make_async_remote_copy(
                src_ref=source,
                dst_ref=target,
                send_sem=send,
                recv_sem=recv,
                device_id={"tp": other},
                device_id_type=pl.DeviceIdType.MESH,
            )

        first, second = pl.ds(0, ROW_CUT), pl.ds(ROW_CUT, count - ROW_CUT)
        front, rear = pl.ds(0, count), pl.ds(count, count)

        def forward(step):
            return (
                remote(seen.at[step, first], seen.at[step + 1, first],
                       fwd_send.at[step], fwd_recv.at[step + 1], ahead),
                remote(seen.at[step, second], seen.at[step + 1, second],
                       back_send.at[step], back_recv.at[step + 1], behind),
            )

        def forward_own():
            return (
                remote(x_ref.at[first], seen.at[1, first], fwd_send.at[0], fwd_recv.at[1], ahead),
                remote(x_ref.at[second], seen.at[1, second],
                       back_send.at[0], back_recv.at[1], behind),
            )

        def share(step):
            return remote(seen.at[step, front], seen.at[step, rear],
                          twin_send.at[step], twin_recv.at[step], twin)

        def share_own():
            return remote(x_ref, seen.at[0, rear], twin_send.at[0], twin_recv.at[0], twin)

        def chip_at(distance):
            return (chip + chips + distance) % chips

        def tell(step):
            away, near = toward * step, (chips - toward) * step
            parts = (
                (first, 0, chip_at(near) * 2 + core, 0),
                (second, ROW_CUT, chip_at(away) * 2 + core, 1),
                (first, count, chip_at(away) * 2 + 1 - core, 0),
                (second, count + ROW_CUT, chip_at(near) * 2 + 1 - core, 1),
            )
            columns = pl.ds(pl.multiple_of(place * hidden, hidden), hidden)
            return [
                remote(inner_ref.at[step, pl.ds(start, rows.size)], hid_ref.at[rows, columns],
                       hid_send.at[step * 4 + order], hid_recv.at[place * 2 + half], owner)
                for order, (rows, start, owner, half) in enumerate(parts)
            ]

        def hear(lane):
            columns = pl.ds(pl.multiple_of(lane * hidden, hidden), hidden)
            return [
                remote(inner_ref.at[0, pl.ds(0, rows.size)], hid_ref.at[rows, columns],
                       hid_send.at[half], hid_recv.at[lane * 2 + half], twin)
                for half, rows in enumerate((first, second))
            ]

        def experts(step):
            pre = jnp.dot(seen[step], both_ref[...], preferred_element_type=jnp.float32)
            inner_ref[step] = (jax.nn.silu(pre[:, :hidden]) * pre[:, hidden:]).astype(
                jnp.bfloat16
            )

        for copy in (*forward_own(), share_own()):
            copy.start()
        for load in loads:
            load.wait()
        seen[0, front, :] = x_ref[...]
        share_own().wait_recv()
        experts(0)
        hid_ref[:, pl.ds(pl.multiple_of(place * hidden, hidden), hidden)] = inner_ref[0, front, :]
        for copy in tell(0)[2:]:
            copy.start()

        def step_of(step, _):
            for copy in forward(step - 1):
                copy.wait_recv()

            @pl.when(step < chips - 1)
            def _():
                for copy in forward(step):
                    copy.start()

            share(step).start()
            share(step).wait_recv()
            experts(step)
            for copy in tell(step):
                copy.start()

        lax.fori_loop(1, chips, step_of, None)

        def gathered(lane, _):
            @pl.when(lane != place)
            def _():
                load_down(lane).wait()
                for copy in hear(lane):
                    copy.wait_recv()

        lax.fori_loop(0, 2 * chips, gathered, None)
        own_down.wait()

        def project(index, _):
            columns = pl.ds(pl.multiple_of(index * 512, 512), 512)
            served_ref[:, columns] = jnp.dot(
                hid_ref[...], down_ref[:, columns], preferred_element_type=jnp.float32
            )

        lax.fori_loop(0, width // 512, project, None)
        for chunk in range(chunks):
            wide_ref[pl.ds(chunk, count, stride=chunks), :] = served_ref[
                :, chunk * 128 : (chunk + 1) * 128
            ]
        home_ref[...] = wide_ref[...].astype(jnp.bfloat16)
        exchange(home_ref, back_ref, home_send, home_recv)
        wide_ref[...] = back_ref[...].astype(jnp.float32)
        narrow(ret_ref)
        returned = ret_ref[...]
        out_ref[...] = (
            middle_ref[...]
            + jnp.dot(mix_ref[0], returned, preferred_element_type=jnp.float32)
            + jnp.dot(mix_ref[1], returned, preferred_element_type=jnp.float32)
            + jnp.dot(mix_ref[2], returned, preferred_element_type=jnp.float32)
        ).astype(jnp.bfloat16)

        def settle(turn, _):
            swap(away_ref, got_ref, away_send, away_recv, turn).wait_send()
            swap(home_ref, back_ref, home_send, home_recv, turn).wait_send()

        lax.fori_loop(1, places, settle, None)

        for copy in (*forward_own(), share_own(), *tell(0)[2:]):
            copy.wait_send()

        def drain(step, _):
            @pl.when(step < chips - 1)
            def _():
                for copy in forward(step):
                    copy.wait_send()

            share(step).wait_send()
            for copy in tell(step):
                copy.wait_send()

        lax.fori_loop(1, chips, drain, None)

    block = (count, width)
    sems = [pltpu.SemaphoreType.DMA((chips + 1,)) for _ in range(6)]
    sems += [pltpu.SemaphoreType.DMA((4 * chips,)) for _ in range(2)]
    return pl.pallas_call(
        kernel,
        out_shape=jax.ShapeDtypeStruct(middle.shape, jnp.bfloat16),
        in_specs=[pl.BlockSpec(memory_space=pltpu.VMEM)] * 2
        + [pl.BlockSpec(memory_space=pltpu.HBM)] * 4
        + [pl.BlockSpec(memory_space=pltpu.VMEM)] * 2,
        out_specs=pl.BlockSpec(memory_space=pltpu.VMEM),
        scratch_shapes=[
            pltpu.VMEM((count * chunks, 128), jnp.float32),
            pltpu.SemaphoreType.DMA((2,)),
            *[pltpu.VMEM((count * chunks, 128), jnp.bfloat16) for _ in range(4)],
            pltpu.VMEM(block, jnp.bfloat16),
            pltpu.VMEM(block, jnp.bfloat16),
            *[pltpu.SemaphoreType.DMA((places,)) for _ in range(4)],
            pltpu.VMEM((width, 2 * hidden), jnp.bfloat16),
            pltpu.VMEM((2 * chips * hidden, width), jnp.bfloat16),
            pltpu.SemaphoreType.DMA((2 * chips,)),
            pltpu.VMEM((chips, both, width), jnp.bfloat16),
            pltpu.VMEM((chips, both, hidden), jnp.bfloat16),
            pltpu.VMEM((count, 2 * chips * hidden), jnp.bfloat16),
            pltpu.VMEM(block, jnp.float32),
            *sems,
        ],
        compiler_params=pltpu.CompilerParams(
            collective_id=3, has_side_effects=True, vmem_limit_bytes=50 * 1024 * 1024
        ),
    )(chooser, ffn_input, gate, up, down, all_down, near_weights, middle)


def shards(
    queries,
    latent,
    rot_key,
    latent_gain,
    key_up,
    value_up,
    query_gain,
    key_gain,
    out_gain,
    out_weight,
    residual,
    ffn_gain,
    routes,
    route_weights,
    expert_gate,
    expert_up,
    expert_down,
):
    shard_len = queries.shape[0]
    local_heads = key_up.shape[1] // NOPE
    sp_count = lax.axis_size("sp")
    my_first = lax.axis_index("sp") * shard_len
    positions = my_first + jnp.arange(shard_len, dtype=jnp.int32)
    inverse = rope_base ** (-jnp.arange(0, ROPE, 2, dtype=jnp.float32) / ROPE)
    angles = positions.astype(jnp.float32)[:, None] * inverse[None, :]
    lat_f32 = latent.astype(jnp.float32)
    normed_latent = (lat_f32 * rms_scale(lat_f32) * latent_gain).astype(jnp.bfloat16)
    key_nope = jnp.dot(normed_latent, key_up, preferred_element_type=jnp.float32).astype(
        jnp.bfloat16
    )
    value_rows = jnp.dot(normed_latent, value_up, preferred_element_type=jnp.float32).astype(
        jnp.bfloat16
    )
    shared = rot_key.astype(jnp.float32)[:, None, :]
    raw_keys = jnp.concatenate(
        [key_nope.astype(jnp.float32).reshape(shard_len, local_heads, NOPE), shared], axis=-1
    )
    key_rows = head_prepare(raw_keys, key_gain, angles)
    query_rows = head_prepare(
        queries.astype(jnp.float32).reshape(shard_len, local_heads, QK), query_gain, angles
    )
    bundle = jnp.concatenate([key_rows.reshape(shard_len, QK).T, value_rows.T], axis=0)
    tok_count = residual.shape[0]
    by_head, all_down = attention(
        jnp.pad(query_rows.reshape(shard_len, QK), ((0, 0), (0, 128 - QK))), bundle, expert_down[0]
    )
    token_rows = (
        jnp.transpose(by_head.reshape(*by_head.shape[:2], 2, VH), (2, 1, 0, 3))
        .reshape(tok_count, -1)
        .astype(jnp.float32)
    )
    normed_rows = (token_rows * rms_scale(token_rows) * out_gain).astype(jnp.bfloat16)
    mixed = jnp.dot(normed_rows, out_weight, preferred_element_type=jnp.float32)
    middle = residual.astype(jnp.float32) + mixed
    ffn_input = (middle * rms_scale(middle) * ffn_gain).astype(jnp.bfloat16)
    slot_cap = max(2, 9 * tok_count * TOPK // (8 * sp_count))
    slot_total = sp_count * slot_cap
    targets = slot_targets(routes, sp_count, slot_cap)
    slot_ids = jnp.arange(slot_total, dtype=jnp.int32)
    hits = targets[:, :, None] == slot_ids[None, None, :]
    chooser = jnp.any(slot_ids[:, None, None] == targets[None, :, :], axis=2).astype(jnp.bfloat16)
    mix = jnp.sum(jnp.where(hits, route_weights[:, :, None], 0.0), axis=1)
    mix_high = lax.reduce_precision(mix, 8, 7)
    mix_mid = lax.reduce_precision(mix - mix_high, 8, 7)
    mix_low = mix - mix_high - mix_mid
    mix_parts = jnp.stack([mix_high, mix_mid, mix_low]).astype(jnp.bfloat16)
    return expert_ring(
        chooser, ffn_input, expert_gate[0], expert_up[0], expert_down[0], all_down, mix_parts,
        middle,
    )


def solution(mesh):
    return jax.shard_map(
        shards,
        mesh=mesh,
        in_specs=(
            P("sp", "tp"),
            P("sp", None),
            P("sp", None),
            P(),
            P(None, "tp"),
            P(None, "tp"),
            P(),
            P(),
            P(),
            P(),
            P(("sp", "tp"), None),
            P(),
            P(("sp", "tp"), None),
            P(("sp", "tp"), None),
            P("sp", None, "tp"),
            P("sp", None, "tp"),
            P("sp", "tp", None),
        ),
        out_specs=P(("sp", "tp"), None),
        check_vma=False,
    )
```

```python
import jax
import jax.numpy as jnp
from jax import lax
from jax.experimental import pallas as pl
from jax.experimental.pallas import tpu as pltpu
from jax.sharding import PartitionSpec as P

D = 2048
NOPE = 64
ROPE = 32
VH = 64
TOPK = 2
QK = 96


epsilon = 1e-06
rope_base = 10000.0


def rms_scale(values):
    return lax.rsqrt(jnp.mean(values * values, axis=-1, keepdims=True) + epsilon)


def rotate_half(values, angles):
    half_dims = values.shape[-1] // 2
    first_half = values[..., :half_dims]
    second_half = values[..., half_dims:]
    cosine = jnp.cos(angles)
    sine_val = jnp.sin(angles)
    return jnp.concatenate(
        [
            first_half * cosine - second_half * sine_val,
            second_half * cosine + first_half * sine_val,
        ],
        axis=-1,
    )


def head_prepare(raw_rows, gain_vec, angles):
    normed_rows = raw_rows * rms_scale(raw_rows) * gain_vec
    turned_rows = rotate_half(normed_rows[..., NOPE:], angles[:, None, :])
    return jnp.concatenate([normed_rows[..., :NOPE], turned_rows], axis=-1).astype(jnp.bfloat16)


def slot_targets(route_rows, expert_total, slot_cap):
    flat_routes = route_rows.reshape(-1)
    one_hot = (flat_routes[:, None] == jnp.arange(expert_total, dtype=jnp.int32)[None, :]).astype(
        jnp.int32
    )
    earlier = jnp.cumsum(one_hot, axis=0) - one_hot
    rank_in = jnp.sum(earlier * one_hot, axis=1)
    return (flat_routes * slot_cap + rank_in).reshape(route_rows.shape)


SCORE_EXP = 1.4426950408889634 * QK ** (-0.5)
Q_TILE = 256
SIDE = 4
VISITS = (
    (0, 0), (1, 0), (3, 0), (0, 1), (0, 3), (1, 1), (1, 3), (3, 1),
    (3, 3), (2, 0), (0, 2), (2, 1), (2, 3), (1, 2), (3, 2), (2, 2),
)


EARLY = 5


def chunk_order(chips):
    far = chips // 2
    return [(1 + n // 2, n % 2) for n in range(2 * far - 1)]


def attention(query_rows, bundle, down):
    shard_len = query_rows.shape[0]
    half = shard_len // 2
    block_count = lax.axis_size("sp")
    tp_count = lax.axis_size("tp")
    tok = shard_len // tp_count
    chips = tp_count // 2
    pack = tok // 2
    groups = tp_count // 4
    hidden, width = down.shape
    share_rows = hidden // 2
    bundle_rows = bundle.shape[0]
    part_rows = bundle_rows // 2

    def kernel(
        q_ref, own_ref, down_ref, out_ref, all_ref,
        kv_ref, pair_ref, peak_ref, acc_ref, val_ref, done_ref, tok_ref,
        kv_send, kv_recv, q_send, q_recv, out_send, out_recv,
        w_send, w_recv, twin_send, twin_recv,
    ):
        mine = lax.axis_index("sp")
        head = lax.axis_index("tp")
        mirror = block_count - 1 - mine
        low = jnp.minimum(mine, mirror)
        high = jnp.maximum(mine, mirror)
        early = mine < block_count // 2
        shift = pl.multiple_of(jnp.where(early, 0, 2 * tok), 2 * tok)
        own_slot = pl.multiple_of(jnp.where(early, 0, half), half)
        far_slot = pl.multiple_of(half - own_slot, half)
        chip, core = head // 2, head % 2
        twin = chip * 2 + 1 - core
        row, col = mine // SIDE, mine % SIDE

        def block_at(dx, dy):
            return ((row + dy) % SIDE) * SIDE + (col + dx) % SIDE

        barrier = pltpu.get_barrier_semaphore()

        def greet(place, lane):
            pl.semaphore_signal(
                barrier,
                inc=1,
                device_id={"sp": place, "tp": lane},
                device_id_type=pl.DeviceIdType.MESH,
            )

        for dx, dy in ((1, 0), (3, 0), (0, 1), (0, 3)):
            greet(block_at(dx, dy), head)
        for other in range(tp_count):
            greet(mirror, other)

            @pl.when(other != head)
            def _():
                greet(mine, other)

        pl.semaphore_wait(barrier, 4 + 2 * tp_count - 1)

        def remote(source, target, send, recv, place, lane):
            return pltpu.make_async_remote_copy(
                src_ref=source,
                dst_ref=target,
                send_sem=send,
                recv_sem=recv,
                device_id={"sp": place, "tp": lane},
                device_id_type=pl.DeviceIdType.MESH,
            )

        def queries_of(group, offset):
            return q_ref.at[pl.ds(pl.multiple_of(group * 4 * tok + offset, 2 * tok), 2 * tok)]

        def trade(group, slot):
            target = pair_ref.at[pl.ds(pl.multiple_of(slot + group * 2 * tok, 2 * tok), 2 * tok)]
            return remote(queries_of(group, 2 * tok - shift), target,
                          q_send.at[group], q_recv.at[group], mirror, head)

        def lane_of(way, distance):
            return ((chip + (chips - distance if way == 0 else distance)) % chips) * 2 + core

        early_chunks = chunk_order(chips)[:EARLY]

        def weight(way, distance, part):
            lane = lane_of(way, distance - 1)
            rows = pl.ds(part * share_rows, share_rows)
            source = down_ref.at[rows] if distance == 1 else all_ref.at[lane, rows]
            index = (way * chips + distance) * 2 + part
            return remote(source, all_ref.at[lane, rows], w_send.at[index], w_recv.at[index],
                          mine, ((chip + (1 if way == 0 else chips - 1)) % chips) * 2 + core)

        def share(way, distance, part):
            lane = lane_of(way, distance)
            rows = pl.ds(part * share_rows, share_rows)
            source = down_ref.at[rows] if distance == 0 else all_ref.at[lane, rows]
            index = (way * chips + distance) * 2 + part
            return remote(source, all_ref.at[lane, rows],
                          twin_send.at[index], twin_recv.at[index], mine, twin)

        def weights_arrive(distance, turn):
            for way in (0, 1):
                part = turn ^ way
                weight(way, distance, part).wait_recv()
                if (distance + 1, turn) in early_chunks:
                    weight(way, distance + 1, part).start()
                share(way, distance, part).start()

        def at(part, along, across):
            return (along, across) if part == 0 else (across, along)

        def piece(part, where, way, own=False, side=None):
            block = block_at(*where)
            rows = pl.ds(part * part_rows, part_rows)
            cols = slice(None) if side is None else pl.ds(side * half, half)
            index = (part * block_count + block) * 2
            source = own_ref.at[rows] if own else kv_ref.at[block, rows, cols]
            compass = ((1, 0), (3, 0), (0, 1), (0, 3)).index(way)
            return remote(source, kv_ref.at[block, rows, cols],
                          kv_send.at[index * 2 + compass],
                          kv_recv.at[index + (0 if side is None else side)],
                          block_at(*way), head)

        def landed(part, where, side=None):
            piece(part, where, (1, 0), side=side).wait_recv()

        sent = []

        def push(part, where, way, own=False, side=None):
            piece(part, where, way, own, side).start()
            sent.append((part, where, way, own, side))

        def spread(part, where):
            push(part, where, at(part, 0, 1))
            push(part, where, at(part, 0, 3))

        def neighbours_first():
            for part in (0, 1):
                for along, side, way in ((3, 0, 1), (1, 1, 3)):
                    landed(part, at(part, along, 0))
                    push(part, at(part, along, 0), at(part, way, 0), side=side)
                    spread(part, at(part, along, 0))

        def pass_across(alongs):
            for part in (0, 1):
                for along in alongs:
                    for across, side, way in ((3, 0, 1), (1, 1, 3)):
                        landed(part, at(part, along, across))
                        push(part, at(part, along, across), at(part, 0, way), side=side)

        def far_first():
            for part in (0, 1):
                landed(part, at(part, 2, 0), 0)
                landed(part, at(part, 2, 0), 1)
                spread(part, at(part, 2, 0))

        def far_across(alongs):
            for part in (0, 1):
                for along in alongs:
                    landed(part, at(part, along, 2), 0)
                    landed(part, at(part, along, 2), 1)

        for group in range(groups):
            trade(group, own_slot).start()
        for part in (0, 1):
            for way in (0, 1):
                weight(way, 1, part ^ way).start()
            share(0, 0, part).start()
        for part in (0, 1):
            push(part, (0, 0), at(part, 1, 0), own=True)
            push(part, (0, 0), at(part, 3, 0), own=True)
        for part in (0, 1):
            push(part, (0, 0), at(part, 0, 1), own=True)
            push(part, (0, 0), at(part, 0, 3), own=True)
        kv_ref[mine] = own_ref[...]
        for group in range(groups):
            target = pl.ds(pl.multiple_of(own_slot + group * 2 * tok, 2 * tok), 2 * tok)
            pair_ref[target, :] = queries_of(group, shift)[...]
        peak_ref[...] = jnp.full_like(peak_ref, -1e30)
        acc_ref[...] = jnp.zeros_like(acc_ref)
        lane = lax.broadcasted_iota(jnp.int32, (shard_len, 128), 1)
        val_ref[...] = jnp.where(lane == VH, 1.0, 0.0).astype(jnp.bfloat16)

        def attend(block, parts):
            keys = kv_ref[block, :QK, :]
            val_ref[:, :VH] = kv_ref[block, QK:, :].T
            values = val_ref[...]
            for start, masked in parts:
                for first in range(start, start + half, Q_TILE):
                    rows = pl.ds(first, Q_TILE)
                    scores = jnp.dot(
                        pair_ref[rows, :QK], keys, preferred_element_type=jnp.float32
                    )
                    if masked:
                        q_pos = lax.broadcasted_iota(jnp.int32, scores.shape, 0)
                        k_pos = lax.broadcasted_iota(jnp.int32, scores.shape, 1)
                        q_pos = q_pos + (first - start)
                        q_pos = q_pos + (q_pos // (2 * tok)) * (2 * tok)
                        scores = jnp.where(k_pos - q_pos <= shift, scores, -1e30)
                    old = peak_ref[rows, :]
                    new = jnp.maximum(old, jnp.max(scores, axis=1, keepdims=True))
                    weights = jnp.exp2((scores - new[:, :1]) * SCORE_EXP).astype(jnp.bfloat16)
                    factor = jnp.exp2((old - new) * SCORE_EXP)
                    peak_ref[rows, :] = new
                    acc_ref[rows, :] = acc_ref[rows, :] * factor + jnp.dot(
                        weights, values, preferred_element_type=jnp.float32
                    )

        def visit(step, _):
            @pl.when(step == 0)
            def _():
                neighbours_first()
                for group in range(groups):
                    trade(group, far_slot).wait_recv()

            @pl.when(step == 1)
            def _():
                pass_across((0,))
                weights_arrive(1, 0)

            @pl.when(step == 3)
            def _():
                weights_arrive(1, 1)

            @pl.when(step == 6)
            def _():
                weights_arrive(2, 0)

            @pl.when(step == 8)
            def _():
                weights_arrive(2, 1)

            @pl.when(step == 11)
            def _():
                weights_arrive(3, 0)

            @pl.when(step == 2)
            def _():
                far_first()

            @pl.when(step == 5)
            def _():
                pass_across((1, 3))

            @pl.when(step == 9)
            def _():
                far_across((0,))
                pass_across((2,))

            @pl.when(step == 11)
            def _():
                far_across((1, 3))

            @pl.when(step == 15)
            def _():
                far_across((2,))

            dx = sum(jnp.where(step == k, v[0], 0) for k, v in enumerate(VISITS) if v[0])
            dy = sum(jnp.where(step == k, v[1], 0) for k, v in enumerate(VISITS) if v[1])
            block = block_at(dx, dy)

            @pl.when(block < low)
            def _():
                attend(block, ((0, False), (half, False)))

            @pl.when(block == low)
            def _():
                attend(block, ((0, True), (half, False)))

            @pl.when((block > low) & (block < high))
            def _():
                attend(block, ((half, False),))

            @pl.when(block == high)
            def _():
                attend(block, ((half, True),))

        lax.fori_loop(0, block_count, visit, None)
        shares = (acc_ref[...] / acc_ref[:, VH : VH + 1]).reshape(tp_count, 2, pack, 128)
        lanes = lax.broadcasted_iota(jnp.int32, (tp_count, pack, 128), 2)
        done_ref[...] = (
            jnp.where(lanes < VH, shares[:, 0], pltpu.roll(shares[:, 1], VH, 2))
            .reshape(tp_count * pack, 128)
            .astype(jnp.bfloat16)
        )

        per_slot = tp_count // 2

        def piece_of(slot, order):
            return pl.ds(pl.multiple_of((slot // tok + order) * pack, pack), pack)

        def result(index):
            side, order = index // per_slot, index % per_slot
            slot = jnp.where(side == 0, own_slot, far_slot)
            return remote(done_ref.at[piece_of(slot, order)], tok_ref.at[head],
                          out_send.at[index], out_recv.at[head],
                          jnp.where(side == 0, mine, mirror),
                          (order // 2) * 4 + shift // tok + order % 2)

        here = (chip % 2) * 2 * tok == shift
        self_order = (head // 4) * 2 + core
        self_index = jnp.where(here, self_order, tp_count)

        def send_result(index, _):
            @pl.when(index != self_index)
            def _():
                result(index).start()

        lax.fori_loop(0, tp_count, send_result, None)

        @pl.when(here)
        def _():
            tok_ref[head] = done_ref[piece_of(own_slot, self_order), :]

        def take_result(index, _):
            @pl.when(jnp.logical_not(here & (index == head)))
            def _():
                remote(done_ref.at[pl.ds(0, pack)], tok_ref.at[index],
                       out_send.at[index], out_recv.at[index], mirror, head).wait_recv()

        lax.fori_loop(0, tp_count, take_result, None)
        out_ref[...] = tok_ref[...]

        for part in (0, 1):
            share(0, 0, part).wait()
        for distance, turn in early_chunks:
            for way in (0, 1):
                weight(way, distance, turn ^ way).wait_send()
                share(way, distance, turn ^ way).wait()
        for group in range(groups):
            trade(group, own_slot).wait_send()
        for message in sent:
            piece(*message).wait_send()

        def drain(index, _):
            @pl.when(index != self_index)
            def _():
                result(index).wait_send()

        lax.fori_loop(0, tp_count, drain, None)

    return pl.pallas_call(
        kernel,
        out_shape=(
            jax.ShapeDtypeStruct((tp_count, pack, 128), jnp.bfloat16),
            jax.ShapeDtypeStruct((tp_count, hidden, width), jnp.bfloat16),
        ),
        in_specs=[pl.BlockSpec(memory_space=pltpu.VMEM)] * 2
        + [pl.BlockSpec(memory_space=pltpu.HBM)],
        out_specs=(
            pl.BlockSpec(memory_space=pltpu.VMEM),
            pl.BlockSpec(memory_space=pltpu.HBM),
        ),
        scratch_shapes=[
            pltpu.VMEM((block_count, bundle_rows, shard_len), jnp.bfloat16),
            pltpu.VMEM((shard_len, 128), jnp.bfloat16),
            pltpu.VMEM((shard_len, 128), jnp.float32),
            pltpu.VMEM((shard_len, 128), jnp.float32),
            pltpu.VMEM((shard_len, 128), jnp.bfloat16),
            pltpu.VMEM((tp_count * pack, 128), jnp.bfloat16),
            pltpu.VMEM((tp_count, pack, 128), jnp.bfloat16),
            pltpu.SemaphoreType.DMA((block_count * 8,)),
            pltpu.SemaphoreType.DMA((block_count * 4,)),
            pltpu.SemaphoreType.DMA((groups,)),
            pltpu.SemaphoreType.DMA((groups,)),
            pltpu.SemaphoreType.DMA((tp_count,)),
            pltpu.SemaphoreType.DMA((tp_count,)),
            *[pltpu.SemaphoreType.DMA((4 * chips,)) for _ in range(4)],
        ],
        compiler_params=pltpu.CompilerParams(
            collective_id=4, has_side_effects=True, vmem_limit_bytes=60 * 1024 * 1024
        ),
    )(query_rows, bundle, down)


ROW_CUT = 80


def expert_ring(chooser, ffn_input, gate, up, down, all_down, near_weights, middle):
    count = chooser.shape[0]
    width = ffn_input.shape[1]
    places = lax.axis_size("sp")
    slots = count // places
    chunks = width // 128
    slab = slots * chunks
    hidden = gate.shape[1]
    chips = lax.axis_size("tp") // 2
    both = 2 * count

    def kernel(
        choose_ref, token_ref, gate_ref, up_ref, down_hbm, all_hbm, mix_ref, middle_ref, out_ref,
        wide_ref, load_sem, away_ref, got_ref, home_ref, back_ref, ret_ref, x_ref,
        away_send, away_recv, home_send, home_recv,
        both_ref, down_ref, down_sem, late_send, late_recv, pair_send, pair_recv, seen, inner_ref, hid_ref, served_ref,
        hop_send, hop_recv, twin_send, twin_recv, hid_send, hid_recv,
    ):
        place = lax.axis_index("tp")
        chip, core = place // 2, place % 2
        toward = jnp.where(core == 0, 1, chips - 1)
        ahead = ((chip + toward) % chips) * 2 + core
        behind = ((chip + chips - toward) % chips) * 2 + core
        twin = chip * 2 + 1 - core

        barrier = pltpu.get_barrier_semaphore()
        for other in (ahead, behind, twin):
            pl.semaphore_signal(
                barrier, inc=1, device_id={"tp": other}, device_id_type=pl.DeviceIdType.MESH
            )
        mine = lax.axis_index("sp")

        def peer(turn):
            return (mine + turn) % places

        def greet(turn, _):
            pl.semaphore_signal(
                barrier, inc=1, device_id={"sp": peer(turn)}, device_id_type=pl.DeviceIdType.MESH
            )

        lax.fori_loop(1, places, greet, None)
        loads = (
            pltpu.make_async_copy(gate_ref, both_ref.at[:, pl.ds(0, hidden)], load_sem.at[0]),
            pltpu.make_async_copy(up_ref, both_ref.at[:, pl.ds(hidden, hidden)], load_sem.at[1]),
        )
        for load in loads:
            load.start()

        share_rows = hidden // 2
        chunks_in_order = chunk_order(chips)

        def weight_rows(lane, part):
            return pl.ds(
                pl.multiple_of(lane * hidden + part * share_rows, share_rows), share_rows
            )

        def lane_of(way, distance, side):
            far = (chip + (chips - distance if way == 0 else distance)) % chips
            return far * 2 + side

        def load_down(lane, part, index, own=False):
            rows = pl.ds(part * share_rows, share_rows)
            source = down_hbm.at[rows] if own else all_hbm.at[lane, rows]
            return pltpu.make_async_copy(
                source, down_ref.at[weight_rows(lane, part)], down_sem.at[index]
            )

        def down_loads():
            loads = []
            for part in (0, 1):
                loads.append(load_down(place, part, len(loads), own=True))
                loads.append(load_down(twin, part, len(loads)))
            for distance, turn in chunks_in_order[:EARLY]:
                for way in (0, 1):
                    for side in (0, 1):
                        lane = lane_of(way, distance, side)
                        loads.append(load_down(lane, turn ^ way, len(loads)))
            return loads

        for load in down_loads():
            load.start()

        def late_copy(source, target, sems, index, other):
            return pltpu.make_async_remote_copy(
                src_ref=source,
                dst_ref=target,
                send_sem=sems[0].at[index],
                recv_sem=sems[1].at[index],
                device_id={"tp": other},
                device_id_type=pl.DeviceIdType.MESH,
            )

        def late_weights():
            copies = []
            for distance, turn in chunks_in_order[EARLY:]:
                for way in (0, 1):
                    part = turn ^ way
                    lane = lane_of(way, distance - 1, core)
                    following = ((chip + (1 if way == 0 else chips - 1)) % chips) * 2 + core
                    copies.append(
                        late_copy(
                            all_hbm.at[lane, pl.ds(part * share_rows, share_rows)],
                            down_ref.at[weight_rows(lane, part)],
                            (late_send, late_recv), len(copies), following,
                        )
                    )
            return copies

        def late_shares():
            copies = []
            for distance, turn in chunks_in_order[EARLY:]:
                for way in (0, 1):
                    rows = weight_rows(lane_of(way, distance, core), turn ^ way)
                    copies.append(
                        late_copy(down_ref.at[rows], down_ref.at[rows],
                                  (pair_send, pair_recv), len(copies), twin)
                    )
            return copies

        chosen = jnp.dot(choose_ref[...], token_ref[...], preferred_element_type=jnp.float32)
        for chunk in range(chunks):
            wide_ref[pl.ds(chunk, count, stride=chunks), :] = chosen[
                :, chunk * 128 : (chunk + 1) * 128
            ]
        away_ref[...] = wide_ref[...].astype(jnp.bfloat16)
        pl.semaphore_wait(barrier, 3 + places - 1)
        for copy in late_weights():
            copy.start()

        def slab_of(place):
            return pl.ds(pl.multiple_of(place * slab, slab), slab)

        def swap(source, target, send, recv, turn):
            return pltpu.make_async_remote_copy(
                src_ref=source.at[slab_of(peer(turn))],
                dst_ref=target.at[slab_of(mine)],
                send_sem=send.at[turn],
                recv_sem=recv.at[turn],
                device_id={"sp": peer(turn)},
                device_id_type=pl.DeviceIdType.MESH,
            )

        def exchange(source, target, send, recv):
            def start(turn, _):
                swap(source, target, send, recv, turn).start()

            lax.fori_loop(1, places, start, None)
            target[slab_of(mine), :] = source[slab_of(mine), :]

            def finish(turn, _):
                swap(source, target, send, recv, turn).wait_recv()

            lax.fori_loop(1, places, finish, None)

        def narrow(target):
            for chunk in range(chunks):
                target[:, pl.ds(chunk * 128, 128)] = wide_ref[
                    pl.ds(chunk, count, stride=chunks), :
                ].astype(jnp.bfloat16)

        exchange(away_ref, got_ref, away_send, away_recv)
        wide_ref[...] = got_ref[...].astype(jnp.float32)
        narrow(x_ref)

        def remote(source, target, send, recv, other):
            return pltpu.make_async_remote_copy(
                src_ref=source,
                dst_ref=target,
                send_sem=send,
                recv_sem=recv,
                device_id={"tp": other},
                device_id_type=pl.DeviceIdType.MESH,
            )

        first, second = pl.ds(0, ROW_CUT), pl.ds(ROW_CUT, count - ROW_CUT)
        front, rear = pl.ds(0, count), pl.ds(count, count)

        cuts = ((0, 48), (80, 32), (48, 32), (112, 32))

        def forward(step, source=None):
            copies = []
            for index, (start, size) in enumerate(cuts):
                rows = pl.ds(start, size)
                copies.append(
                    remote(
                        seen.at[step, rows] if source is None else source.at[rows],
                        seen.at[step + 1, rows],
                        hop_send.at[step * 4 + index],
                        hop_recv.at[step * 4 + index],
                        ahead if start < ROW_CUT else behind,
                    )
                )
            return copies

        def share(step):
            return remote(seen.at[step, front], seen.at[step, rear],
                          twin_send.at[step], twin_recv.at[step], twin)

        def share_own():
            return remote(x_ref, seen.at[0, rear], twin_send.at[0], twin_recv.at[0], twin)

        def chip_at(distance):
            return (chip + chips + distance) % chips

        def tell(step):
            away, near = toward * step, (chips - toward) * step
            parts = (
                (first, 0, chip_at(near) * 2 + core, 0),
                (second, ROW_CUT, chip_at(away) * 2 + core, 1),
                (first, count, chip_at(away) * 2 + 1 - core, 0),
                (second, count + ROW_CUT, chip_at(near) * 2 + 1 - core, 1),
            )
            columns = pl.ds(pl.multiple_of(place * hidden, hidden), hidden)
            return [
                remote(inner_ref.at[step, pl.ds(start, rows.size)], hid_ref.at[rows, columns],
                       hid_send.at[step * 4 + order], hid_recv.at[place * 2 + half], owner)
                for order, (rows, start, owner, half) in enumerate(parts)
            ]

        def hear(lane):
            columns = pl.ds(pl.multiple_of(lane * hidden, hidden), hidden)
            return [
                remote(inner_ref.at[0, pl.ds(0, rows.size)], hid_ref.at[rows, columns],
                       hid_send.at[half], hid_recv.at[lane * 2 + half], twin)
                for half, rows in enumerate((first, second))
            ]

        def experts(step):
            pre = jnp.dot(seen[step], both_ref[...], preferred_element_type=jnp.float32)
            inner_ref[step] = (jax.nn.silu(pre[:, :hidden]) * pre[:, hidden:]).astype(
                jnp.bfloat16
            )

        for copy in (*forward(0, x_ref), share_own()):
            copy.start()
        for load in loads:
            load.wait()
        seen[0, front, :] = x_ref[...]
        share_own().wait_recv()
        experts(0)
        hid_ref[:, pl.ds(pl.multiple_of(place * hidden, hidden), hidden)] = inner_ref[0, front, :]
        for copy in tell(0)[2:]:
            copy.start()

        def finish_step(step):
            share(step).wait_recv()
            experts(step)
            for copy in tell(step):
                copy.start()

        def step_of(step, _):
            for arrived, onward in zip(forward(step - 1), forward(step)):
                arrived.wait_recv()

                @pl.when(step < chips - 1)
                def _():
                    onward.start()

            share(step).start()

            @pl.when(step == 2)
            def _():
                for copy, onward in zip(late_weights(), late_shares()):
                    copy.wait_recv()
                    onward.start()

            @pl.when(step > 1)
            def _():
                finish_step(step - 1)

        lax.fori_loop(1, chips, step_of, None)
        finish_step(chips - 1)

        def gathered(lane, _):
            @pl.when(lane != place)
            def _():
                for copy in hear(lane):
                    copy.wait_recv()

        lax.fori_loop(0, 2 * chips, gathered, None)
        for load in down_loads():
            load.wait()
        for copy in late_shares():
            copy.wait()
        for copy in late_weights():
            copy.wait_send()

        def project(index, _):
            columns = pl.ds(pl.multiple_of(index * 512, 512), 512)
            served_ref[:, columns] = jnp.dot(
                hid_ref[...], down_ref[:, columns], preferred_element_type=jnp.float32
            )

        lax.fori_loop(0, width // 512, project, None)
        for chunk in range(chunks):
            wide_ref[pl.ds(chunk, count, stride=chunks), :] = served_ref[
                :, chunk * 128 : (chunk + 1) * 128
            ]
        home_ref[...] = wide_ref[...].astype(jnp.bfloat16)
        exchange(home_ref, back_ref, home_send, home_recv)
        wide_ref[...] = back_ref[...].astype(jnp.float32)
        narrow(ret_ref)
        returned = ret_ref[...]
        out_ref[...] = (
            middle_ref[...]
            + jnp.dot(mix_ref[0], returned, preferred_element_type=jnp.float32)
            + jnp.dot(mix_ref[1], returned, preferred_element_type=jnp.float32)
            + jnp.dot(mix_ref[2], returned, preferred_element_type=jnp.float32)
        ).astype(jnp.bfloat16)

        def settle(turn, _):
            swap(away_ref, got_ref, away_send, away_recv, turn).wait_send()
            swap(home_ref, back_ref, home_send, home_recv, turn).wait_send()

        lax.fori_loop(1, places, settle, None)

        for copy in (*forward(0, x_ref), share_own(), *tell(0)[2:]):
            copy.wait_send()

        def drain(step, _):
            @pl.when(step < chips - 1)
            def _():
                for copy in forward(step):
                    copy.wait_send()

            share(step).wait_send()
            for copy in tell(step):
                copy.wait_send()

        lax.fori_loop(1, chips, drain, None)

    block = (count, width)
    sems = [pltpu.SemaphoreType.DMA((4 * chips,)) for _ in range(6)]
    return pl.pallas_call(
        kernel,
        out_shape=jax.ShapeDtypeStruct(middle.shape, jnp.bfloat16),
        in_specs=[pl.BlockSpec(memory_space=pltpu.VMEM)] * 2
        + [pl.BlockSpec(memory_space=pltpu.HBM)] * 4
        + [pl.BlockSpec(memory_space=pltpu.VMEM)] * 2,
        out_specs=pl.BlockSpec(memory_space=pltpu.VMEM),
        scratch_shapes=[
            pltpu.VMEM((count * chunks, 128), jnp.float32),
            pltpu.SemaphoreType.DMA((2,)),
            *[pltpu.VMEM((count * chunks, 128), jnp.bfloat16) for _ in range(4)],
            pltpu.VMEM(block, jnp.bfloat16),
            pltpu.VMEM(block, jnp.bfloat16),
            *[pltpu.SemaphoreType.DMA((places,)) for _ in range(4)],
            pltpu.VMEM((width, 2 * hidden), jnp.bfloat16),
            pltpu.VMEM((2 * chips * hidden, width), jnp.bfloat16),
            pltpu.SemaphoreType.DMA((4 + 4 * EARLY,)),
            *[pltpu.SemaphoreType.DMA((2 * chips,)) for _ in range(4)],
            pltpu.VMEM((chips, both, width), jnp.bfloat16),
            pltpu.VMEM((chips, both, hidden), jnp.bfloat16),
            pltpu.VMEM((count, 2 * chips * hidden), jnp.bfloat16),
            pltpu.VMEM(block, jnp.float32),
            *sems,
        ],
        compiler_params=pltpu.CompilerParams(
            collective_id=3, has_side_effects=True, vmem_limit_bytes=60 * 1024 * 1024
        ),
    )(chooser, ffn_input, gate, up, down, all_down, near_weights, middle)


def shards(
    queries,
    latent,
    rot_key,
    latent_gain,
    key_up,
    value_up,
    query_gain,
    key_gain,
    out_gain,
    out_weight,
    residual,
    ffn_gain,
    routes,
    route_weights,
    expert_gate,
    expert_up,
    expert_down,
):
    shard_len = queries.shape[0]
    local_heads = key_up.shape[1] // NOPE
    sp_count = lax.axis_size("sp")
    my_first = lax.axis_index("sp") * shard_len
    positions = my_first + jnp.arange(shard_len, dtype=jnp.int32)
    inverse = rope_base ** (-jnp.arange(0, ROPE, 2, dtype=jnp.float32) / ROPE)
    angles = positions.astype(jnp.float32)[:, None] * inverse[None, :]
    lat_f32 = latent.astype(jnp.float32)
    normed_latent = (lat_f32 * rms_scale(lat_f32) * latent_gain).astype(jnp.bfloat16)
    key_nope = jnp.dot(normed_latent, key_up, preferred_element_type=jnp.float32).astype(
        jnp.bfloat16
    )
    value_rows = jnp.dot(normed_latent, value_up, preferred_element_type=jnp.float32).astype(
        jnp.bfloat16
    )
    shared = rot_key.astype(jnp.float32)[:, None, :]
    raw_keys = jnp.concatenate(
        [key_nope.astype(jnp.float32).reshape(shard_len, local_heads, NOPE), shared], axis=-1
    )
    key_rows = head_prepare(raw_keys, key_gain, angles)
    query_rows = head_prepare(
        queries.astype(jnp.float32).reshape(shard_len, local_heads, QK), query_gain, angles
    )
    bundle = jnp.concatenate([key_rows.reshape(shard_len, QK).T, value_rows.T], axis=0)
    tok_count = residual.shape[0]
    by_head, all_down = attention(
        jnp.pad(query_rows.reshape(shard_len, QK), ((0, 0), (0, 128 - QK))), bundle, expert_down[0]
    )
    token_rows = (
        jnp.transpose(by_head.reshape(*by_head.shape[:2], 2, VH), (2, 1, 0, 3))
        .reshape(tok_count, -1)
        .astype(jnp.float32)
    )
    normed_rows = (token_rows * rms_scale(token_rows) * out_gain).astype(jnp.bfloat16)
    mixed = jnp.dot(normed_rows, out_weight, preferred_element_type=jnp.float32)
    middle = residual.astype(jnp.float32) + mixed
    ffn_input = (middle * rms_scale(middle) * ffn_gain).astype(jnp.bfloat16)
    slot_cap = max(2, 9 * tok_count * TOPK // (8 * sp_count))
    slot_total = sp_count * slot_cap
    targets = slot_targets(routes, sp_count, slot_cap)
    slot_ids = jnp.arange(slot_total, dtype=jnp.int32)
    hits = targets[:, :, None] == slot_ids[None, None, :]
    chooser = jnp.any(slot_ids[:, None, None] == targets[None, :, :], axis=2).astype(jnp.bfloat16)
    mix = jnp.sum(jnp.where(hits, route_weights[:, :, None], 0.0), axis=1)
    mix_high = lax.reduce_precision(mix, 8, 7)
    mix_mid = lax.reduce_precision(mix - mix_high, 8, 7)
    mix_low = mix - mix_high - mix_mid
    mix_parts = jnp.stack([mix_high, mix_mid, mix_low]).astype(jnp.bfloat16)
    return expert_ring(
        chooser, ffn_input, expert_gate[0], expert_up[0], expert_down[0], all_down, mix_parts,
        middle,
    )


def solution(mesh):
    return jax.shard_map(
        shards,
        mesh=mesh,
        in_specs=(
            P("sp", "tp"),
            P("sp", None),
            P("sp", None),
            P(),
            P(None, "tp"),
            P(None, "tp"),
            P(),
            P(),
            P(),
            P(),
            P(("sp", "tp"), None),
            P(),
            P(("sp", "tp"), None),
            P(("sp", "tp"), None),
            P("sp", None, "tp"),
            P("sp", None, "tp"),
            P("sp", "tp", None),
        ),
        out_specs=P(("sp", "tp"), None),
        check_vma=False,
    )
```

```python
import jax
import jax.numpy as jnp
from jax import lax
from jax.experimental import pallas as pl
from jax.experimental.pallas import tpu as pltpu
from jax.sharding import PartitionSpec as P

D = 2048
NOPE = 64
ROPE = 32
VH = 64
TOPK = 2
QK = 96


epsilon = 1e-06
rope_base = 10000.0


def rms_scale(values):
    return lax.rsqrt(jnp.mean(values * values, axis=-1, keepdims=True) + epsilon)


def rotate_half(values, angles):
    half_dims = values.shape[-1] // 2
    first_half = values[..., :half_dims]
    second_half = values[..., half_dims:]
    cosine = jnp.cos(angles)
    sine_val = jnp.sin(angles)
    return jnp.concatenate(
        [
            first_half * cosine - second_half * sine_val,
            second_half * cosine + first_half * sine_val,
        ],
        axis=-1,
    )


def head_prepare(raw_rows, gain_vec, angles):
    normed_rows = raw_rows * rms_scale(raw_rows) * gain_vec
    turned_rows = rotate_half(normed_rows[..., NOPE:], angles[:, None, :])
    return jnp.concatenate([normed_rows[..., :NOPE], turned_rows], axis=-1).astype(jnp.bfloat16)


def slot_targets(route_rows, expert_total, slot_cap):
    flat_routes = route_rows.reshape(-1)
    one_hot = (flat_routes[:, None] == jnp.arange(expert_total, dtype=jnp.int32)[None, :]).astype(
        jnp.int32
    )
    earlier = jnp.cumsum(one_hot, axis=0) - one_hot
    rank_in = jnp.sum(earlier * one_hot, axis=1)
    return (flat_routes * slot_cap + rank_in).reshape(route_rows.shape)


SCORE_EXP = 1.4426950408889634 * QK ** (-0.5)
Q_TILE = 256
SIDE = 4
VISITS = (
    (0, 0), (1, 0), (3, 0), (0, 1), (0, 3), (1, 1), (1, 3), (3, 1),
    (3, 3), (2, 0), (0, 2), (2, 1), (2, 3), (1, 2), (3, 2), (2, 2),
)


WEIGHT_STEPS = (1, 3, 6, 8, 11, 13)


def chunk_order(chips):
    far = chips // 2
    return [(1 + n // 2, n % 2) for n in range(2 * far - 1)]


def attention_phase(
    q_ref, own_ref, down_ref, project_hbm, res_ref, out_gain_ref, ffn_gain_ref,
    out_ref, middle_ref, all_ref, project_ref, project_sem, att_ref,
    kv_ref, pair_ref, peak_ref, acc_ref, val_ref, done_ref, tok_ref,
    kv_send, kv_recv, q_send, q_recv, out_send, out_recv,
    w_send, w_recv, twin_send, twin_recv, meet,
):
    shard_len = q_ref.shape[0]
    half = shard_len // 2
    block_count = lax.axis_size("sp")
    tp_count = lax.axis_size("tp")
    tok = shard_len // tp_count
    chips = tp_count // 2
    pack = tok // 2
    groups = tp_count // 4
    hidden = down_ref.shape[0]
    share_rows = hidden // 2
    part_rows = own_ref.shape[0] // 2
    mine = lax.axis_index("sp")
    head = lax.axis_index("tp")
    mirror = block_count - 1 - mine
    low = jnp.minimum(mine, mirror)
    high = jnp.maximum(mine, mirror)
    early = mine < block_count // 2
    shift = pl.multiple_of(jnp.where(early, 0, 2 * tok), 2 * tok)
    own_slot = pl.multiple_of(jnp.where(early, 0, half), half)
    far_slot = pl.multiple_of(half - own_slot, half)
    chip, core = head // 2, head % 2
    twin = chip * 2 + 1 - core
    row, col = mine // SIDE, mine % SIDE

    def block_at(dx, dy):
        return ((row + dy) % SIDE) * SIDE + (col + dx) % SIDE

    project_load = pltpu.make_async_copy(project_hbm, project_ref, project_sem.at[0])
    project_load.start()
    own_load = pltpu.make_async_copy(down_ref, all_ref.at[head], project_sem.at[1])
    own_load.start()
    meet()
    def remote(source, target, send, recv, place, lane):
        return pltpu.make_async_remote_copy(
            src_ref=source,
            dst_ref=target,
            send_sem=send,
            recv_sem=recv,
            device_id={"sp": place, "tp": lane},
            device_id_type=pl.DeviceIdType.MESH,
        )

    def queries_of(group, offset):
        return q_ref.at[pl.ds(pl.multiple_of(group * 4 * tok + offset, 2 * tok), 2 * tok)]

    def trade(group, slot):
        target = pair_ref.at[pl.ds(pl.multiple_of(slot + group * 2 * tok, 2 * tok), 2 * tok)]
        return remote(queries_of(group, 2 * tok - shift), target,
                      q_send.at[group], q_recv.at[group], mirror, head)

    def lane_of(way, distance):
        return ((chip + (chips - distance if way == 0 else distance)) % chips) * 2 + core

    early_chunks = chunk_order(chips)

    def weight(way, distance, part):
        lane = lane_of(way, distance - 1)
        rows = pl.ds(part * share_rows, share_rows)
        source = down_ref.at[rows] if distance == 1 else all_ref.at[lane, rows]
        index = (way * chips + distance) * 2 + part
        return remote(source, all_ref.at[lane, rows], w_send.at[index], w_recv.at[index],
                      mine, ((chip + (1 if way == 0 else chips - 1)) % chips) * 2 + core)

    def share(way, distance, part):
        lane = lane_of(way, distance)
        rows = pl.ds(part * share_rows, share_rows)
        source = down_ref.at[rows] if distance == 0 else all_ref.at[lane, rows]
        index = (way * chips + distance) * 2 + part
        return remote(source, all_ref.at[lane, rows],
                      twin_send.at[index], twin_recv.at[index], mine, twin)

    def weights_arrive(distance, turn):
        for way in (0, 1):
            part = turn ^ way
            weight(way, distance, part).wait_recv()
            if (distance + 1, turn) in early_chunks:
                weight(way, distance + 1, part).start()
            share(way, distance, part).start()

    def at(part, along, across):
        return (along, across) if part == 0 else (across, along)

    def piece(part, where, way, own=False, side=None):
        block = block_at(*where)
        rows = pl.ds(part * part_rows, part_rows)
        cols = slice(None) if side is None else pl.ds(side * half, half)
        index = (part * block_count + block) * 2
        source = own_ref.at[rows] if own else kv_ref.at[block, rows, cols]
        compass = ((1, 0), (3, 0), (0, 1), (0, 3)).index(way)
        return remote(source, kv_ref.at[block, rows, cols],
                      kv_send.at[index * 2 + compass],
                      kv_recv.at[index + (0 if side is None else side)],
                      block_at(*way), head)

    def landed(part, where, side=None):
        piece(part, where, (1, 0), side=side).wait_recv()

    sent = []

    def push(part, where, way, own=False, side=None):
        piece(part, where, way, own, side).start()
        sent.append((part, where, way, own, side))

    def spread(part, where):
        push(part, where, at(part, 0, 1))
        push(part, where, at(part, 0, 3))

    def neighbours_first():
        for part in (0, 1):
            for along, side, way in ((3, 0, 1), (1, 1, 3)):
                landed(part, at(part, along, 0))
                push(part, at(part, along, 0), at(part, way, 0), side=side)
                spread(part, at(part, along, 0))

    def pass_across(alongs):
        for part in (0, 1):
            for along in alongs:
                for across, side, way in ((3, 0, 1), (1, 1, 3)):
                    landed(part, at(part, along, across))
                    push(part, at(part, along, across), at(part, 0, way), side=side)

    def far_first():
        for part in (0, 1):
            landed(part, at(part, 2, 0), 0)
            landed(part, at(part, 2, 0), 1)
            spread(part, at(part, 2, 0))

    def far_across(alongs):
        for part in (0, 1):
            for along in alongs:
                landed(part, at(part, along, 2), 0)
                landed(part, at(part, along, 2), 1)

    for group in range(groups):
        trade(group, own_slot).start()
    for part in (0, 1):
        for way in (0, 1):
            weight(way, 1, part ^ way).start()
        share(0, 0, part).start()
    for part in (0, 1):
        push(part, (0, 0), at(part, 1, 0), own=True)
        push(part, (0, 0), at(part, 3, 0), own=True)
    for part in (0, 1):
        push(part, (0, 0), at(part, 0, 1), own=True)
        push(part, (0, 0), at(part, 0, 3), own=True)
    kv_ref[mine] = own_ref[...]
    for group in range(groups):
        target = pl.ds(pl.multiple_of(own_slot + group * 2 * tok, 2 * tok), 2 * tok)
        pair_ref[target, :] = queries_of(group, shift)[...]
    peak_ref[...] = jnp.full_like(peak_ref, -1e30)
    acc_ref[...] = jnp.zeros_like(acc_ref)
    lane = lax.broadcasted_iota(jnp.int32, (shard_len, 128), 1)
    val_ref[...] = jnp.where(lane == VH, 1.0, 0.0).astype(jnp.bfloat16)

    def attend(block, parts):
        keys = kv_ref[block, :QK, :]
        val_ref[:, :VH] = kv_ref[block, QK:, :].T
        values = val_ref[...]
        for start, masked in parts:
            for first in range(start, start + half, Q_TILE):
                rows = pl.ds(first, Q_TILE)
                scores = jnp.dot(
                    pair_ref[rows, :QK], keys, preferred_element_type=jnp.float32
                )
                if masked:
                    q_pos = lax.broadcasted_iota(jnp.int32, scores.shape, 0)
                    k_pos = lax.broadcasted_iota(jnp.int32, scores.shape, 1)
                    q_pos = q_pos + (first - start)
                    q_pos = q_pos + (q_pos // (2 * tok)) * (2 * tok)
                    scores = jnp.where(k_pos - q_pos <= shift, scores, -1e30)
                old = peak_ref[rows, :]
                new = jnp.maximum(old, jnp.max(scores, axis=1, keepdims=True))
                weights = jnp.exp2((scores - new[:, :1]) * SCORE_EXP).astype(jnp.bfloat16)
                factor = jnp.exp2((old - new) * SCORE_EXP)
                peak_ref[rows, :] = new
                acc_ref[rows, :] = acc_ref[rows, :] * factor + jnp.dot(
                    weights, values, preferred_element_type=jnp.float32
                )

    def visit(step, _):
        @pl.when(step == 0)
        def _():
            neighbours_first()
            for group in range(groups):
                trade(group, far_slot).wait_recv()

        @pl.when(step == 1)
        def _():
            pass_across((0,))

        for turn_at, chunk in zip(WEIGHT_STEPS, early_chunks):

            @pl.when(step == turn_at)
            def _(chunk=chunk):
                weights_arrive(*chunk)

        @pl.when(step == 2)
        def _():
            far_first()

        @pl.when(step == 5)
        def _():
            pass_across((1, 3))

        @pl.when(step == 9)
        def _():
            far_across((0,))
            pass_across((2,))

        @pl.when(step == 11)
        def _():
            far_across((1, 3))

        @pl.when(step == 15)
        def _():
            far_across((2,))

        dx = sum(jnp.where(step == k, v[0], 0) for k, v in enumerate(VISITS) if v[0])
        dy = sum(jnp.where(step == k, v[1], 0) for k, v in enumerate(VISITS) if v[1])
        block = block_at(dx, dy)

        @pl.when(block < low)
        def _():
            attend(block, ((0, False), (half, False)))

        @pl.when(block == low)
        def _():
            attend(block, ((0, True), (half, False)))

        @pl.when((block > low) & (block < high))
        def _():
            attend(block, ((half, False),))

        @pl.when(block == high)
        def _():
            attend(block, ((half, True),))

    lax.fori_loop(0, block_count, visit, None)
    shares = (acc_ref[...] / acc_ref[:, VH : VH + 1]).reshape(tp_count, 2, pack, 128)
    lanes = lax.broadcasted_iota(jnp.int32, (tp_count, pack, 128), 2)
    done_ref[...] = (
        jnp.where(lanes < VH, shares[:, 0], pltpu.roll(shares[:, 1], VH, 2))
        .reshape(tp_count * pack, 128)
        .astype(jnp.bfloat16)
    )

    per_slot = tp_count // 2

    def piece_of(slot, order):
        return pl.ds(pl.multiple_of((slot // tok + order) * pack, pack), pack)

    def result(index):
        side, order = index // per_slot, index % per_slot
        slot = jnp.where(side == 0, own_slot, far_slot)
        return remote(done_ref.at[piece_of(slot, order)], tok_ref.at[head],
                      out_send.at[index], out_recv.at[head],
                      jnp.where(side == 0, mine, mirror),
                      (order // 2) * 4 + shift // tok + order % 2)

    here = (chip % 2) * 2 * tok == shift
    self_order = (head // 4) * 2 + core
    self_index = jnp.where(here, self_order, tp_count)

    def send_result(index, _):
        @pl.when(index != self_index)
        def _():
            result(index).start()

    lax.fori_loop(0, tp_count, send_result, None)

    @pl.when(here)
    def _():
        tok_ref[head] = done_ref[piece_of(own_slot, self_order), :]

    def take_result(index, _):
        @pl.when(jnp.logical_not(here & (index == head)))
        def _():
            remote(done_ref.at[pl.ds(0, pack)], tok_ref.at[index],
                   out_send.at[index], out_recv.at[index], mirror, head).wait_recv()

    lax.fori_loop(0, tp_count, take_result, None)
    token_heads = tok_ref[...].astype(jnp.float32)
    squares = jnp.sum(token_heads * token_heads, axis=0)
    lane_id = lax.broadcasted_iota(jnp.int32, (pack, 128), 1)
    left = lane_id < VH
    scales = [
        lax.rsqrt(
            jnp.sum(jnp.where(side, squares, 0.0), axis=1, keepdims=True)
            * (1.0 / (tp_count * VH))
            + epsilon
        )
        for side in (left, lane_id >= VH)
    ]
    for pair in range(tp_count // 2):
        columns = pl.ds(pair * 128, 128)
        one, two = token_heads[2 * pair], token_heads[2 * pair + 1]
        top = jnp.where(left, one, pltpu.roll(two, VH, 1)) * scales[0]
        bottom = jnp.where(left, pltpu.roll(one, VH, 1), two) * scales[1]
        att_ref[:pack, columns] = (top * out_gain_ref[:, columns]).astype(jnp.bfloat16)
        att_ref[pack:, columns] = (bottom * out_gain_ref[:, columns]).astype(jnp.bfloat16)
    project_load.wait()
    middle = res_ref[...].astype(jnp.float32) + jnp.dot(
        att_ref[...], project_ref[...], preferred_element_type=jnp.float32
    )
    middle_ref[...] = middle
    out_ref[...] = (middle * rms_scale(middle) * ffn_gain_ref[...]).astype(jnp.bfloat16)

    def late():
        for chunk in early_chunks[len(WEIGHT_STEPS) :]:
            weights_arrive(*chunk)

    def finish():
        own_load.wait()
        for part in (0, 1):
            share(0, 0, part).wait()
        for distance, turn in early_chunks:
            for way in (0, 1):
                weight(way, distance, turn ^ way).wait_send()
                share(way, distance, turn ^ way).wait()
        for group in range(groups):
            trade(group, own_slot).wait_send()
        for message in sent:
            piece(*message).wait_send()

        def drain(index, _):
            @pl.when(index != self_index)
            def _():
                result(index).wait_send()

        lax.fori_loop(0, tp_count, drain, None)

    return late, finish


ROW_CUT = 80


def expert_loads(gate_ref, up_ref, both_ref, load_sem):
    hidden = gate_ref.shape[1]
    return (
        pltpu.make_async_copy(gate_ref, both_ref.at[:, pl.ds(0, hidden)], load_sem.at[0]),
        pltpu.make_async_copy(up_ref, both_ref.at[:, pl.ds(hidden, hidden)], load_sem.at[1]),
    )


def expert_phase(
    choose_ref, token_ref, down_ref, mix_ref, middle_ref, out_ref, loads, late, finish,
    wide_ref, away_ref, got_ref, home_ref, back_ref, ret_ref, x_ref,
    away_send, away_recv, home_send, home_recv, both_ref, seen, inner_ref, hid_ref, served_ref,
    hop_send, hop_recv, twin_send, twin_recv, hid_send, hid_recv,
):
    count = choose_ref.shape[0]
    width = token_ref.shape[1]
    places = lax.axis_size("sp")
    chunks = width // 128
    slab = (count // places) * chunks
    hidden = down_ref.shape[1]
    chips = lax.axis_size("tp") // 2
    place = lax.axis_index("tp")
    chip, core = place // 2, place % 2
    toward = jnp.where(core == 0, 1, chips - 1)
    ahead = ((chip + toward) % chips) * 2 + core
    behind = ((chip + chips - toward) % chips) * 2 + core
    twin = chip * 2 + 1 - core

    mine = lax.axis_index("sp")

    def peer(turn):
        return (mine + turn) % places

    chosen = jnp.dot(choose_ref[...], token_ref[...], preferred_element_type=jnp.float32)
    for chunk in range(chunks):
        wide_ref[pl.ds(chunk, count, stride=chunks), :] = chosen[
            :, chunk * 128 : (chunk + 1) * 128
        ]
    away_ref[...] = wide_ref[...].astype(jnp.bfloat16)

    def slab_of(place):
        return pl.ds(pl.multiple_of(place * slab, slab), slab)

    def swap(source, target, send, recv, turn):
        return pltpu.make_async_remote_copy(
            src_ref=source.at[slab_of(peer(turn))],
            dst_ref=target.at[slab_of(mine)],
            send_sem=send.at[turn],
            recv_sem=recv.at[turn],
            device_id={"sp": peer(turn)},
            device_id_type=pl.DeviceIdType.MESH,
        )

    def exchange(source, target, send, recv):
        def start(turn, _):
            swap(source, target, send, recv, turn).start()

        lax.fori_loop(1, places, start, None)
        target[slab_of(mine), :] = source[slab_of(mine), :]

        def finish(turn, _):
            swap(source, target, send, recv, turn).wait_recv()

        lax.fori_loop(1, places, finish, None)

    def narrow(target):
        for chunk in range(chunks):
            target[:, pl.ds(chunk * 128, 128)] = wide_ref[
                pl.ds(chunk, count, stride=chunks), :
            ].astype(jnp.bfloat16)

    exchange(away_ref, got_ref, away_send, away_recv)
    wide_ref[...] = got_ref[...].astype(jnp.float32)
    narrow(x_ref)

    def remote(source, target, send, recv, other):
        return pltpu.make_async_remote_copy(
            src_ref=source,
            dst_ref=target,
            send_sem=send,
            recv_sem=recv,
            device_id={"tp": other},
            device_id_type=pl.DeviceIdType.MESH,
        )

    first, second = pl.ds(0, ROW_CUT), pl.ds(ROW_CUT, count - ROW_CUT)
    front, rear = pl.ds(0, count), pl.ds(count, count)

    cuts = ((0, 48), (80, 32), (48, 32), (112, 32))

    def forward(step, source=None):
        copies = []
        for index, (start, size) in enumerate(cuts):
            rows = pl.ds(start, size)
            copies.append(
                remote(
                    seen.at[step, rows] if source is None else source.at[rows],
                    seen.at[step + 1, rows],
                    hop_send.at[step * 4 + index],
                    hop_recv.at[step * 4 + index],
                    ahead if start < ROW_CUT else behind,
                )
            )
        return copies

    def share(step):
        return remote(seen.at[step, front], seen.at[step, rear],
                      twin_send.at[step], twin_recv.at[step], twin)

    def share_own():
        return remote(x_ref, seen.at[0, rear], twin_send.at[0], twin_recv.at[0], twin)

    def chip_at(distance):
        return (chip + chips + distance) % chips

    def tell(step):
        away, near = toward * step, (chips - toward) * step
        parts = (
            (first, 0, chip_at(near) * 2 + core, 0),
            (second, ROW_CUT, chip_at(away) * 2 + core, 1),
            (first, count, chip_at(away) * 2 + 1 - core, 0),
            (second, count + ROW_CUT, chip_at(near) * 2 + 1 - core, 1),
        )
        columns = pl.ds(pl.multiple_of(place * hidden, hidden), hidden)
        return [
            remote(inner_ref.at[step, pl.ds(start, rows.size)], hid_ref.at[rows, columns],
                   hid_send.at[step * 4 + order], hid_recv.at[place * 2 + half], owner)
            for order, (rows, start, owner, half) in enumerate(parts)
        ]

    def hear(lane):
        columns = pl.ds(pl.multiple_of(lane * hidden, hidden), hidden)
        return [
            remote(inner_ref.at[0, pl.ds(0, rows.size)], hid_ref.at[rows, columns],
                   hid_send.at[half], hid_recv.at[lane * 2 + half], twin)
            for half, rows in enumerate((first, second))
        ]

    def experts(step):
        pre = jnp.dot(seen[step], both_ref[...], preferred_element_type=jnp.float32)
        inner_ref[step] = (jax.nn.silu(pre[:, :hidden]) * pre[:, hidden:]).astype(
            jnp.bfloat16
        )

    for copy in (*forward(0, x_ref), share_own()):
        copy.start()
    for load in loads:
        load.wait()
    seen[0, front, :] = x_ref[...]
    share_own().wait_recv()
    experts(0)
    hid_ref[:, pl.ds(pl.multiple_of(place * hidden, hidden), hidden)] = inner_ref[0, front, :]
    for copy in tell(0)[2:]:
        copy.start()

    def finish_step(step):
        share(step).wait_recv()
        experts(step)
        for copy in tell(step):
            copy.start()

    def step_of(step, _):
        for arrived, onward in zip(forward(step - 1), forward(step)):
            arrived.wait_recv()

            @pl.when(step < chips - 1)
            def _():
                onward.start()

        share(step).start()

        @pl.when(step == 2)
        def _():
            late()

        @pl.when(step > 1)
        def _():
            finish_step(step - 1)

    lax.fori_loop(1, chips, step_of, None)
    finish_step(chips - 1)

    def gathered(lane, _):
        @pl.when(lane != place)
        def _():
            for copy in hear(lane):
                copy.wait_recv()

    lax.fori_loop(0, 2 * chips, gathered, None)
    finish()

    def project(index, _):
        columns = pl.ds(pl.multiple_of(index * 512, 512), 512)
        served_ref[:, columns] = jnp.dot(
            hid_ref[...], down_ref[:, :, columns].reshape(2 * chips * hidden, 512),
            preferred_element_type=jnp.float32
        )

    lax.fori_loop(0, width // 512, project, None)
    for chunk in range(chunks):
        wide_ref[pl.ds(chunk, count, stride=chunks), :] = served_ref[
            :, chunk * 128 : (chunk + 1) * 128
        ]
    home_ref[...] = wide_ref[...].astype(jnp.bfloat16)
    exchange(home_ref, back_ref, home_send, home_recv)
    wide_ref[...] = back_ref[...].astype(jnp.float32)
    narrow(ret_ref)
    returned = ret_ref[...]
    out_ref[...] = (
        middle_ref[...]
        + jnp.dot(mix_ref[0], returned, preferred_element_type=jnp.float32)
        + jnp.dot(mix_ref[1], returned, preferred_element_type=jnp.float32)
        + jnp.dot(mix_ref[2], returned, preferred_element_type=jnp.float32)
    ).astype(jnp.bfloat16)

    def settle(turn, _):
        swap(away_ref, got_ref, away_send, away_recv, turn).wait_send()
        swap(home_ref, back_ref, home_send, home_recv, turn).wait_send()

    lax.fori_loop(1, places, settle, None)

    for copy in (*forward(0, x_ref), share_own(), *tell(0)[2:]):
        copy.wait_send()

    def drain(step, _):
        @pl.when(step < chips - 1)
        def _():
            for copy in forward(step):
                copy.wait_send()

        share(step).wait_send()
        for copy in tell(step):
            copy.wait_send()

    lax.fori_loop(1, chips, drain, None)


def layer(
    query_rows, bundle, down, project, residual, out_gain, ffn_gain, chooser, gate, up, mix_parts
):
    shard_len = query_rows.shape[0]
    block_count = lax.axis_size("sp")
    tp_count = lax.axis_size("tp")
    tok = shard_len // tp_count
    chips = tp_count // 2
    pack = tok // 2
    groups = tp_count // 4
    hidden, width = down.shape
    count = chooser.shape[0]
    rows = count * (width // 128)
    attention_scratch = [
        pltpu.VMEM((tok, width), jnp.bfloat16),
        pltpu.VMEM((tok, width), jnp.float32),
        pltpu.VMEM((tp_count, hidden, width), jnp.bfloat16),
        pltpu.VMEM(project.shape, jnp.bfloat16),
        pltpu.SemaphoreType.DMA((2,)),
        pltpu.VMEM((tok, tp_count * VH), jnp.bfloat16),
        pltpu.VMEM((block_count, *bundle.shape), jnp.bfloat16),
        pltpu.VMEM((shard_len, 128), jnp.bfloat16),
        pltpu.VMEM((shard_len, 128), jnp.float32),
        pltpu.VMEM((shard_len, 128), jnp.float32),
        pltpu.VMEM((shard_len, 128), jnp.bfloat16),
        pltpu.VMEM((tp_count * pack, 128), jnp.bfloat16),
        pltpu.VMEM((tp_count, pack, 128), jnp.bfloat16),
        pltpu.SemaphoreType.DMA((block_count * 8,)),
        pltpu.SemaphoreType.DMA((block_count * 4,)),
        pltpu.SemaphoreType.DMA((groups,)),
        pltpu.SemaphoreType.DMA((groups,)),
        pltpu.SemaphoreType.DMA((tp_count,)),
        pltpu.SemaphoreType.DMA((tp_count,)),
        *[pltpu.SemaphoreType.DMA((4 * chips,)) for _ in range(4)],
    ]
    expert_scratch = [
        pltpu.VMEM((rows, 128), jnp.float32),
        *[pltpu.VMEM((rows, 128), jnp.bfloat16) for _ in range(4)],
        pltpu.VMEM((count, width), jnp.bfloat16),
        pltpu.VMEM((count, width), jnp.bfloat16),
        *[pltpu.SemaphoreType.DMA((block_count,)) for _ in range(4)],
        pltpu.VMEM((width, 2 * hidden), jnp.bfloat16),
        pltpu.VMEM((chips, 2 * count, width), jnp.bfloat16),
        pltpu.VMEM((chips, 2 * count, hidden), jnp.bfloat16),
        pltpu.VMEM((count, tp_count * hidden), jnp.bfloat16),
        pltpu.VMEM((count, width), jnp.float32),
        *[pltpu.SemaphoreType.DMA((4 * chips,)) for _ in range(6)],
    ]
    split = len(attention_scratch)

    def kernel(
        q_ref, own_ref, down_ref, project_hbm, res_ref, out_gain_ref, ffn_gain_ref,
        choose_ref, gate_ref, up_ref, mix_ref, out_ref, load_sem, *scratch,
    ):
        attention_refs, expert_refs = scratch[:split], scratch[split:]
        token_ref, middle_ref, all_ref = attention_refs[:3]
        loads = expert_loads(gate_ref, up_ref, expert_refs[11], load_sem)
        for load in loads:
            load.start()

        def meet():
            mine = lax.axis_index("sp")
            head = lax.axis_index("tp")
            mirror = block_count - 1 - mine
            row, col = mine // SIDE, mine % SIDE

            def block_at(dx, dy):
                return ((row + dy) % SIDE) * SIDE + (col + dx) % SIDE

            barrier = pltpu.get_barrier_semaphore()

            def greet(place, lane):
                pl.semaphore_signal(
                    barrier,
                    inc=1,
                    device_id={"sp": place, "tp": lane},
                    device_id_type=pl.DeviceIdType.MESH,
                )

            for dx, dy in ((1, 0), (3, 0), (0, 1), (0, 3)):
                greet(block_at(dx, dy), head)
            for other in range(tp_count):
                greet(mirror, other)

                @pl.when(other != head)
                def _():
                    greet(mine, other)

            def greet_place(turn, _):
                greet((mine + turn) % block_count, head)

            lax.fori_loop(1, block_count, greet_place, None)
            pl.semaphore_wait(barrier, 4 + 2 * tp_count - 1 + block_count - 1)

        late, finish = attention_phase(
            q_ref, own_ref, down_ref, project_hbm, res_ref, out_gain_ref, ffn_gain_ref,
            *attention_refs, meet,
        )
        expert_phase(
            choose_ref, token_ref, all_ref, mix_ref, middle_ref, out_ref, loads, late, finish,
            *expert_refs,
        )

    vmem, hbm = pl.BlockSpec(memory_space=pltpu.VMEM), pl.BlockSpec(memory_space=pltpu.HBM)
    return pl.pallas_call(
        kernel,
        out_shape=jax.ShapeDtypeStruct(residual.shape, jnp.bfloat16),
        in_specs=[vmem, vmem, hbm, hbm, vmem, vmem, vmem, vmem, hbm, hbm, vmem],
        out_specs=vmem,
        scratch_shapes=[pltpu.SemaphoreType.DMA((2,)), *attention_scratch, *expert_scratch],
        compiler_params=pltpu.CompilerParams(
            collective_id=5, has_side_effects=True, vmem_limit_bytes=56 * 1024 * 1024
        ),
    )(query_rows, bundle, down, project, residual, out_gain, ffn_gain, chooser, gate, up, mix_parts)


def shards(
    queries,
    latent,
    rot_key,
    latent_gain,
    key_up,
    value_up,
    query_gain,
    key_gain,
    out_gain,
    out_weight,
    residual,
    ffn_gain,
    routes,
    route_weights,
    expert_gate,
    expert_up,
    expert_down,
):
    shard_len = queries.shape[0]
    local_heads = key_up.shape[1] // NOPE
    sp_count = lax.axis_size("sp")
    my_first = lax.axis_index("sp") * shard_len
    positions = my_first + jnp.arange(shard_len, dtype=jnp.int32)
    inverse = rope_base ** (-jnp.arange(0, ROPE, 2, dtype=jnp.float32) / ROPE)
    angles = positions.astype(jnp.float32)[:, None] * inverse[None, :]
    lat_f32 = latent.astype(jnp.float32)
    normed_latent = (lat_f32 * rms_scale(lat_f32) * latent_gain).astype(jnp.bfloat16)
    key_nope = jnp.dot(normed_latent, key_up, preferred_element_type=jnp.float32).astype(
        jnp.bfloat16
    )
    value_rows = jnp.dot(normed_latent, value_up, preferred_element_type=jnp.float32).astype(
        jnp.bfloat16
    )
    shared = rot_key.astype(jnp.float32)[:, None, :]
    raw_keys = jnp.concatenate(
        [key_nope.astype(jnp.float32).reshape(shard_len, local_heads, NOPE), shared], axis=-1
    )
    key_rows = head_prepare(raw_keys, key_gain, angles)
    query_rows = head_prepare(
        queries.astype(jnp.float32).reshape(shard_len, local_heads, QK), query_gain, angles
    )
    bundle = jnp.concatenate([key_rows.reshape(shard_len, QK).T, value_rows.T], axis=0)
    tok_count = residual.shape[0]
    slot_cap = max(2, 9 * tok_count * TOPK // (8 * sp_count))
    slot_total = sp_count * slot_cap
    targets = slot_targets(routes, sp_count, slot_cap)
    slot_ids = jnp.arange(slot_total, dtype=jnp.int32)
    hits = targets[:, :, None] == slot_ids[None, None, :]
    chooser = jnp.any(slot_ids[:, None, None] == targets[None, :, :], axis=2).astype(jnp.bfloat16)
    mix = jnp.sum(jnp.where(hits, route_weights[:, :, None], 0.0), axis=1)
    mix_high = lax.reduce_precision(mix, 8, 7)
    mix_mid = lax.reduce_precision(mix - mix_high, 8, 7)
    mix_low = mix - mix_high - mix_mid
    mix_parts = jnp.stack([mix_high, mix_mid, mix_low]).astype(jnp.bfloat16)
    return layer(
        jnp.pad(query_rows.reshape(shard_len, QK), ((0, 0), (0, 128 - QK))),
        bundle,
        expert_down[0],
        out_weight,
        residual,
        out_gain[None, :],
        ffn_gain[None, :],
        chooser,
        expert_gate[0],
        expert_up[0],
        mix_parts,
    )


def solution(mesh):
    return jax.shard_map(
        shards,
        mesh=mesh,
        in_specs=(
            P("sp", "tp"),
            P("sp", None),
            P("sp", None),
            P(),
            P(None, "tp"),
            P(None, "tp"),
            P(),
            P(),
            P(),
            P(),
            P(("sp", "tp"), None),
            P(),
            P(("sp", "tp"), None),
            P(("sp", "tp"), None),
            P("sp", None, "tp"),
            P("sp", None, "tp"),
            P("sp", "tp", None),
        ),
        out_specs=P(("sp", "tp"), None),
        check_vma=False,
    )
```

```python
import jax
import jax.numpy as jnp
from jax import lax
from jax.experimental import pallas as pl
from jax.experimental.pallas import tpu as pltpu
from jax.sharding import PartitionSpec as P

D = 2048
NOPE = 64
ROPE = 32
VH = 64
TOPK = 2
QK = 96


epsilon = 1e-06
rope_base = 10000.0


def rms_scale(values):
    return lax.rsqrt(jnp.mean(values * values, axis=-1, keepdims=True) + epsilon)


def rotate_half(values, angles):
    half_dims = values.shape[-1] // 2
    first_half = values[..., :half_dims]
    second_half = values[..., half_dims:]
    cosine = jnp.cos(angles)
    sine_val = jnp.sin(angles)
    return jnp.concatenate(
        [
            first_half * cosine - second_half * sine_val,
            second_half * cosine + first_half * sine_val,
        ],
        axis=-1,
    )


def head_prepare(raw_rows, gain_vec, angles):
    normed_rows = raw_rows * rms_scale(raw_rows) * gain_vec
    turned_rows = rotate_half(normed_rows[..., NOPE:], angles[:, None, :])
    return jnp.concatenate([normed_rows[..., :NOPE], turned_rows], axis=-1).astype(jnp.bfloat16)


def slot_targets(route_rows, expert_total, slot_cap):
    flat_routes = route_rows.reshape(-1)
    one_hot = (flat_routes[:, None] == jnp.arange(expert_total, dtype=jnp.int32)[None, :]).astype(
        jnp.int32
    )
    earlier = jnp.cumsum(one_hot, axis=0) - one_hot
    rank_in = jnp.sum(earlier * one_hot, axis=1)
    return (flat_routes * slot_cap + rank_in).reshape(route_rows.shape)


SCORE_EXP = 1.4426950408889634 * QK ** (-0.5)
Q_TILE = 128
SIDE = 4
VISITS = (
    (0, 0), (1, 0), (3, 0), (0, 1), (0, 3), (1, 1), (1, 3), (3, 1),
    (3, 3), (2, 0), (0, 2), (2, 1), (2, 3), (1, 2), (3, 2), (2, 2),
)


WEIGHT_STEPS = (1, 3, 6, 8, 11, 13)


def chunk_order(chips):
    far = chips // 2
    return [(1 + n // 2, n % 2) for n in range(2 * far - 1)]


def attention_phase(
    q_ref, own_ref, down_ref, project_hbm, res_ref, out_gain_ref, ffn_gain_ref,
    out_ref, middle_ref, all_ref, project_ref, project_sem, att_ref,
    kv_ref, pair_ref, peak_ref, acc_ref, val_ref, done_ref, tok_ref,
    kv_send, kv_recv, q_send, q_recv, out_send, out_recv,
    w_send, w_recv, twin_send, twin_recv, meet,
):
    shard_len = q_ref.shape[0]
    half = shard_len // 2
    block_count = lax.axis_size("sp")
    tp_count = lax.axis_size("tp")
    tok = shard_len // tp_count
    chips = tp_count // 2
    pack = tok // 2
    groups = tp_count // 4
    hidden = down_ref.shape[0]
    share_rows = hidden // 2
    part_rows = own_ref.shape[0] // 2
    mine = lax.axis_index("sp")
    head = lax.axis_index("tp")
    mirror = block_count - 1 - mine
    low = jnp.minimum(mine, mirror)
    high = jnp.maximum(mine, mirror)
    early = mine < block_count // 2
    shift = pl.multiple_of(jnp.where(early, 0, 2 * tok), 2 * tok)
    own_slot = pl.multiple_of(jnp.where(early, 0, half), half)
    far_slot = pl.multiple_of(half - own_slot, half)
    chip, core = head // 2, head % 2
    twin = chip * 2 + 1 - core
    row, col = mine // SIDE, mine % SIDE

    def block_at(dx, dy):
        return ((row + dy) % SIDE) * SIDE + (col + dx) % SIDE

    project_load = pltpu.make_async_copy(project_hbm, project_ref, project_sem.at[0])
    project_load.start()
    own_load = pltpu.make_async_copy(down_ref, all_ref.at[head], project_sem.at[1])
    own_load.start()
    meet()
    def remote(source, target, send, recv, place, lane):
        return pltpu.make_async_remote_copy(
            src_ref=source,
            dst_ref=target,
            send_sem=send,
            recv_sem=recv,
            device_id={"sp": place, "tp": lane},
            device_id_type=pl.DeviceIdType.MESH,
        )

    def queries_of(group, offset):
        return q_ref.at[pl.ds(pl.multiple_of(group * 4 * tok + offset, 2 * tok), 2 * tok)]

    def trade(group, slot):
        target = pair_ref.at[pl.ds(pl.multiple_of(slot + group * 2 * tok, 2 * tok), 2 * tok)]
        return remote(queries_of(group, 2 * tok - shift), target,
                      q_send.at[group], q_recv.at[group], mirror, head)

    def lane_of(way, distance):
        return ((chip + (chips - distance if way == 0 else distance)) % chips) * 2 + core

    early_chunks = chunk_order(chips)

    def weight(way, distance, part):
        lane = lane_of(way, distance - 1)
        rows = pl.ds(part * share_rows, share_rows)
        source = down_ref.at[rows] if distance == 1 else all_ref.at[lane, rows]
        index = (way * chips + distance) * 2 + part
        return remote(source, all_ref.at[lane, rows], w_send.at[index], w_recv.at[index],
                      mine, ((chip + (1 if way == 0 else chips - 1)) % chips) * 2 + core)

    def share(way, distance, part):
        lane = lane_of(way, distance)
        rows = pl.ds(part * share_rows, share_rows)
        source = down_ref.at[rows] if distance == 0 else all_ref.at[lane, rows]
        index = (way * chips + distance) * 2 + part
        return remote(source, all_ref.at[lane, rows],
                      twin_send.at[index], twin_recv.at[index], mine, twin)

    def weights_arrive(distance, turn):
        for way in (0, 1):
            part = turn ^ way
            weight(way, distance, part).wait_recv()
            if (distance + 1, turn) in early_chunks:
                weight(way, distance + 1, part).start()
            share(way, distance, part).start()

    def at(part, along, across):
        return (along, across) if part == 0 else (across, along)

    def piece(part, where, way, own=False, side=None):
        block = block_at(*where)
        rows = pl.ds(part * part_rows, part_rows)
        cols = slice(None) if side is None else pl.ds(side * half, half)
        index = (part * block_count + block) * 2
        source = own_ref.at[rows] if own else kv_ref.at[block, rows, cols]
        compass = ((1, 0), (3, 0), (0, 1), (0, 3)).index(way)
        return remote(source, kv_ref.at[block, rows, cols],
                      kv_send.at[index * 2 + compass],
                      kv_recv.at[index + (0 if side is None else side)],
                      block_at(*way), head)

    def landed(part, where, side=None):
        piece(part, where, (1, 0), side=side).wait_recv()

    sent = []

    def push(part, where, way, own=False, side=None):
        piece(part, where, way, own, side).start()
        sent.append((part, where, way, own, side))

    def spread(part, where):
        push(part, where, at(part, 0, 1))
        push(part, where, at(part, 0, 3))

    def neighbours_first():
        for part in (0, 1):
            for along, side, way in ((3, 0, 1), (1, 1, 3)):
                landed(part, at(part, along, 0))
                push(part, at(part, along, 0), at(part, way, 0), side=side)
                spread(part, at(part, along, 0))

    def pass_across(alongs):
        for part in (0, 1):
            for along in alongs:
                for across, side, way in ((3, 0, 1), (1, 1, 3)):
                    landed(part, at(part, along, across))
                    push(part, at(part, along, across), at(part, 0, way), side=side)

    def far_first():
        for part in (0, 1):
            landed(part, at(part, 2, 0), 0)
            landed(part, at(part, 2, 0), 1)
            spread(part, at(part, 2, 0))

    def far_across(alongs):
        for part in (0, 1):
            for along in alongs:
                landed(part, at(part, along, 2), 0)
                landed(part, at(part, along, 2), 1)

    for group in range(groups):
        trade(group, own_slot).start()
    for part in (0, 1):
        for way in (0, 1):
            weight(way, 1, part ^ way).start()
        share(0, 0, part).start()
    for part in (0, 1):
        push(part, (0, 0), at(part, 1, 0), own=True)
        push(part, (0, 0), at(part, 3, 0), own=True)
    for part in (0, 1):
        push(part, (0, 0), at(part, 0, 1), own=True)
        push(part, (0, 0), at(part, 0, 3), own=True)
    kv_ref[mine] = own_ref[...]
    for group in range(groups):
        target = pl.ds(pl.multiple_of(own_slot + group * 2 * tok, 2 * tok), 2 * tok)
        pair_ref[target, :] = queries_of(group, shift)[...]
    peak_ref[...] = jnp.full_like(peak_ref, -1e30)
    acc_ref[...] = jnp.zeros_like(acc_ref)
    lane = lax.broadcasted_iota(jnp.int32, (shard_len, 128), 1)
    val_ref[...] = jnp.where(lane == VH, 1.0, 0.0).astype(jnp.bfloat16)

    def attend(block, parts):
        keys = kv_ref[block, :QK, :]
        val_ref[:, :VH] = kv_ref[block, QK:, :].T
        values = val_ref[...]
        for start, masked in parts:
            tiles = range(start, start + half, Q_TILE)
            all_scores = [
                jnp.dot(
                    pair_ref[pl.ds(first, Q_TILE), :QK], keys, preferred_element_type=jnp.float32
                )
                for first in tiles
            ]
            for first, scores in zip(tiles, all_scores):
                rows = pl.ds(first, Q_TILE)
                if masked:
                    q_pos = lax.broadcasted_iota(jnp.int32, scores.shape, 0)
                    k_pos = lax.broadcasted_iota(jnp.int32, scores.shape, 1)
                    q_pos = q_pos + (first - start)
                    q_pos = q_pos + (q_pos // (2 * tok)) * (2 * tok)
                    scores = jnp.where(k_pos - q_pos <= shift, scores, -1e30)
                old = peak_ref[rows, :]
                new = jnp.maximum(old, jnp.max(scores, axis=1, keepdims=True))
                spread_peak = jnp.tile(new, (1, shard_len // 128))
                weights = jnp.exp2((scores - spread_peak) * SCORE_EXP).astype(jnp.bfloat16)
                factor = jnp.exp2((old - new) * SCORE_EXP)
                peak_ref[rows, :] = new
                acc_ref[rows, :] = acc_ref[rows, :] * factor + jnp.dot(
                    weights, values, preferred_element_type=jnp.float32
                )

    def visit(step, _):
        @pl.when(step == 0)
        def _():
            neighbours_first()
            for group in range(groups):
                trade(group, far_slot).wait_recv()

        @pl.when(step == 1)
        def _():
            pass_across((0,))

        for turn_at, chunk in zip(WEIGHT_STEPS, early_chunks):

            @pl.when(step == turn_at)
            def _(chunk=chunk):
                weights_arrive(*chunk)

        @pl.when(step == 2)
        def _():
            far_first()

        @pl.when(step == 5)
        def _():
            pass_across((1, 3))

        @pl.when(step == 9)
        def _():
            far_across((0,))
            pass_across((2,))

        @pl.when(step == 11)
        def _():
            far_across((1, 3))

        @pl.when(step == 15)
        def _():
            far_across((2,))

        dx = sum(jnp.where(step == k, v[0], 0) for k, v in enumerate(VISITS) if v[0])
        dy = sum(jnp.where(step == k, v[1], 0) for k, v in enumerate(VISITS) if v[1])
        block = block_at(dx, dy)

        @pl.when(block < low)
        def _():
            attend(block, ((0, False), (half, False)))

        @pl.when(block == low)
        def _():
            attend(block, ((0, True), (half, False)))

        @pl.when((block > low) & (block < high))
        def _():
            attend(block, ((half, False),))

        @pl.when(block == high)
        def _():
            attend(block, ((half, True),))

    lax.fori_loop(0, block_count, visit, None)
    shares = (acc_ref[...] / acc_ref[:, VH : VH + 1]).reshape(tp_count, 2, pack, 128)
    lanes = lax.broadcasted_iota(jnp.int32, (tp_count, pack, 128), 2)
    done_ref[...] = (
        jnp.where(lanes < VH, shares[:, 0], pltpu.roll(shares[:, 1], VH, 2))
        .reshape(tp_count * pack, 128)
        .astype(jnp.bfloat16)
    )

    per_slot = tp_count // 2

    def piece_of(slot, order):
        return pl.ds(pl.multiple_of((slot // tok + order) * pack, pack), pack)

    def result(index):
        side, order = index // per_slot, index % per_slot
        slot = jnp.where(side == 0, own_slot, far_slot)
        return remote(done_ref.at[piece_of(slot, order)], tok_ref.at[head],
                      out_send.at[index], out_recv.at[head],
                      jnp.where(side == 0, mine, mirror),
                      (order // 2) * 4 + shift // tok + order % 2)

    here = (chip % 2) * 2 * tok == shift
    self_order = (head // 4) * 2 + core
    self_index = jnp.where(here, self_order, tp_count)

    def send_result(index, _):
        @pl.when(index != self_index)
        def _():
            result(index).start()

    lax.fori_loop(0, tp_count, send_result, None)

    @pl.when(here)
    def _():
        tok_ref[head] = done_ref[piece_of(own_slot, self_order), :]

    def take_result(index, _):
        @pl.when(jnp.logical_not(here & (index == head)))
        def _():
            remote(done_ref.at[pl.ds(0, pack)], tok_ref.at[index],
                   out_send.at[index], out_recv.at[index], mirror, head).wait_recv()

    lax.fori_loop(0, tp_count, take_result, None)
    token_heads = tok_ref[...].astype(jnp.float32)
    squares = jnp.sum(token_heads * token_heads, axis=0)
    lane_id = lax.broadcasted_iota(jnp.int32, (pack, 128), 1)
    left = lane_id < VH
    scales = [
        lax.rsqrt(
            jnp.sum(jnp.where(side, squares, 0.0), axis=1, keepdims=True)
            * (1.0 / (tp_count * VH))
            + epsilon
        )
        for side in (left, lane_id >= VH)
    ]
    for pair in range(tp_count // 2):
        columns = pl.ds(pair * 128, 128)
        one, two = token_heads[2 * pair], token_heads[2 * pair + 1]
        top = jnp.where(left, one, pltpu.roll(two, VH, 1)) * scales[0]
        bottom = jnp.where(left, pltpu.roll(one, VH, 1), two) * scales[1]
        att_ref[:pack, columns] = (top * out_gain_ref[:, columns]).astype(jnp.bfloat16)
        att_ref[pack:, columns] = (bottom * out_gain_ref[:, columns]).astype(jnp.bfloat16)
    project_load.wait()
    middle = res_ref[...].astype(jnp.float32) + jnp.dot(
        att_ref[...], project_ref[...], preferred_element_type=jnp.float32
    )
    middle_ref[...] = middle
    out_ref[...] = (middle * rms_scale(middle) * ffn_gain_ref[...]).astype(jnp.bfloat16)

    def late():
        for chunk in early_chunks[len(WEIGHT_STEPS) :]:
            weights_arrive(*chunk)

    def finish():
        own_load.wait()
        for part in (0, 1):
            share(0, 0, part).wait()
        for distance, turn in early_chunks:
            for way in (0, 1):
                weight(way, distance, turn ^ way).wait_send()
                share(way, distance, turn ^ way).wait()
        for group in range(groups):
            trade(group, own_slot).wait_send()
        for message in sent:
            piece(*message).wait_send()

        def drain(index, _):
            @pl.when(index != self_index)
            def _():
                result(index).wait_send()

        lax.fori_loop(0, tp_count, drain, None)

    return late, finish


ROW_CUT = 80


def expert_loads(gate_ref, up_ref, both_ref, load_sem):
    hidden = gate_ref.shape[1]
    return (
        pltpu.make_async_copy(gate_ref, both_ref.at[:, pl.ds(0, hidden)], load_sem.at[0]),
        pltpu.make_async_copy(up_ref, both_ref.at[:, pl.ds(hidden, hidden)], load_sem.at[1]),
    )


def expert_phase(
    choose_ref, token_ref, down_ref, mix_ref, middle_ref, out_ref, loads, late, finish,
    wide_ref, away_ref, got_ref, home_ref, back_ref, ret_ref, x_ref,
    away_send, away_recv, home_send, home_recv, both_ref, seen, inner_ref, hid_ref, served_ref,
    hop_send, hop_recv, twin_send, twin_recv, hid_send, hid_recv,
):
    count = choose_ref.shape[0]
    width = token_ref.shape[1]
    places = lax.axis_size("sp")
    chunks = width // 128
    slab = (count // places) * chunks
    hidden = down_ref.shape[1]
    chips = lax.axis_size("tp") // 2
    place = lax.axis_index("tp")
    chip, core = place // 2, place % 2
    toward = jnp.where(core == 0, 1, chips - 1)
    ahead = ((chip + toward) % chips) * 2 + core
    behind = ((chip + chips - toward) % chips) * 2 + core
    twin = chip * 2 + 1 - core

    mine = lax.axis_index("sp")

    def peer(turn):
        return (mine + turn) % places

    chosen = jnp.dot(choose_ref[...], token_ref[...], preferred_element_type=jnp.float32)
    for chunk in range(chunks):
        wide_ref[pl.ds(chunk, count, stride=chunks), :] = chosen[
            :, chunk * 128 : (chunk + 1) * 128
        ]
    away_ref[...] = wide_ref[...].astype(jnp.bfloat16)

    def slab_of(place):
        return pl.ds(pl.multiple_of(place * slab, slab), slab)

    def swap(source, target, send, recv, turn):
        return pltpu.make_async_remote_copy(
            src_ref=source.at[slab_of(peer(turn))],
            dst_ref=target.at[slab_of(mine)],
            send_sem=send.at[turn],
            recv_sem=recv.at[turn],
            device_id={"sp": peer(turn)},
            device_id_type=pl.DeviceIdType.MESH,
        )

    def exchange(source, target, send, recv):
        def start(turn, _):
            swap(source, target, send, recv, turn).start()

        lax.fori_loop(1, places, start, None)
        target[slab_of(mine), :] = source[slab_of(mine), :]

        def finish(turn, _):
            swap(source, target, send, recv, turn).wait_recv()

        lax.fori_loop(1, places, finish, None)

    def narrow(target):
        for chunk in range(chunks):
            target[:, pl.ds(chunk * 128, 128)] = wide_ref[
                pl.ds(chunk, count, stride=chunks), :
            ].astype(jnp.bfloat16)

    exchange(away_ref, got_ref, away_send, away_recv)
    wide_ref[...] = got_ref[...].astype(jnp.float32)
    narrow(x_ref)

    def remote(source, target, send, recv, other):
        return pltpu.make_async_remote_copy(
            src_ref=source,
            dst_ref=target,
            send_sem=send,
            recv_sem=recv,
            device_id={"tp": other},
            device_id_type=pl.DeviceIdType.MESH,
        )

    first, second = pl.ds(0, ROW_CUT), pl.ds(ROW_CUT, count - ROW_CUT)
    front, rear = pl.ds(0, count), pl.ds(count, count)

    cuts = ((0, 48), (80, 32), (48, 32), (112, 32))

    def forward(step, source=None):
        copies = []
        for index, (start, size) in enumerate(cuts):
            rows = pl.ds(start, size)
            copies.append(
                remote(
                    seen.at[step, rows] if source is None else source.at[rows],
                    seen.at[step + 1, rows],
                    hop_send.at[step * 4 + index],
                    hop_recv.at[step * 4 + index],
                    ahead if start < ROW_CUT else behind,
                )
            )
        return copies

    def share(step):
        return remote(seen.at[step, front], seen.at[step, rear],
                      twin_send.at[step], twin_recv.at[step], twin)

    def share_own():
        return remote(x_ref, seen.at[0, rear], twin_send.at[0], twin_recv.at[0], twin)

    def chip_at(distance):
        return (chip + chips + distance) % chips

    def tell(step):
        away, near = toward * step, (chips - toward) * step
        parts = (
            (first, 0, chip_at(near) * 2 + core, 0),
            (second, ROW_CUT, chip_at(away) * 2 + core, 1),
            (first, count, chip_at(away) * 2 + 1 - core, 0),
            (second, count + ROW_CUT, chip_at(near) * 2 + 1 - core, 1),
        )
        columns = pl.ds(pl.multiple_of(place * hidden, hidden), hidden)
        return [
            remote(inner_ref.at[step, pl.ds(start, rows.size)], hid_ref.at[rows, columns],
                   hid_send.at[step * 4 + order], hid_recv.at[place * 2 + half], owner)
            for order, (rows, start, owner, half) in enumerate(parts)
        ]

    def hear(lane):
        columns = pl.ds(pl.multiple_of(lane * hidden, hidden), hidden)
        return [
            remote(inner_ref.at[0, pl.ds(0, rows.size)], hid_ref.at[rows, columns],
                   hid_send.at[half], hid_recv.at[lane * 2 + half], twin)
            for half, rows in enumerate((first, second))
        ]

    def experts(step):
        pre = jnp.dot(seen[step], both_ref[...], preferred_element_type=jnp.float32)
        inner_ref[step] = (jax.nn.silu(pre[:, :hidden]) * pre[:, hidden:]).astype(
            jnp.bfloat16
        )

    for copy in (*forward(0, x_ref), share_own()):
        copy.start()
    for load in loads:
        load.wait()
    seen[0, front, :] = x_ref[...]
    share_own().wait_recv()
    experts(0)
    hid_ref[:, pl.ds(pl.multiple_of(place * hidden, hidden), hidden)] = inner_ref[0, front, :]
    for copy in tell(0)[2:]:
        copy.start()

    def finish_step(step):
        share(step).wait_recv()
        experts(step)
        for copy in tell(step):
            copy.start()

    def step_of(step, _):
        for arrived, onward in zip(forward(step - 1), forward(step)):
            arrived.wait_recv()

            @pl.when(step < chips - 1)
            def _():
                onward.start()

        share(step).start()

        @pl.when(step == 2)
        def _():
            late()

        @pl.when(step > 1)
        def _():
            finish_step(step - 1)

    lax.fori_loop(1, chips, step_of, None)
    finish_step(chips - 1)

    def gathered(lane, _):
        @pl.when(lane != place)
        def _():
            for copy in hear(lane):
                copy.wait_recv()

    lax.fori_loop(0, 2 * chips, gathered, None)
    finish()

    def project(index, _):
        columns = pl.ds(pl.multiple_of(index * 512, 512), 512)
        served_ref[:, columns] = jnp.dot(
            hid_ref[...], down_ref[:, :, columns].reshape(2 * chips * hidden, 512),
            preferred_element_type=jnp.float32
        )

    lax.fori_loop(0, width // 512, project, None)
    for chunk in range(chunks):
        wide_ref[pl.ds(chunk, count, stride=chunks), :] = served_ref[
            :, chunk * 128 : (chunk + 1) * 128
        ]
    home_ref[...] = wide_ref[...].astype(jnp.bfloat16)
    exchange(home_ref, back_ref, home_send, home_recv)
    wide_ref[...] = back_ref[...].astype(jnp.float32)
    narrow(ret_ref)
    returned = ret_ref[...]
    out_ref[...] = (
        middle_ref[...]
        + jnp.dot(mix_ref[0], returned, preferred_element_type=jnp.float32)
        + jnp.dot(mix_ref[1], returned, preferred_element_type=jnp.float32)
        + jnp.dot(mix_ref[2], returned, preferred_element_type=jnp.float32)
    ).astype(jnp.bfloat16)

    def settle(turn, _):
        swap(away_ref, got_ref, away_send, away_recv, turn).wait_send()
        swap(home_ref, back_ref, home_send, home_recv, turn).wait_send()

    lax.fori_loop(1, places, settle, None)

    for copy in (*forward(0, x_ref), share_own(), *tell(0)[2:]):
        copy.wait_send()

    def drain(step, _):
        @pl.when(step < chips - 1)
        def _():
            for copy in forward(step):
                copy.wait_send()

        share(step).wait_send()
        for copy in tell(step):
            copy.wait_send()

    lax.fori_loop(1, chips, drain, None)


def layer(
    query_rows, bundle, down, project, residual, out_gain, ffn_gain, chooser, gate, up, mix_parts
):
    shard_len = query_rows.shape[0]
    block_count = lax.axis_size("sp")
    tp_count = lax.axis_size("tp")
    tok = shard_len // tp_count
    chips = tp_count // 2
    pack = tok // 2
    groups = tp_count // 4
    hidden, width = down.shape
    count = chooser.shape[0]
    rows = count * (width // 128)
    attention_scratch = [
        pltpu.VMEM((tok, width), jnp.bfloat16),
        pltpu.VMEM((tok, width), jnp.float32),
        pltpu.VMEM((tp_count, hidden, width), jnp.bfloat16),
        pltpu.VMEM(project.shape, jnp.bfloat16),
        pltpu.SemaphoreType.DMA((2,)),
        pltpu.VMEM((tok, tp_count * VH), jnp.bfloat16),
        pltpu.VMEM((block_count, *bundle.shape), jnp.bfloat16),
        pltpu.VMEM((shard_len, 128), jnp.bfloat16),
        pltpu.VMEM((shard_len, 128), jnp.float32),
        pltpu.VMEM((shard_len, 128), jnp.float32),
        pltpu.VMEM((shard_len, 128), jnp.bfloat16),
        pltpu.VMEM((tp_count * pack, 128), jnp.bfloat16),
        pltpu.VMEM((tp_count, pack, 128), jnp.bfloat16),
        pltpu.SemaphoreType.DMA((block_count * 8,)),
        pltpu.SemaphoreType.DMA((block_count * 4,)),
        pltpu.SemaphoreType.DMA((groups,)),
        pltpu.SemaphoreType.DMA((groups,)),
        pltpu.SemaphoreType.DMA((tp_count,)),
        pltpu.SemaphoreType.DMA((tp_count,)),
        *[pltpu.SemaphoreType.DMA((4 * chips,)) for _ in range(4)],
    ]
    expert_scratch = [
        pltpu.VMEM((rows, 128), jnp.float32),
        *[pltpu.VMEM((rows, 128), jnp.bfloat16) for _ in range(4)],
        pltpu.VMEM((count, width), jnp.bfloat16),
        pltpu.VMEM((count, width), jnp.bfloat16),
        *[pltpu.SemaphoreType.DMA((block_count,)) for _ in range(4)],
        pltpu.VMEM((width, 2 * hidden), jnp.bfloat16),
        pltpu.VMEM((chips, 2 * count, width), jnp.bfloat16),
        pltpu.VMEM((chips, 2 * count, hidden), jnp.bfloat16),
        pltpu.VMEM((count, tp_count * hidden), jnp.bfloat16),
        pltpu.VMEM((count, width), jnp.float32),
        *[pltpu.SemaphoreType.DMA((4 * chips,)) for _ in range(6)],
    ]
    split = len(attention_scratch)

    def kernel(
        q_ref, own_ref, down_ref, project_hbm, res_ref, out_gain_ref, ffn_gain_ref,
        choose_ref, gate_ref, up_ref, mix_ref, out_ref, load_sem, *scratch,
    ):
        attention_refs, expert_refs = scratch[:split], scratch[split:]
        token_ref, middle_ref, all_ref = attention_refs[:3]
        loads = expert_loads(gate_ref, up_ref, expert_refs[11], load_sem)
        for load in loads:
            load.start()

        def meet():
            mine = lax.axis_index("sp")
            head = lax.axis_index("tp")
            mirror = block_count - 1 - mine
            row, col = mine // SIDE, mine % SIDE

            def block_at(dx, dy):
                return ((row + dy) % SIDE) * SIDE + (col + dx) % SIDE

            barrier = pltpu.get_barrier_semaphore()

            def greet(place, lane):
                pl.semaphore_signal(
                    barrier,
                    inc=1,
                    device_id={"sp": place, "tp": lane},
                    device_id_type=pl.DeviceIdType.MESH,
                )

            for dx, dy in ((1, 0), (3, 0), (0, 1), (0, 3)):
                greet(block_at(dx, dy), head)
            for other in range(tp_count):
                greet(mirror, other)

                @pl.when(other != head)
                def _():
                    greet(mine, other)

            def greet_place(turn, _):
                greet((mine + turn) % block_count, head)

            lax.fori_loop(1, block_count, greet_place, None)
            pl.semaphore_wait(barrier, 4 + 2 * tp_count - 1 + block_count - 1)

        late, finish = attention_phase(
            q_ref, own_ref, down_ref, project_hbm, res_ref, out_gain_ref, ffn_gain_ref,
            *attention_refs, meet,
        )
        expert_phase(
            choose_ref, token_ref, all_ref, mix_ref, middle_ref, out_ref, loads, late, finish,
            *expert_refs,
        )

    vmem, hbm = pl.BlockSpec(memory_space=pltpu.VMEM), pl.BlockSpec(memory_space=pltpu.HBM)
    return pl.pallas_call(
        kernel,
        out_shape=jax.ShapeDtypeStruct(residual.shape, jnp.bfloat16),
        in_specs=[vmem, vmem, hbm, hbm, vmem, vmem, vmem, vmem, hbm, hbm, vmem],
        out_specs=vmem,
        scratch_shapes=[pltpu.SemaphoreType.DMA((2,)), *attention_scratch, *expert_scratch],
        compiler_params=pltpu.CompilerParams(
            collective_id=5, has_side_effects=True, vmem_limit_bytes=56 * 1024 * 1024
        ),
    )(query_rows, bundle, down, project, residual, out_gain, ffn_gain, chooser, gate, up, mix_parts)


def shards(
    queries,
    latent,
    rot_key,
    latent_gain,
    key_up,
    value_up,
    query_gain,
    key_gain,
    out_gain,
    out_weight,
    residual,
    ffn_gain,
    routes,
    route_weights,
    expert_gate,
    expert_up,
    expert_down,
):
    shard_len = queries.shape[0]
    local_heads = key_up.shape[1] // NOPE
    sp_count = lax.axis_size("sp")
    my_first = lax.axis_index("sp") * shard_len
    positions = my_first + jnp.arange(shard_len, dtype=jnp.int32)
    inverse = rope_base ** (-jnp.arange(0, ROPE, 2, dtype=jnp.float32) / ROPE)
    angles = positions.astype(jnp.float32)[:, None] * inverse[None, :]
    lat_f32 = latent.astype(jnp.float32)
    normed_latent = (lat_f32 * rms_scale(lat_f32) * latent_gain).astype(jnp.bfloat16)
    key_nope = jnp.dot(normed_latent, key_up, preferred_element_type=jnp.float32).astype(
        jnp.bfloat16
    )
    value_rows = jnp.dot(normed_latent, value_up, preferred_element_type=jnp.float32).astype(
        jnp.bfloat16
    )
    shared = rot_key.astype(jnp.float32)[:, None, :]
    raw_keys = jnp.concatenate(
        [key_nope.astype(jnp.float32).reshape(shard_len, local_heads, NOPE), shared], axis=-1
    )
    key_rows = head_prepare(raw_keys, key_gain, angles)
    query_rows = head_prepare(
        queries.astype(jnp.float32).reshape(shard_len, local_heads, QK), query_gain, angles
    )
    bundle = jnp.concatenate([key_rows.reshape(shard_len, QK).T, value_rows.T], axis=0)
    tok_count = residual.shape[0]
    slot_cap = max(2, 9 * tok_count * TOPK // (8 * sp_count))
    slot_total = sp_count * slot_cap
    targets = slot_targets(routes, sp_count, slot_cap)
    slot_ids = jnp.arange(slot_total, dtype=jnp.int32)
    hits = targets[:, :, None] == slot_ids[None, None, :]
    chooser = jnp.any(slot_ids[:, None, None] == targets[None, :, :], axis=2).astype(jnp.bfloat16)
    mix = jnp.sum(jnp.where(hits, route_weights[:, :, None], 0.0), axis=1)
    mix_high = lax.reduce_precision(mix, 8, 7)
    mix_mid = lax.reduce_precision(mix - mix_high, 8, 7)
    mix_low = mix - mix_high - mix_mid
    mix_parts = jnp.stack([mix_high, mix_mid, mix_low]).astype(jnp.bfloat16)
    return layer(
        jnp.pad(query_rows.reshape(shard_len, QK), ((0, 0), (0, 128 - QK))),
        bundle,
        expert_down[0],
        out_weight,
        residual,
        out_gain[None, :],
        ffn_gain[None, :],
        chooser,
        expert_gate[0],
        expert_up[0],
        mix_parts,
    )


def solution(mesh):
    return jax.shard_map(
        shards,
        mesh=mesh,
        in_specs=(
            P("sp", "tp"),
            P("sp", None),
            P("sp", None),
            P(),
            P(None, "tp"),
            P(None, "tp"),
            P(),
            P(),
            P(),
            P(),
            P(("sp", "tp"), None),
            P(),
            P(("sp", "tp"), None),
            P(("sp", "tp"), None),
            P("sp", None, "tp"),
            P("sp", None, "tp"),
            P("sp", "tp", None),
        ),
        out_specs=P(("sp", "tp"), None),
        check_vma=False,
    )
```

```python
import jax
import jax.numpy as jnp
from jax import lax
from jax.experimental import pallas as pl
from jax.experimental.pallas import tpu as pltpu
from jax.sharding import PartitionSpec as P

D = 2048
NOPE = 64
ROPE = 32
VH = 64
TOPK = 2
QK = 96


epsilon = 1e-06
rope_base = 10000.0


def rms_scale(values):
    return lax.rsqrt(jnp.mean(values * values, axis=-1, keepdims=True) + epsilon)


def rotate_half(values, angles):
    half_dims = values.shape[-1] // 2
    first_half = values[..., :half_dims]
    second_half = values[..., half_dims:]
    cosine = jnp.cos(angles)
    sine_val = jnp.sin(angles)
    return jnp.concatenate(
        [
            first_half * cosine - second_half * sine_val,
            second_half * cosine + first_half * sine_val,
        ],
        axis=-1,
    )


def head_prepare(raw_rows, gain_vec, angles):
    normed_rows = raw_rows * rms_scale(raw_rows) * gain_vec
    turned_rows = rotate_half(normed_rows[..., NOPE:], angles[:, None, :])
    return jnp.concatenate([normed_rows[..., :NOPE], turned_rows], axis=-1).astype(jnp.bfloat16)


def slot_targets(route_rows, expert_total, slot_cap):
    flat_routes = route_rows.reshape(-1)
    one_hot = (flat_routes[:, None] == jnp.arange(expert_total, dtype=jnp.int32)[None, :]).astype(
        jnp.int32
    )
    earlier = jnp.cumsum(one_hot, axis=0) - one_hot
    rank_in = jnp.sum(earlier * one_hot, axis=1)
    return (flat_routes * slot_cap + rank_in).reshape(route_rows.shape)


SCORE_EXP = 1.4426950408889634 * QK ** (-0.5)
Q_TILE = 128
SIDE = 4
VISITS = (
    (0, 0), (1, 0), (3, 0), (0, 1), (0, 3), (1, 1), (1, 3), (3, 1),
    (3, 3), (2, 0), (0, 2), (2, 1), (2, 3), (1, 2), (3, 2), (2, 2),
)


WEIGHT_STEPS = (1, 3, 6, 8, 11, 13)


def chunk_order(chips):
    far = chips // 2
    return [(1 + n // 2, n % 2) for n in range(2 * far - 1)]


def attention_phase(
    q_ref, own_ref, down_ref, project_hbm, res_ref, out_gain_ref, ffn_gain_ref,
    out_ref, middle_ref, all_ref, project_ref, project_sem, att_ref,
    kv_ref, pair_ref, peak_ref, acc_ref, val_ref, done_ref, tok_ref,
    kv_send, kv_recv, q_send, q_recv, out_send, out_recv,
    w_send, w_recv, twin_send, twin_recv, meet,
):
    shard_len = q_ref.shape[0]
    half = shard_len // 2
    block_count = lax.axis_size("sp")
    tp_count = lax.axis_size("tp")
    tok = shard_len // tp_count
    chips = tp_count // 2
    pack = tok // 2
    groups = tp_count // 4
    hidden = down_ref.shape[0]
    share_rows = hidden // 2
    part_rows = own_ref.shape[0] // 2
    mine = lax.axis_index("sp")
    head = lax.axis_index("tp")
    mirror = block_count - 1 - mine
    low = jnp.minimum(mine, mirror)
    high = jnp.maximum(mine, mirror)
    early = mine < block_count // 2
    shift = pl.multiple_of(jnp.where(early, 0, 2 * tok), 2 * tok)
    own_slot = pl.multiple_of(jnp.where(early, 0, half), half)
    far_slot = pl.multiple_of(half - own_slot, half)
    chip, core = head // 2, head % 2
    twin = chip * 2 + 1 - core
    row, col = mine // SIDE, mine % SIDE

    def block_at(dx, dy):
        return ((row + dy) % SIDE) * SIDE + (col + dx) % SIDE

    project_load = pltpu.make_async_copy(project_hbm, project_ref, project_sem.at[0])
    project_load.start()
    own_load = pltpu.make_async_copy(down_ref, all_ref.at[head], project_sem.at[1])
    own_load.start()
    meet()
    def remote(source, target, send, recv, place, lane):
        return pltpu.make_async_remote_copy(
            src_ref=source,
            dst_ref=target,
            send_sem=send,
            recv_sem=recv,
            device_id={"sp": place, "tp": lane},
            device_id_type=pl.DeviceIdType.MESH,
        )

    def queries_of(group, offset):
        return q_ref.at[pl.ds(pl.multiple_of(group * 4 * tok + offset, 2 * tok), 2 * tok)]

    def trade(group, slot):
        target = pair_ref.at[pl.ds(pl.multiple_of(slot + group * 2 * tok, 2 * tok), 2 * tok)]
        return remote(queries_of(group, 2 * tok - shift), target,
                      q_send.at[group], q_recv.at[group], mirror, head)

    def lane_of(way, distance):
        return ((chip + (chips - distance if way == 0 else distance)) % chips) * 2 + core

    early_chunks = chunk_order(chips)

    def weight(way, distance, part):
        lane = lane_of(way, distance - 1)
        rows = pl.ds(part * share_rows, share_rows)
        source = down_ref.at[rows] if distance == 1 else all_ref.at[lane, rows]
        index = (way * chips + distance) * 2 + part
        return remote(source, all_ref.at[lane, rows], w_send.at[index], w_recv.at[index],
                      mine, ((chip + (1 if way == 0 else chips - 1)) % chips) * 2 + core)

    def share(way, distance, part):
        lane = lane_of(way, distance)
        rows = pl.ds(part * share_rows, share_rows)
        source = down_ref.at[rows] if distance == 0 else all_ref.at[lane, rows]
        index = (way * chips + distance) * 2 + part
        return remote(source, all_ref.at[lane, rows],
                      twin_send.at[index], twin_recv.at[index], mine, twin)

    def weights_arrive(distance, turn):
        for way in (0, 1):
            part = turn ^ way
            weight(way, distance, part).wait_recv()
            if (distance + 1, turn) in early_chunks:
                weight(way, distance + 1, part).start()
            share(way, distance, part).start()

    def at(part, along, across):
        return (along, across) if part == 0 else (across, along)

    def piece(part, where, way, own=False, side=None):
        block = block_at(*where)
        rows = pl.ds(part * part_rows, part_rows)
        cols = slice(None) if side is None else pl.ds(side * half, half)
        index = (part * block_count + block) * 2
        source = own_ref.at[rows] if own else kv_ref.at[block, rows, cols]
        compass = ((1, 0), (3, 0), (0, 1), (0, 3)).index(way)
        return remote(source, kv_ref.at[block, rows, cols],
                      kv_send.at[index * 2 + compass],
                      kv_recv.at[index + (0 if side is None else side)],
                      block_at(*way), head)

    def landed(part, where, side=None):
        piece(part, where, (1, 0), side=side).wait_recv()

    sent = []

    def push(part, where, way, own=False, side=None):
        piece(part, where, way, own, side).start()
        sent.append((part, where, way, own, side))

    def spread(part, where):
        push(part, where, at(part, 0, 1))
        push(part, where, at(part, 0, 3))

    def neighbours_first():
        for part in (0, 1):
            for along, side, way in ((3, 0, 1), (1, 1, 3)):
                landed(part, at(part, along, 0))
                push(part, at(part, along, 0), at(part, way, 0), side=side)
                spread(part, at(part, along, 0))

    def pass_across(alongs):
        for part in (0, 1):
            for along in alongs:
                for across, side, way in ((3, 0, 1), (1, 1, 3)):
                    landed(part, at(part, along, across))
                    push(part, at(part, along, across), at(part, 0, way), side=side)

    def far_first():
        for part in (0, 1):
            landed(part, at(part, 2, 0), 0)
            landed(part, at(part, 2, 0), 1)
            spread(part, at(part, 2, 0))

    def far_across(alongs):
        for part in (0, 1):
            for along in alongs:
                landed(part, at(part, along, 2), 0)
                landed(part, at(part, along, 2), 1)

    for group in range(groups):
        trade(group, own_slot).start()
    for part in (0, 1):
        for way in (0, 1):
            weight(way, 1, part ^ way).start()
        share(0, 0, part).start()
    for part in (0, 1):
        push(part, (0, 0), at(part, 1, 0), own=True)
        push(part, (0, 0), at(part, 3, 0), own=True)
    for part in (0, 1):
        push(part, (0, 0), at(part, 0, 1), own=True)
        push(part, (0, 0), at(part, 0, 3), own=True)
    kv_ref[mine] = own_ref[...]
    for group in range(groups):
        target = pl.ds(pl.multiple_of(own_slot + group * 2 * tok, 2 * tok), 2 * tok)
        pair_ref[target, :] = queries_of(group, shift)[...]
    peak_ref[...] = jnp.full_like(peak_ref, -1e30)
    acc_ref[...] = jnp.zeros_like(acc_ref)
    lane = lax.broadcasted_iota(jnp.int32, (shard_len, 128), 1)
    val_ref[...] = jnp.where(lane == VH, 1.0, 0.0).astype(jnp.bfloat16)

    def attend(block, parts):
        keys = kv_ref[block, :QK, :]
        val_ref[:, :VH] = kv_ref[block, QK:, :].T
        values = val_ref[...]
        for start, masked in parts:
            tiles = range(start, start + half, Q_TILE)
            all_scores = [
                jnp.dot(
                    pair_ref[pl.ds(first, Q_TILE), :QK], keys, preferred_element_type=jnp.float32
                )
                for first in tiles
            ]
            for first, scores in zip(tiles, all_scores):
                rows = pl.ds(first, Q_TILE)
                if masked:
                    q_pos = lax.broadcasted_iota(jnp.int32, scores.shape, 0)
                    k_pos = lax.broadcasted_iota(jnp.int32, scores.shape, 1)
                    q_pos = q_pos + (first - start)
                    q_pos = q_pos + (q_pos // (2 * tok)) * (2 * tok)
                    scores = jnp.where(k_pos - q_pos <= shift, scores, -1e30)
                old = peak_ref[rows, :]
                new = jnp.maximum(old, jnp.max(scores, axis=1, keepdims=True))
                spread_peak = jnp.tile(new, (1, shard_len // 128))
                weights = jnp.exp2((scores - spread_peak) * SCORE_EXP).astype(jnp.bfloat16)
                factor = jnp.exp2((old - new) * SCORE_EXP)
                peak_ref[rows, :] = new
                acc_ref[rows, :] = acc_ref[rows, :] * factor + jnp.dot(
                    weights, values, preferred_element_type=jnp.float32
                )

    def visit(step, _):
        @pl.when(step == 0)
        def _():
            neighbours_first()
            for group in range(groups):
                trade(group, far_slot).wait_recv()

        @pl.when(step == 1)
        def _():
            pass_across((0,))

        for turn_at, chunk in zip(WEIGHT_STEPS, early_chunks):

            @pl.when(step == turn_at)
            def _(chunk=chunk):
                weights_arrive(*chunk)

        @pl.when(step == 2)
        def _():
            far_first()

        @pl.when(step == 5)
        def _():
            pass_across((1, 3))

        @pl.when(step == 9)
        def _():
            far_across((0,))
            pass_across((2,))

        @pl.when(step == 11)
        def _():
            far_across((1, 3))

        @pl.when(step == 15)
        def _():
            far_across((2,))

        dx = sum(jnp.where(step == k, v[0], 0) for k, v in enumerate(VISITS) if v[0])
        dy = sum(jnp.where(step == k, v[1], 0) for k, v in enumerate(VISITS) if v[1])
        block = block_at(dx, dy)

        @pl.when(block < low)
        def _():
            attend(block, ((0, False), (half, False)))

        @pl.when(block == low)
        def _():
            attend(block, ((0, True), (half, False)))

        @pl.when((block > low) & (block < high))
        def _():
            attend(block, ((half, False),))

        @pl.when(block == high)
        def _():
            attend(block, ((half, True),))

    lax.fori_loop(0, block_count, visit, None)
    shares = (acc_ref[...] / acc_ref[:, VH : VH + 1]).reshape(tp_count, 2, pack, 128)
    lanes = lax.broadcasted_iota(jnp.int32, (tp_count, pack, 128), 2)
    done_ref[...] = (
        jnp.where(lanes < VH, shares[:, 0], pltpu.roll(shares[:, 1], VH, 2))
        .reshape(tp_count * pack, 128)
        .astype(jnp.bfloat16)
    )

    per_slot = tp_count // 2

    def piece_of(slot, order):
        return pl.ds(pl.multiple_of((slot // tok + order) * pack, pack), pack)

    def result(index):
        side, order = index // per_slot, index % per_slot
        slot = jnp.where(side == 0, own_slot, far_slot)
        return remote(done_ref.at[piece_of(slot, order)], tok_ref.at[head],
                      out_send.at[index], out_recv.at[head],
                      jnp.where(side == 0, mine, mirror),
                      (order // 2) * 4 + shift // tok + order % 2)

    here = (chip % 2) * 2 * tok == shift
    self_order = (head // 4) * 2 + core
    self_index = jnp.where(here, self_order, tp_count)

    def send_result(index, _):
        @pl.when(index != self_index)
        def _():
            result(index).start()

    lax.fori_loop(0, tp_count, send_result, None)

    @pl.when(here)
    def _():
        tok_ref[head] = done_ref[piece_of(own_slot, self_order), :]

    def take_result(index, _):
        @pl.when(jnp.logical_not(here & (index == head)))
        def _():
            remote(done_ref.at[pl.ds(0, pack)], tok_ref.at[index],
                   out_send.at[index], out_recv.at[index], mirror, head).wait_recv()

    lax.fori_loop(0, tp_count, take_result, None)
    token_heads = tok_ref[...].astype(jnp.float32)
    squares = jnp.sum(token_heads * token_heads, axis=0)
    lane_id = lax.broadcasted_iota(jnp.int32, (pack, 128), 1)
    left = lane_id < VH
    scales = [
        lax.rsqrt(
            jnp.sum(jnp.where(side, squares, 0.0), axis=1, keepdims=True)
            * (1.0 / (tp_count * VH))
            + epsilon
        )
        for side in (left, lane_id >= VH)
    ]
    for pair in range(tp_count // 2):
        columns = pl.ds(pair * 128, 128)
        one, two = token_heads[2 * pair], token_heads[2 * pair + 1]
        top = jnp.where(left, one, pltpu.roll(two, VH, 1)) * scales[0]
        bottom = jnp.where(left, pltpu.roll(one, VH, 1), two) * scales[1]
        att_ref[:pack, columns] = (top * out_gain_ref[:, columns]).astype(jnp.bfloat16)
        att_ref[pack:, columns] = (bottom * out_gain_ref[:, columns]).astype(jnp.bfloat16)
    project_load.wait()
    middle = res_ref[...].astype(jnp.float32) + jnp.dot(
        att_ref[...], project_ref[...], preferred_element_type=jnp.float32
    )
    middle_ref[...] = middle
    out_ref[...] = (middle * rms_scale(middle) * ffn_gain_ref[...]).astype(jnp.bfloat16)

    def late():
        for chunk in early_chunks[len(WEIGHT_STEPS) :]:
            weights_arrive(*chunk)

    def finish():
        own_load.wait()
        for part in (0, 1):
            share(0, 0, part).wait()
        for distance, turn in early_chunks:
            for way in (0, 1):
                weight(way, distance, turn ^ way).wait_send()
                share(way, distance, turn ^ way).wait()
        for group in range(groups):
            trade(group, own_slot).wait_send()
        for message in sent:
            piece(*message).wait_send()

        def drain(index, _):
            @pl.when(index != self_index)
            def _():
                result(index).wait_send()

        lax.fori_loop(0, tp_count, drain, None)

    return late, finish


ROW_CUT = 80


def expert_loads(gate_ref, up_ref, both_ref, load_sem):
    hidden = gate_ref.shape[1]
    return (
        pltpu.make_async_copy(gate_ref, both_ref.at[:, pl.ds(0, hidden)], load_sem.at[0]),
        pltpu.make_async_copy(up_ref, both_ref.at[:, pl.ds(hidden, hidden)], load_sem.at[1]),
    )


def expert_phase(
    choose_ref, token_ref, down_ref, mix_ref, middle_ref, out_ref, loads, late, finish,
    wide_ref, away_ref, got_ref, home_ref, back_ref, ret_ref, x_ref,
    away_send, away_recv, home_send, home_recv, both_ref, seen, inner_ref, hid_ref, served_ref,
    hop_send, hop_recv, twin_send, twin_recv, hid_send, hid_recv,
):
    count = choose_ref.shape[0]
    width = token_ref.shape[1]
    places = lax.axis_size("sp")
    chunks = width // 128
    slab = (count // places) * chunks
    hidden = down_ref.shape[1]
    chips = lax.axis_size("tp") // 2
    place = lax.axis_index("tp")
    chip, core = place // 2, place % 2
    toward = jnp.where(core == 0, 1, chips - 1)
    ahead = ((chip + toward) % chips) * 2 + core
    behind = ((chip + chips - toward) % chips) * 2 + core
    twin = chip * 2 + 1 - core

    mine = lax.axis_index("sp")

    def peer(turn):
        return (mine + turn) % places

    chosen = jnp.dot(choose_ref[...], token_ref[...], preferred_element_type=jnp.float32)
    for chunk in range(chunks):
        wide_ref[pl.ds(chunk, count, stride=chunks), :] = chosen[
            :, chunk * 128 : (chunk + 1) * 128
        ]
    away_ref[...] = wide_ref[...].astype(jnp.bfloat16)

    def slab_of(place):
        return pl.ds(pl.multiple_of(place * slab, slab), slab)

    def swap(source, target, send, recv, turn):
        return pltpu.make_async_remote_copy(
            src_ref=source.at[slab_of(peer(turn))],
            dst_ref=target.at[slab_of(mine)],
            send_sem=send.at[turn],
            recv_sem=recv.at[turn],
            device_id={"sp": peer(turn)},
            device_id_type=pl.DeviceIdType.MESH,
        )

    def exchange(source, target, send, recv):
        def start(turn, _):
            swap(source, target, send, recv, turn).start()

        lax.fori_loop(1, places, start, None)
        target[slab_of(mine), :] = source[slab_of(mine), :]

        def finish(turn, _):
            swap(source, target, send, recv, turn).wait_recv()

        lax.fori_loop(1, places, finish, None)

    def narrow(target):
        for chunk in range(chunks):
            target[:, pl.ds(chunk * 128, 128)] = wide_ref[
                pl.ds(chunk, count, stride=chunks), :
            ].astype(jnp.bfloat16)

    exchange(away_ref, got_ref, away_send, away_recv)
    wide_ref[...] = got_ref[...].astype(jnp.float32)
    narrow(x_ref)

    def remote(source, target, send, recv, other):
        return pltpu.make_async_remote_copy(
            src_ref=source,
            dst_ref=target,
            send_sem=send,
            recv_sem=recv,
            device_id={"tp": other},
            device_id_type=pl.DeviceIdType.MESH,
        )

    first, second = pl.ds(0, ROW_CUT), pl.ds(ROW_CUT, count - ROW_CUT)
    front, rear = pl.ds(0, count), pl.ds(count, count)

    cuts = ((0, 48), (80, 32), (48, 32), (112, 32))

    def forward(step, source=None):
        copies = []
        for index, (start, size) in enumerate(cuts):
            rows = pl.ds(start, size)
            copies.append(
                remote(
                    seen.at[step, rows] if source is None else source.at[rows],
                    seen.at[step + 1, rows],
                    hop_send.at[step * 4 + index],
                    hop_recv.at[step * 4 + index],
                    ahead if start < ROW_CUT else behind,
                )
            )
        return copies

    def share(step):
        return remote(seen.at[step, front], seen.at[step, rear],
                      twin_send.at[step], twin_recv.at[step], twin)

    def share_own():
        return remote(x_ref, seen.at[0, rear], twin_send.at[0], twin_recv.at[0], twin)

    def chip_at(distance):
        return (chip + chips + distance) % chips

    def tell(step):
        away, near = toward * step, (chips - toward) * step
        parts = (
            (first, 0, chip_at(near) * 2 + core, 0),
            (second, ROW_CUT, chip_at(away) * 2 + core, 1),
            (first, count, chip_at(away) * 2 + 1 - core, 0),
            (second, count + ROW_CUT, chip_at(near) * 2 + 1 - core, 1),
        )
        columns = pl.ds(pl.multiple_of(place * hidden, hidden), hidden)
        return [
            remote(inner_ref.at[step, pl.ds(start, rows.size)], hid_ref.at[rows, columns],
                   hid_send.at[step * 4 + order], hid_recv.at[place * 2 + half], owner)
            for order, (rows, start, owner, half) in enumerate(parts)
        ]

    def hear(lane):
        columns = pl.ds(pl.multiple_of(lane * hidden, hidden), hidden)
        return [
            remote(inner_ref.at[0, pl.ds(0, rows.size)], hid_ref.at[rows, columns],
                   hid_send.at[half], hid_recv.at[lane * 2 + half], twin)
            for half, rows in enumerate((first, second))
        ]

    def experts(step):
        pre = jnp.dot(seen[step], both_ref[...], preferred_element_type=jnp.float32)
        inner_ref[step] = (jax.nn.silu(pre[:, :hidden]) * pre[:, hidden:]).astype(
            jnp.bfloat16
        )

    for copy in (*forward(0, x_ref), share_own()):
        copy.start()
    for load in loads:
        load.wait()
    seen[0, front, :] = x_ref[...]
    share_own().wait_recv()
    experts(0)
    hid_ref[:, pl.ds(pl.multiple_of(place * hidden, hidden), hidden)] = inner_ref[0, front, :]
    for copy in tell(0)[2:]:
        copy.start()

    def finish_step(step):
        share(step).wait_recv()
        experts(step)
        for copy in tell(step):
            copy.start()

    def step_of(step, _):
        for arrived, onward in zip(forward(step - 1), forward(step)):
            arrived.wait_recv()

            @pl.when(step < chips - 1)
            def _():
                onward.start()

        share(step).start()

        @pl.when(step == 2)
        def _():
            late()

        @pl.when(step > 1)
        def _():
            finish_step(step - 1)

    lax.fori_loop(1, chips, step_of, None)
    finish_step(chips - 1)

    def gathered(lane, _):
        @pl.when(lane != place)
        def _():
            for copy in hear(lane):
                copy.wait_recv()

    lax.fori_loop(0, 2 * chips, gathered, None)
    finish()

    def project(index, _):
        columns = pl.ds(pl.multiple_of(index * 512, 512), 512)
        served_ref[:, columns] = jnp.dot(
            hid_ref[...], down_ref[:, :, columns].reshape(2 * chips * hidden, 512),
            preferred_element_type=jnp.float32
        )

    lax.fori_loop(0, width // 512, project, None)
    for chunk in range(chunks):
        wide_ref[pl.ds(chunk, count, stride=chunks), :] = served_ref[
            :, chunk * 128 : (chunk + 1) * 128
        ]
    home_ref[...] = wide_ref[...].astype(jnp.bfloat16)
    exchange(home_ref, back_ref, home_send, home_recv)
    wide_ref[...] = back_ref[...].astype(jnp.float32)
    narrow(ret_ref)
    returned = ret_ref[...]
    out_ref[...] = (
        middle_ref[...]
        + jnp.dot(mix_ref[0], returned, preferred_element_type=jnp.float32)
        + jnp.dot(mix_ref[1], returned, preferred_element_type=jnp.float32)
        + jnp.dot(mix_ref[2], returned, preferred_element_type=jnp.float32)
    ).astype(jnp.bfloat16)

    def settle(turn, _):
        swap(away_ref, got_ref, away_send, away_recv, turn).wait_send()
        swap(home_ref, back_ref, home_send, home_recv, turn).wait_send()

    lax.fori_loop(1, places, settle, None)

    for copy in (*forward(0, x_ref), share_own(), *tell(0)[2:]):
        copy.wait_send()

    def drain(step, _):
        @pl.when(step < chips - 1)
        def _():
            for copy in forward(step):
                copy.wait_send()

        share(step).wait_send()
        for copy in tell(step):
            copy.wait_send()

    lax.fori_loop(1, chips, drain, None)


def layer(
    query_rows, bundle, down, project, residual, out_gain, ffn_gain, chooser, gate, up, mix_parts
):
    shard_len = query_rows.shape[0]
    block_count = lax.axis_size("sp")
    tp_count = lax.axis_size("tp")
    tok = shard_len // tp_count
    chips = tp_count // 2
    pack = tok // 2
    groups = tp_count // 4
    hidden, width = down.shape
    count = chooser.shape[0]
    rows = count * (width // 128)
    attention_scratch = [
        pltpu.VMEM((tok, width), jnp.bfloat16),
        pltpu.VMEM((tok, width), jnp.float32),
        pltpu.VMEM((tp_count, hidden, width), jnp.bfloat16),
        pltpu.VMEM(project.shape, jnp.bfloat16),
        pltpu.SemaphoreType.DMA((2,)),
        pltpu.VMEM((tok, tp_count * VH), jnp.bfloat16),
        pltpu.VMEM((block_count, *bundle.shape), jnp.bfloat16),
        pltpu.VMEM((shard_len, 128), jnp.bfloat16),
        pltpu.VMEM((shard_len, 128), jnp.float32),
        pltpu.VMEM((shard_len, 128), jnp.float32),
        pltpu.VMEM((shard_len, 128), jnp.bfloat16),
        pltpu.VMEM((tp_count * pack, 128), jnp.bfloat16),
        pltpu.VMEM((tp_count, pack, 128), jnp.bfloat16),
        pltpu.SemaphoreType.DMA((block_count * 8,)),
        pltpu.SemaphoreType.DMA((block_count * 4,)),
        pltpu.SemaphoreType.DMA((groups,)),
        pltpu.SemaphoreType.DMA((groups,)),
        pltpu.SemaphoreType.DMA((tp_count,)),
        pltpu.SemaphoreType.DMA((tp_count,)),
        *[pltpu.SemaphoreType.DMA((4 * chips,)) for _ in range(4)],
    ]
    expert_scratch = [
        pltpu.VMEM((rows, 128), jnp.float32),
        *[pltpu.VMEM((rows, 128), jnp.bfloat16) for _ in range(4)],
        pltpu.VMEM((count, width), jnp.bfloat16),
        pltpu.VMEM((count, width), jnp.bfloat16),
        *[pltpu.SemaphoreType.DMA((block_count,)) for _ in range(4)],
        pltpu.VMEM((width, 2 * hidden), jnp.bfloat16),
        pltpu.VMEM((chips, 2 * count, width), jnp.bfloat16),
        pltpu.VMEM((chips, 2 * count, hidden), jnp.bfloat16),
        pltpu.VMEM((count, tp_count * hidden), jnp.bfloat16),
        pltpu.VMEM((count, width), jnp.float32),
        *[pltpu.SemaphoreType.DMA((4 * chips,)) for _ in range(6)],
    ]
    split = len(attention_scratch)

    def kernel(
        q_ref, own_ref, down_ref, project_hbm, res_ref, out_gain_ref, ffn_gain_ref,
        choose_ref, gate_ref, up_ref, mix_ref, out_ref, load_sem, *scratch,
    ):
        attention_refs, expert_refs = scratch[:split], scratch[split:]
        token_ref, middle_ref, all_ref = attention_refs[:3]
        loads = expert_loads(gate_ref, up_ref, expert_refs[11], load_sem)
        for load in loads:
            load.start()

        def meet():
            mine = lax.axis_index("sp")
            head = lax.axis_index("tp")
            mirror = block_count - 1 - mine
            row, col = mine // SIDE, mine % SIDE

            def block_at(dx, dy):
                return ((row + dy) % SIDE) * SIDE + (col + dx) % SIDE

            barrier = pltpu.get_barrier_semaphore()

            def greet(place, lane):
                pl.semaphore_signal(
                    barrier,
                    inc=1,
                    device_id={"sp": place, "tp": lane},
                    device_id_type=pl.DeviceIdType.MESH,
                )

            for dx, dy in ((1, 0), (3, 0), (0, 1), (0, 3)):
                greet(block_at(dx, dy), head)
            for other in range(tp_count):
                greet(mirror, other)

                @pl.when(other != head)
                def _():
                    greet(mine, other)

            def greet_place(turn, _):
                greet((mine + turn) % block_count, head)

            lax.fori_loop(1, block_count, greet_place, None)
            pl.semaphore_wait(barrier, 4 + 2 * tp_count - 1 + block_count - 1)

        late, finish = attention_phase(
            q_ref, own_ref, down_ref, project_hbm, res_ref, out_gain_ref, ffn_gain_ref,
            *attention_refs, meet,
        )
        expert_phase(
            choose_ref, token_ref, all_ref, mix_ref, middle_ref, out_ref, loads, late, finish,
            *expert_refs,
        )

    vmem, hbm = pl.BlockSpec(memory_space=pltpu.VMEM), pl.BlockSpec(memory_space=pltpu.HBM)
    return pl.pallas_call(
        kernel,
        out_shape=jax.ShapeDtypeStruct(residual.shape, jnp.bfloat16),
        in_specs=[vmem, vmem, hbm, hbm, vmem, vmem, vmem, vmem, hbm, hbm, vmem],
        out_specs=vmem,
        scratch_shapes=[pltpu.SemaphoreType.DMA((2,)), *attention_scratch, *expert_scratch],
        compiler_params=pltpu.CompilerParams(
            collective_id=5, has_side_effects=True, vmem_limit_bytes=50 * 1024 * 1024
        ),
    )(query_rows, bundle, down, project, residual, out_gain, ffn_gain, chooser, gate, up, mix_parts)


def shards(
    queries,
    latent,
    rot_key,
    latent_gain,
    key_up,
    value_up,
    query_gain,
    key_gain,
    out_gain,
    out_weight,
    residual,
    ffn_gain,
    routes,
    route_weights,
    expert_gate,
    expert_up,
    expert_down,
):
    shard_len = queries.shape[0]
    local_heads = key_up.shape[1] // NOPE
    sp_count = lax.axis_size("sp")
    my_first = lax.axis_index("sp") * shard_len
    positions = my_first + jnp.arange(shard_len, dtype=jnp.int32)
    inverse = rope_base ** (-jnp.arange(0, ROPE, 2, dtype=jnp.float32) / ROPE)
    angles = positions.astype(jnp.float32)[:, None] * inverse[None, :]
    lat_f32 = latent.astype(jnp.float32)
    normed_latent = (lat_f32 * rms_scale(lat_f32) * latent_gain).astype(jnp.bfloat16)
    key_nope = jnp.dot(normed_latent, key_up, preferred_element_type=jnp.float32).astype(
        jnp.bfloat16
    )
    value_rows = jnp.dot(normed_latent, value_up, preferred_element_type=jnp.float32).astype(
        jnp.bfloat16
    )
    shared = rot_key.astype(jnp.float32)[:, None, :]
    raw_keys = jnp.concatenate(
        [key_nope.astype(jnp.float32).reshape(shard_len, local_heads, NOPE), shared], axis=-1
    )
    key_rows = head_prepare(raw_keys, key_gain, angles)
    query_rows = head_prepare(
        queries.astype(jnp.float32).reshape(shard_len, local_heads, QK), query_gain, angles
    )
    bundle = jnp.concatenate([key_rows.reshape(shard_len, QK).T, value_rows.T], axis=0)
    tok_count = residual.shape[0]
    slot_cap = max(2, 9 * tok_count * TOPK // (8 * sp_count))
    slot_total = sp_count * slot_cap
    targets = slot_targets(routes, sp_count, slot_cap)
    slot_ids = jnp.arange(slot_total, dtype=jnp.int32)
    hits = targets[:, :, None] == slot_ids[None, None, :]
    chooser = jnp.any(slot_ids[:, None, None] == targets[None, :, :], axis=2).astype(jnp.bfloat16)
    mix = jnp.sum(jnp.where(hits, route_weights[:, :, None], 0.0), axis=1)
    mix_high = lax.reduce_precision(mix, 8, 7)
    mix_mid = lax.reduce_precision(mix - mix_high, 8, 7)
    mix_low = mix - mix_high - mix_mid
    mix_parts = jnp.stack([mix_high, mix_mid, mix_low]).astype(jnp.bfloat16)
    return layer(
        jnp.pad(query_rows.reshape(shard_len, QK), ((0, 0), (0, 128 - QK))),
        bundle,
        expert_down[0],
        out_weight,
        residual,
        out_gain[None, :],
        ffn_gain[None, :],
        chooser,
        expert_gate[0],
        expert_up[0],
        mix_parts,
    )


def solution(mesh):
    return jax.shard_map(
        shards,
        mesh=mesh,
        in_specs=(
            P("sp", "tp"),
            P("sp", None),
            P("sp", None),
            P(),
            P(None, "tp"),
            P(None, "tp"),
            P(),
            P(),
            P(),
            P(),
            P(("sp", "tp"), None),
            P(),
            P(("sp", "tp"), None),
            P(("sp", "tp"), None),
            P("sp", None, "tp"),
            P("sp", None, "tp"),
            P("sp", "tp", None),
        ),
        out_specs=P(("sp", "tp"), None),
        check_vma=False,
    )
```
